256 devices in a mesh: rep: 2 (over z_hi), fs: 16 (over z_lo, y), tp: 8 (over x, core).
Axes of the slice: x: 4, y: 4, z: 8 (z_hi: 2, z_lo: 4; z = z_hi * 4 + z_lo), core: 2. Of those that a mesh axis runs over, the one named last changes fastest.
Arguments:
- activations: bfloat16 [12288, 2048], P(('rep', 'fs'), 'tp'), may hold values from -16 to 16
- norm_gain: float32 [2048], replicated, may hold values from 0.1 to 1.9
- query_weight: bfloat16 [2048, 512], P('fs', 'tp'), may hold values from -0.125 to 0.125
- key_weight: bfloat16 [2048, 512], P('fs', 'tp'), may hold values from -0.125 to 0.125
- value_weight: bfloat16 [2048, 512], P('fs', 'tp'), may hold values from -0.125 to 0.125
- gate_weight: bfloat16 [2048, 512], P('fs', 'tp'), may hold values from -0.125 to 0.125
- out_weight: bfloat16 [512, 2048], P('tp', 'fs'), may hold values from -0.25 to 0.25
- mlp_gain: float32 [2048], replicated, may hold values from 0.1 to 1.9
- up_weight: bfloat16 [2048, 8192], P('fs', 'tp'), may hold values from -0.125 to 0.125
- down_weight: bfloat16 [8192, 2048], P('tp', 'fs'), may hold values from -0.0625 to 0.0625
Outputs:
- layer_out: bfloat16 [12288, 2048], P(('rep', 'fs'), 'tp')
The draws below stay inside these ranges and needn't reach their ends.
All inputs are finite; a program needn't handle non-finite values.
Results may differ from the reference program's by a relative error of at most 0.012.
Values may be sent and summed in bfloat16 or wider, within the bound.
A program may use at most 64 MiB of HBM per device.

```python
import math
import jax
import jax.numpy as jnp
from jax import lax

D = 2048
FF = 8192
HEADS = 8
HEAD_DIM = 64
BLOCK = 64
SEQ_LEN = 128
TOKENS = 12288
N_TP = 8


def draw_activations(key, part):
    key_base, key_column, key_row = jax.random.split(jax.random.fold_in(key, 11), 3)
    column_index = jnp.arange(D, dtype=jnp.float32)
    column_scale = jnp.power(3.0, column_index / (D - 1)) * jnp.exp(jax.random.uniform(key_column, (D,), jnp.float32, -0.35, 0.35))
    base_draw = jax.random.normal(key_base, (TOKENS, D), jnp.float32)
    row_scale = jnp.exp(jax.random.uniform(key_row, (TOKENS, 1), jnp.float32, 0.0, math.log(4.0)))
    return jnp.clip(0.5 * base_draw * row_scale * column_scale[None, :], -16.0, 16.0).astype(jnp.bfloat16)


def level_of(key, shape, cuts, least, largest):
    loudness = 1.0
    for dim, shards_of in cuts:
        steps = jax.random.uniform(jax.random.fold_in(jax.random.fold_in(key, 6), dim), (shards_of,), jnp.float32, least / len(cuts), largest / len(cuts))
        loudness = loudness * jnp.repeat(jnp.exp(steps), shape[dim] // shards_of).reshape((-1,) + (1,) * (len(shape) - 1 - dim))
    return loudness


def noise(key, extent, scale, bound, cuts=(), kind=jnp.bfloat16):
    factor_of = level_of(key, extent, cuts, -0.22, 0.18) if cuts else 1.0
    values = jax.random.normal(key, extent, jnp.float32) * scale * factor_of
    return jnp.minimum(jnp.maximum(values, -bound), bound).astype(kind)


def setup_inputs(seed: int = 0) -> dict:
    streams_of = jax.random.split(jax.random.key(seed), 11)
    return {
        "activations": draw_activations(jax.random.fold_in(streams_of[10], 71), 0),
        "norm_gain": jnp.clip(1.0 + 0.18 * jax.random.normal(streams_of[1], (D,), jnp.float32), 0.1, 1.9),
        "query_weight": noise(streams_of[2], (D, HEADS * HEAD_DIM), D ** -0.5, 0.125, ((0, 16), (1, 8))),
        "key_weight": noise(streams_of[3], (D, HEADS * HEAD_DIM), D ** -0.5, 0.125, ((0, 16), (1, 8))),
        "value_weight": noise(streams_of[4], (D, HEADS * HEAD_DIM), D ** -0.5, 0.125, ((0, 16), (1, 8))),
        "gate_weight": noise(streams_of[5], (D, HEADS * HEAD_DIM), D ** -0.5, 0.125, ((0, 16), (1, 8))),
        "out_weight": noise(streams_of[6], (HEADS * HEAD_DIM, D), (HEADS * HEAD_DIM) ** -0.5, 0.25, ((0, 8), (1, 16))),
        "mlp_gain": jnp.clip(1.0 + 0.18 * jax.random.normal(streams_of[7], (D,), jnp.float32), 0.1, 1.9),
        "up_weight": noise(streams_of[8], (D, FF), D ** -0.5, 0.125, ((0, 16), (1, 8))),
        "down_weight": noise(streams_of[9], (FF, D), FF ** -0.5, 0.0625, ((0, 8), (1, 16))),
    }


EPSILON = 1e-06

def rms_norm(rows, gain):
    floats = rows.astype(jnp.float32)
    scaled = floats * lax.rsqrt(lax.optimization_barrier(jnp.mean(floats * floats, axis=-1, keepdims=True)) + EPSILON)
    return (scaled * gain.astype(jnp.float32)).astype(jnp.bfloat16)

def rotate(raw, cosine, sine, seqs, heads):
    half = HEAD_DIM // 2
    shaped = raw.reshape(seqs, SEQ_LEN, heads, HEAD_DIM)
    first, second = (shaped[..., :half], shaped[..., half:])
    return jnp.concatenate([first * cosine - second * sine, second * cosine + first * sine], axis=-1)

def retain(query_raw, key_raw, value_rows, gate_rows, first_head):
    tokens = query_raw.shape[0]
    heads = query_raw.shape[1] // HEAD_DIM
    seqs = tokens // SEQ_LEN
    blocks = SEQ_LEN // BLOCK
    half = HEAD_DIM // 2
    position = jnp.arange(SEQ_LEN, dtype=jnp.float32)
    freqs = 10000.0 ** (-jnp.arange(half, dtype=jnp.float32) / half)
    angle = position[:, None] * freqs[None, :]
    cosine = jnp.cos(angle)[:, None, :]
    sine = jnp.sin(angle)[:, None, :]
    shape_five = (seqs, blocks, BLOCK, heads, HEAD_DIM)
    queries = rotate(query_raw, cosine, sine, seqs, heads).astype(jnp.bfloat16).reshape(shape_five)
    key_block = (rotate(key_raw, cosine, sine, seqs, heads) * HEAD_DIM ** (-0.5)).astype(jnp.bfloat16).reshape(shape_five)
    value_block = value_rows.reshape(shape_five)
    head_index = first_head + jnp.arange(heads, dtype=jnp.float32)
    exponent = 5.0 + 4.0 * head_index / (HEADS - 1)
    log_gamma = jnp.log(1.0 - jnp.power(2.0, -exponent))
    offsets = jnp.arange(BLOCK, dtype=jnp.float32)
    distance = offsets[:, None] - offsets[None, :]
    decay_mask = jnp.where(distance[None] >= 0, jnp.exp(jnp.maximum(distance, 0.0)[None] * log_gamma[:, None, None]), 0.0)
    scores = jnp.einsum('snbhd,snchd->snhbc', queries.astype(jnp.float32), key_block.astype(jnp.float32))
    weights = (scores * decay_mask[None, None]).astype(jnp.bfloat16)
    inner = jnp.einsum('snhbc,snchd->snbhd', weights.astype(jnp.float32), value_block.astype(jnp.float32))
    query_decay = queries.astype(jnp.float32) * jnp.exp((offsets + 1.0)[:, None] * log_gamma[None, :])[:, :, None]
    key_decay = key_block.astype(jnp.float32) * jnp.exp((BLOCK - 1.0 - offsets)[:, None] * log_gamma[None, :])[:, :, None]
    block_decay = jnp.exp(BLOCK * log_gamma)[None, :, None, None]

    def advance(state, inputs):
        query_now, key_now, value_now = inputs
        carried = jnp.einsum('sbhd,shde->sbhe', query_now, state, precision=lax.Precision.HIGHEST)
        state = state * block_decay + jnp.einsum('sbhd,sbhe->shde', key_now, value_now, precision=lax.Precision.HIGHEST)
        return (state, carried)
    initial = jnp.zeros((seqs, heads, HEAD_DIM, HEAD_DIM), jnp.float32)
    _, cross = lax.scan(advance, initial, (jnp.moveaxis(query_decay, 1, 0), jnp.moveaxis(key_decay, 1, 0), jnp.moveaxis(value_block.astype(jnp.float32), 1, 0)))
    mixed = (inner + jnp.moveaxis(cross, 0, 1)).reshape(tokens, heads, HEAD_DIM)
    centred = mixed - lax.optimization_barrier(jnp.mean(mixed, axis=-1, keepdims=True))
    normed = centred * lax.rsqrt(lax.optimization_barrier(jnp.mean(centred * centred, axis=-1, keepdims=True)) + EPSILON)
    gated = normed * jax.nn.silu(gate_rows.reshape(tokens, heads, HEAD_DIM))
    return gated.reshape(tokens, heads * HEAD_DIM).astype(jnp.bfloat16)

def reference(activations, norm_gain, query_weight, key_weight, value_weight, gate_weight, out_weight, mlp_gain, up_weight, down_weight):
    normed = rms_norm(activations, norm_gain)
    query_raw = jnp.dot(normed, query_weight, preferred_element_type=jnp.float32)
    key_raw = jnp.dot(normed, key_weight, preferred_element_type=jnp.float32)
    value_rows = jnp.dot(normed, value_weight, preferred_element_type=jnp.float32).astype(jnp.bfloat16)
    gate_rows = jnp.dot(normed, gate_weight, preferred_element_type=jnp.float32)
    retained = retain(query_raw, key_raw, value_rows, gate_rows, 0.0)
    branch = jnp.dot(retained, out_weight, preferred_element_type=jnp.float32)
    middle = (activations.astype(jnp.float32) + branch).astype(jnp.bfloat16)
    second = rms_norm(middle, mlp_gain)
    hidden = jnp.square(jax.nn.relu(jnp.dot(second, up_weight, preferred_element_type=jnp.float32))).astype(jnp.bfloat16)
    group_width = FF // N_TP
    hidden_parts = jnp.moveaxis(hidden.reshape(hidden.shape[0], N_TP, group_width), 1, 0)
    down_parts = down_weight.reshape(N_TP, group_width, D)

    def accumulate(running, inputs):
        part_rows, part_weight = inputs
        rounded = lax.optimization_barrier(jnp.dot(part_rows, part_weight, preferred_element_type=jnp.float32).astype(jnp.bfloat16))
        return (running + rounded.astype(jnp.float32), None)
    summed, _ = lax.scan(accumulate, jnp.zeros((hidden.shape[0], D), jnp.float32), (hidden_parts, down_parts))
    return (middle.astype(jnp.float32) + summed).astype(jnp.bfloat16)
```

```python
import numpy as np
import jax
import jax.numpy as jnp
from jax import lax
from jax.experimental import pallas as pl
from jax.experimental.pallas import tpu as pltpu
from jax.sharding import PartitionSpec as P

HEADS = 8
HEAD_DIM = 64
SEQ_LEN = 128
EPSILON = 1e-06
ROWS = 384
D = 2048
NX = 4
BF = jnp.bfloat16
F32 = jnp.float32
MESH = pl.DeviceIdType.MESH
ATTN, UP, DOWN = 0, 1, 2


def rotary_tables():
    half = HEAD_DIM // 2
    position = np.arange(SEQ_LEN, dtype=np.float32)
    freqs = np.float32(10000.0) ** (-np.arange(half, dtype=np.float32) / np.float32(half))
    angle = position[:, None] * freqs[None, :].astype(np.float32)
    cosine, sine = np.cos(angle), np.sin(angle)
    scale = np.float32(HEAD_DIM**-0.5)
    c = np.concatenate([cosine, cosine, cosine * scale, cosine * scale], axis=1)
    s = np.concatenate([-sine, sine, -sine * scale, sine * scale], axis=1)
    return c.astype(np.float32), s.astype(np.float32)


def log_gammas():
    head = np.arange(HEADS, dtype=np.float32)
    exponent = np.float32(5.0) + np.float32(4.0) * head / np.float32(HEADS - 1)
    return np.log(1.0 - np.power(2.0, -exponent.astype(np.float64)))


def lanes(shape):
    return lax.broadcasted_iota(jnp.int32, shape, len(shape) - 1)


def layer_kernel(
    act_hbm, ng_hbm, qw_hbm, kw_hbm, vw_hbm, gw_hbm, ow_hbm, mg_hbm, uw_hbm, dw_hbm, cos_hbm, sin_hbm,
    out_ref,
    attn, upb, dnb, xall, wo, ret, wide, mid, hid, pps, ppr, rss, rsr,
    small, gains, tables, qkvg, gat, lhs, acc,
    local_sem, ring_send, ring_recv, x_send, x_recv, p_send, p_recv, r_send, r_recv,
):
    rep, fs, tp = lax.axis_index("rep"), lax.axis_index("fs"), lax.axis_index("tp")
    zl, y = lax.div(fs, 4), lax.rem(fs, 4)
    x, core = lax.div(tp, 2), lax.rem(tp, 2)
    zg = rep * 4 + zl

    def y_device(step):
        return {"fs": zl * 4 + lax.rem(y + step + 4, 4)}

    def z_device(step):
        other = lax.rem(zg + step + 8, 8)
        return {"rep": lax.div(other, 4), "fs": lax.rem(other, 4) * 4 + y}

    def x_index(step, c=core):
        return lax.rem(x + step + 4, 4) * 2 + c

    def x_device(step):
        return {"tp": x_index(step)}

    partner = {"tp": x * 2 + (1 - core)}

    loads = [
        pltpu.make_async_copy(qw_hbm, small.at[0], local_sem.at[0]),
        pltpu.make_async_copy(kw_hbm, small.at[1], local_sem.at[1]),
        pltpu.make_async_copy(vw_hbm, small.at[2], local_sem.at[2]),
        pltpu.make_async_copy(gw_hbm, small.at[3], local_sem.at[3]),
        pltpu.make_async_copy(ow_hbm.at[pl.ds(0, 32)], attn.at[0, zl, y, pl.ds(128, 32)], local_sem.at[4]),
        pltpu.make_async_copy(ow_hbm.at[pl.ds(32, 32)], attn.at[1, zl, y, pl.ds(128, 32)], local_sem.at[5]),
        pltpu.make_async_copy(act_hbm, xall.at[tp], local_sem.at[6]),
        pltpu.make_async_copy(uw_hbm.at[:, pl.ds(0, 512)], upb.at[0, zl, y], local_sem.at[7]),
        pltpu.make_async_copy(uw_hbm.at[:, pl.ds(512, 512)], upb.at[1, zl, y], local_sem.at[8]),
        pltpu.make_async_copy(dw_hbm.at[pl.ds(0, 512)], dnb.at[0, zl, y], local_sem.at[9]),
        pltpu.make_async_copy(dw_hbm.at[pl.ds(512, 512)], dnb.at[1, zl, y], local_sem.at[10]),
        pltpu.make_async_copy(ng_hbm, gains.at[0], local_sem.at[11]),
        pltpu.make_async_copy(mg_hbm, gains.at[1], local_sem.at[12]),
        pltpu.make_async_copy(cos_hbm, tables.at[0], local_sem.at[13]),
        pltpu.make_async_copy(sin_hbm, tables.at[1], local_sem.at[14]),
    ]
    for copy in loads:
        copy.start()

    barrier = pltpu.get_barrier_semaphore()
    peers = [y_device(1), y_device(-1), z_device(1), z_device(-1), x_device(1), x_device(-1), x_device(2), partner]
    for peer in peers:
        pl.semaphore_signal(barrier, inc=1, device_id=peer, device_id_type=MESH)
    for copy in loads:
        copy.wait()
    attn[0, zl, y, 0:128, :] = jnp.concatenate([small[0], small[1]], axis=1)
    attn[1, zl, y, 0:128, :] = jnp.concatenate([small[2], small[3]], axis=1)
    pl.semaphore_wait(barrier, len(peers))

    started = []

    def send(src, dst, send_sem, recv_sem, device):
        copy = pltpu.make_async_remote_copy(
            src_ref=src, dst_ref=dst, send_sem=send_sem, recv_sem=recv_sem, device_id=device, device_id_type=MESH
        )
        copy.start()
        started.append(copy)

    def arrive(region, send_sem, recv_sem, device):
        pltpu.make_async_remote_copy(
            src_ref=region, dst_ref=region, send_sem=send_sem, recv_sem=recv_sem, device_id=device, device_id_type=MESH
        ).wait_recv()

    bufs = (attn, upb, dnb)
    depth = (160, 128, 512)

    def along_y(half, phase):
        return (half + phase) % 2 == 0

    def piece(item, half, phase, step, p):
        buf, cut = bufs[item], depth[item] // 2
        if along_y(half, phase):
            j = lax.rem(y + step + 4, 4)
            if phase == 0:
                return buf.at[half, zl, j, pl.ds(p * cut, cut)]
            return buf.at[half, pl.ds(2 * p, 2), j]
        j = lax.rem(zl + step + 4, 4)
        if phase == 0:
            return buf.at[half, j, y, pl.ds(p * cut, cut)]
        return buf.at[half, j, pl.ds(2 * p, 2)]

    def ring_device(half, phase, step):
        return y_device(step) if along_y(half, phase) else z_device(step)

    def ring_sems(item, half, phase, kind):
        k = ((item * 2 + half) * 2 + phase) * 6 + kind
        return ring_send.at[k], ring_recv.at[k]

    def ring_start(item, phase):
        for p in range(2):
            for half in range(2):
                for d in range(2):
                    q = p if d == 0 else 1 - p
                    ref = piece(item, half, phase, 0, q)
                    send(ref, ref, *ring_sems(item, half, phase, 2 * d + q), ring_device(half, phase, 1 - 2 * d))

    def ring_forward(item, phase):
        for half in range(2):
            for d in range(2):
                to = 1 - 2 * d
                ref = piece(item, half, phase, -to, d)
                arrive(ref, *ring_sems(item, half, phase, 2 * d + d), ring_device(half, phase, to))
                send(ref, ref, *ring_sems(item, half, phase, 4 + d), ring_device(half, phase, to))

    def ring_near(item, phase):
        for half in range(2):
            for d in range(2):
                to = 1 - 2 * d
                ref = piece(item, half, phase, -to, 1 - d)
                arrive(ref, *ring_sems(item, half, phase, 2 * d + 1 - d), ring_device(half, phase, to))

    def ring_far(item, phase):
        for half in range(2):
            for d in range(2):
                ref = piece(item, half, phase, 2, d)
                arrive(ref, *ring_sems(item, half, phase, 4 + d), ring_device(half, phase, 1 - 2 * d))

    def x_piece(which, t, p):
        if which == 0:
            return xall.at[t, pl.ds(p * 192, 192)]
        if which == 1:
            return wo.at[t, p]
        return ret.at[t, pl.ds(p * 96, 96)]

    def x_sems(which, kind):
        k = which * 14 + kind
        return x_send.at[k], x_recv.at[k]

    def hand_over(which, place, p):
        ref = x_piece(which, x_index((0, -1, 1, 2)[place]), p)
        send(ref, ref, *x_sems(which, 6 + 2 * place + p), partner)

    def x_start(which):
        for p in range(2):
            for d in range(2):
                q = p if d == 0 else 1 - p
                dst = x_piece(which, tp, q)
                src = attn.at[q, :, :, pl.ds(128, 32)] if which == 1 else dst
                send(src, dst, *x_sems(which, 2 * d + q), x_device(1 - 2 * d))
        for p in range(2):
            dst = x_piece(which, tp, p)
            src = attn.at[p, :, :, pl.ds(128, 32)] if which == 1 else dst
            send(src, dst, *x_sems(which, 6 + p), partner)

    def x_forward(which):
        for d in range(2):
            to = 1 - 2 * d
            ref = x_piece(which, x_index(-to), d)
            arrive(ref, *x_sems(which, 2 * d + d), x_device(to))
            send(ref, ref, *x_sems(which, 4 + d), x_device(to))
            hand_over(which, 1 + d, d)

    def x_near(which):
        for d in range(2):
            to = 1 - 2 * d
            arrive(x_piece(which, x_index(-to), 1 - d), *x_sems(which, 2 * d + 1 - d), x_device(to))
            hand_over(which, 1 + d, 1 - d)

    def x_far(which):
        for d in range(2):
            arrive(x_piece(which, x_index(2), d), *x_sems(which, 4 + d), x_device(1 - 2 * d))
            hand_over(which, 3, d)

    def x_partner(which):
        for place in range(4):
            t = x_index((0, -1, 1, 2)[place], 1 - core)
            for p in range(2):
                arrive(x_piece(which, t, p), *x_sems(which, 6 + 2 * place + p), partner)

    def norm_rows(source, gain):
        @pl.loop(0, ROWS // 16)
        def _(i):
            rows = pl.ds(pl.multiple_of(i * 16, 16), 16)
            blocks = [source[t, rows, :].astype(F32) for t in range(8)]
            squares = blocks[0] * blocks[0]
            for b in blocks[1:]:
                squares = squares + b * b
            scale = lax.rsqrt(jnp.sum(squares, axis=-1, keepdims=True) * (1.0 / D) + EPSILON)
            for t in range(8):
                columns = slice(256 * t, 256 * t + 256)
                wide[rows, columns] = (blocks[t] * scale * gains[gain, :, columns]).astype(BF)

    ring_start(ATTN, 0)
    x_start(0)
    ring_start(UP, 0)
    ring_forward(ATTN, 0)
    ring_near(ATTN, 0)
    x_forward(0)
    ring_far(ATTN, 0)
    ring_start(ATTN, 1)
    ring_forward(UP, 0)
    x_near(0)
    x_far(0)
    ring_forward(ATTN, 1)
    ring_start(DOWN, 0)
    ring_near(UP, 0)
    ring_far(UP, 0)
    ring_start(UP, 1)
    x_partner(0)
    norm_rows(xall, 0)
    ring_near(ATTN, 1)
    ring_far(ATTN, 1)
    x_start(1)
    ring_forward(DOWN, 0)

    weights = jnp.concatenate([attn[h, :, :, 0:128, :].reshape(D, 128) for h in range(2)], axis=1)
    qkvg[...] = jnp.dot(wide[...], weights, preferred_element_type=F32)
    log_gamma = jnp.float32(0.0)
    for h, value in enumerate(log_gammas()):
        log_gamma = jnp.where(tp == h, jnp.float32(value), log_gamma)
    square = (SEQ_LEN, SEQ_LEN)
    distance = (lax.broadcasted_iota(jnp.int32, square, 0) - lanes(square)).astype(F32)
    decay = jnp.where(distance >= 0, jnp.exp(jnp.maximum(distance, 0.0) * log_gamma), 0.0)
    lane = lanes(square)
    first, low = lax.rem(lane, 64) < 32, lane < 64
    for s in range(3):
        rows = slice(SEQ_LEN * s, SEQ_LEN * (s + 1))
        qk, vg = qkvg[rows, 0:128], qkvg[rows, 128:256]
        other = jnp.where(first, pltpu.roll(qk, 96, 1), pltpu.roll(qk, 32, 1))
        turned = (qk * tables[0] + other * tables[1]).astype(BF).astype(F32)
        queries = jnp.where(low, turned, 0.0).astype(BF)
        keys = pltpu.roll(turned, 64, 1).astype(BF)
        scores = lax.dot_general(queries, keys, (((1,), (1,)), ((), ())), preferred_element_type=F32)
        mixed = jnp.dot((scores * decay).astype(BF), vg.astype(BF), preferred_element_type=F32)
        mixed = jnp.where(low, mixed, 0.0)
        mean = jnp.sum(mixed, axis=-1, keepdims=True) * (1.0 / HEAD_DIM)
        centred = jnp.where(low, mixed - mean, 0.0)
        variance = jnp.sum(centred * centred, axis=-1, keepdims=True) * (1.0 / HEAD_DIM)
        gate = pltpu.roll(vg, 64, 1)
        gat[rows, :] = centred * lax.rsqrt(variance + EPSILON) * (gate / (1.0 + jnp.exp(-gate)))
    low = lanes((192, 128)) < 64
    ret[tp] = jnp.where(low, gat[0:192, :], pltpu.roll(gat[192:384, :], 64, 1)).astype(BF)
    x_start(2)
    for h in range(2):
        wo[tp, h] = attn[h, :, :, 128:160, :]
    x_forward(1)
    x_near(1)
    x_forward(2)
    x_near(2)
    x_far(2)
    ring_forward(UP, 1)
    ring_near(DOWN, 0)
    ring_far(DOWN, 0)
    ring_start(DOWN, 1)
    x_far(1)
    x_partner(2)
    x_partner(1)

    for j in range(4):
        a, b = ret[2 * j].astype(F32), ret[2 * j + 1].astype(F32)
        lhs[0:192, 128 * j : 128 * j + 128] = jnp.where(low, a, pltpu.roll(b, 64, 1)).astype(BF)
        lhs[192:384, 128 * j : 128 * j + 128] = jnp.where(low, pltpu.roll(a, 64, 1), b).astype(BF)

    @pl.loop(0, 8)
    def _(t):
        z0, y0 = lax.div(t, 2), lax.rem(t, 2) * 2
        columns = [wo[:, :, z0, y0 + k].reshape(HEADS * HEAD_DIM, 128) for k in range(2)]
        branch = jnp.dot(lhs[...], jnp.concatenate(columns, axis=1), preferred_element_type=F32)
        mid[t] = (xall[t].astype(F32) + branch).astype(BF)

    norm_rows(mid, 1)
    ring_near(UP, 1)
    ring_far(UP, 1)
    for h in range(2):
        raw = jnp.dot(wide[...], upb[h].reshape(D, 512), preferred_element_type=F32)
        raw = jnp.maximum(raw, 0.0)
        hid[:, 512 * h : 512 * h + 512] = (raw * raw).astype(BF)
    ring_forward(DOWN, 1)
    ring_near(DOWN, 1)
    ring_far(DOWN, 1)

    def part(t):
        z0, y0 = lax.div(t, 2), lax.rem(t, 2) * 2
        total = None
        for h in range(2):
            columns = jnp.concatenate([dnb[h, z0, y0], dnb[h, z0, y0 + 1]], axis=1)
            term = jnp.dot(hid[:, 512 * h : 512 * h + 512], columns, preferred_element_type=F32)
            total = term if total is None else total + term
        return total

    for i in (1, 2, 3, 0):
        pps[i] = part(x_index(i, 1 - core)).astype(BF)
        send(pps.at[i], ppr.at[i], p_send.at[i], p_recv.at[i], partner)
    for i in (1, 2, 3, 0):
        total = part(x_index(i))
        arrive(ppr.at[i], p_send.at[i], p_recv.at[i], partner)
        total = total + ppr[i].astype(F32)
        if i:
            rss[i - 1] = total.astype(BF)
            send(rss.at[i - 1], rsr.at[i - 1], r_send.at[i - 1], r_recv.at[i - 1], x_device(i))
        else:
            acc[...] = mid[tp].astype(F32) + total
    for i in range(3):
        arrive(rsr.at[i], r_send.at[i], r_recv.at[i], x_device(i + 1))
    out_ref[...] = (acc[...] + rsr[0].astype(F32) + rsr[1].astype(F32) + rsr[2].astype(F32)).astype(BF)
    for copy in started:
        copy.wait_send()


def local(activations, norm_gain, qw, kw, vw, gw, ow, mlp_gain, uw, dw):
    cosine, sine = rotary_tables()
    operands = (
        activations, norm_gain.reshape(1, D), qw, kw, vw, gw, ow, mlp_gain.reshape(1, D), uw, dw,
        jnp.asarray(cosine), jnp.asarray(sine),
    )
    dma = pltpu.SemaphoreType.DMA
    return pl.pallas_call(
        layer_kernel,
        out_shape=jax.ShapeDtypeStruct((ROWS, D // 8), BF),
        in_specs=[pl.BlockSpec(memory_space=pltpu.HBM)] * len(operands),
        out_specs=pl.BlockSpec(memory_space=pltpu.VMEM),
        scratch_shapes=[
            pltpu.VMEM((2, 4, 4, 160, 128), BF),
            pltpu.VMEM((2, 4, 4, 128, 512), BF),
            pltpu.VMEM((2, 4, 4, 512, 128), BF),
            pltpu.VMEM((8, ROWS, 256), BF),
            pltpu.VMEM((8, 2, 4, 4, 32, 128), BF),
            pltpu.VMEM((8, 192, 128), BF),
            pltpu.VMEM((ROWS, D), BF),
            pltpu.VMEM((8, ROWS, 256), BF),
            pltpu.VMEM((ROWS, 1024), BF),
            pltpu.VMEM((4, ROWS, 256), BF),
            pltpu.VMEM((4, ROWS, 256), BF),
            pltpu.VMEM((3, ROWS, 256), BF),
            pltpu.VMEM((3, ROWS, 256), BF),
            pltpu.VMEM((4, 128, 64), BF),
            pltpu.VMEM((2, 1, D), F32),
            pltpu.VMEM((2, 128, 128), F32),
            pltpu.VMEM((ROWS, 256), F32),
            pltpu.VMEM((ROWS, 128), F32),
            pltpu.VMEM((ROWS, 512), BF),
            pltpu.VMEM((ROWS, 256), F32),
            dma((15,)), dma((72,)), dma((72,)), dma((42,)), dma((42,)), dma((4,)), dma((4,)), dma((3,)), dma((3,)),
        ],
        compiler_params=pltpu.CompilerParams(
            collective_id=0, has_side_effects=True, vmem_limit_bytes=56 * 1024 * 1024
        ),
        name="layer",
    )(*operands)


def solution(mesh):
    in_specs = (
        P(("rep", "fs"), "tp"), P(), P("fs", "tp"), P("fs", "tp"), P("fs", "tp"), P("fs", "tp"), P("tp", "fs"), P(),
        P("fs", "tp"), P("tp", "fs"),
    )
    return jax.shard_map(local, mesh=mesh, in_specs=in_specs, out_specs=P(("rep", "fs"), "tp"), check_vma=False)
```

```python
import numpy as np
import jax
import jax.numpy as jnp
from jax import lax
from jax.experimental import pallas as pl
from jax.experimental.pallas import tpu as pltpu
from jax.sharding import PartitionSpec as P

HEADS = 8
HEAD_DIM = 64
SEQ_LEN = 128
EPSILON = 1e-06
ROWS = 384
D = 2048
NX = 4
BF = jnp.bfloat16
F32 = jnp.float32
MESH = pl.DeviceIdType.MESH
ATTN, UP, DOWN = 0, 1, 2
ORDER = ((0, 1, -1, 2), (-1, 2, 0, 1))


def rotary_tables():
    half = HEAD_DIM // 2
    position = np.arange(SEQ_LEN, dtype=np.float32)
    freqs = np.float32(10000.0) ** (-np.arange(half, dtype=np.float32) / np.float32(half))
    angle = position[:, None] * freqs[None, :].astype(np.float32)
    cosine, sine = np.cos(angle), np.sin(angle)
    scale = np.float32(HEAD_DIM**-0.5)
    c = np.concatenate([cosine, cosine, cosine * scale, cosine * scale], axis=1)
    s = np.concatenate([-sine, sine, -sine * scale, sine * scale], axis=1)
    return c.astype(np.float32), s.astype(np.float32)


def log_gammas():
    head = np.arange(HEADS, dtype=np.float32)
    exponent = np.float32(5.0) + np.float32(4.0) * head / np.float32(HEADS - 1)
    return np.log(1.0 - np.power(2.0, -exponent.astype(np.float64)))


def lanes(shape):
    return lax.broadcasted_iota(jnp.int32, shape, len(shape) - 1)


def layer_kernel(
    act_hbm, ng_hbm, qw_hbm, kw_hbm, vw_hbm, gw_hbm, ow_hbm, mg_hbm, uw_hbm, dw_hbm, cos_hbm, sin_hbm,
    out_ref,
    attn, upb, dnb, xall, wo, ret, wide, mid, hid, pps, ppr, rss, rsr,
    small, gains, tables, qkvg, gat, lhs, acc,
    local_sem, first_send, first_recv, second_send, second_recv, x_send, x_recv, p_send, p_recv, r_send, r_recv,
):
    rep, fs, tp = lax.axis_index("rep"), lax.axis_index("fs"), lax.axis_index("tp")
    zl, y = lax.div(fs, 4), lax.rem(fs, 4)
    x, core = lax.div(tp, 2), lax.rem(tp, 2)
    zg = rep * 4 + zl

    def y_device(step):
        return {"fs": zl * 4 + lax.rem(y + step + 4, 4)}

    def z_device(step):
        other = lax.rem(zg + step + 8, 8)
        return {"rep": lax.div(other, 4), "fs": lax.rem(other, 4) * 4 + y}

    def x_index(step, c=core):
        return lax.rem(x + step + 4, 4) * 2 + c

    def x_device(step):
        return {"tp": x_index(step)}

    partner = {"tp": x * 2 + (1 - core)}

    loads = [
        pltpu.make_async_copy(qw_hbm, small.at[0], local_sem.at[0]),
        pltpu.make_async_copy(kw_hbm, small.at[1], local_sem.at[1]),
        pltpu.make_async_copy(vw_hbm, small.at[2], local_sem.at[2]),
        pltpu.make_async_copy(gw_hbm, small.at[3], local_sem.at[3]),
        pltpu.make_async_copy(ow_hbm.at[pl.ds(0, 32)], attn.at[0, zl, y, pl.ds(128, 32)], local_sem.at[4]),
        pltpu.make_async_copy(ow_hbm.at[pl.ds(32, 32)], attn.at[1, zl, y, pl.ds(128, 32)], local_sem.at[5]),
        pltpu.make_async_copy(act_hbm, xall.at[tp], local_sem.at[6]),
        pltpu.make_async_copy(uw_hbm.at[:, pl.ds(0, 512)], upb.at[0, zl, y], local_sem.at[7]),
        pltpu.make_async_copy(uw_hbm.at[:, pl.ds(512, 512)], upb.at[1, zl, y], local_sem.at[8]),
        pltpu.make_async_copy(dw_hbm.at[pl.ds(0, 512)], dnb.at[0, zl, y], local_sem.at[9]),
        pltpu.make_async_copy(dw_hbm.at[pl.ds(512, 512)], dnb.at[1, zl, y], local_sem.at[10]),
        pltpu.make_async_copy(ng_hbm, gains.at[0], local_sem.at[11]),
        pltpu.make_async_copy(mg_hbm, gains.at[1], local_sem.at[12]),
        pltpu.make_async_copy(cos_hbm, tables.at[0], local_sem.at[13]),
        pltpu.make_async_copy(sin_hbm, tables.at[1], local_sem.at[14]),
    ]
    for copy in loads:
        copy.start()

    barrier = pltpu.get_barrier_semaphore()
    peers = [y_device(1), y_device(-1), z_device(1), z_device(-1), partner]
    peers += [{"tp": x_index(step, c)} for step in (1, -1, 2) for c in range(2)]
    for peer in peers:
        pl.semaphore_signal(barrier, inc=1, device_id=peer, device_id_type=MESH)
    for copy in loads:
        copy.wait()
    for h in range(2):
        attn[h, zl, y, 0:128, :] = small[2 * h : 2 * h + 2].reshape(128, 128).astype(F32).T.astype(BF)
    pl.semaphore_wait(barrier, len(peers))

    started = []

    def send(src, dst, send_sem, recv_sem, device):
        copy = pltpu.make_async_remote_copy(
            src_ref=src, dst_ref=dst, send_sem=send_sem, recv_sem=recv_sem, device_id=device, device_id_type=MESH
        )
        copy.start()
        started.append(copy)

    def arrive(region, send_sem, recv_sem, device):
        pltpu.make_async_remote_copy(
            src_ref=region, dst_ref=region, send_sem=send_sem, recv_sem=recv_sem, device_id=device, device_id_type=MESH
        ).wait_recv()

    bufs = (attn, upb, dnb)
    depth = (160, 128, 512)

    def block(item, half, dz, dy):
        return bufs[item].at[half, lax.rem(zl + dz + 4, 4), lax.rem(y + dy + 4, 4)]

    def along_y(half, phase):
        return (half + phase) % 2 == 0

    def piece(item, half, step, p):
        cut = depth[item] // 2
        dz, dy = (0, step) if half == 0 else (step, 0)
        return block(item, half, dz, dy).at[pl.ds(p * cut, cut)]

    def ring_device(half, phase, step):
        return y_device(step) if along_y(half, phase) else z_device(step)

    def first_sems(item, half, d, kind):
        k = ((item * 2 + half) * 2 + d) * 3 + kind
        return first_send.at[k], first_recv.at[k]

    def first_start(item):
        for n in range(2):
            for half in range(2):
                for d in range(2):
                    p = n if d == 0 else 1 - n
                    ref = piece(item, half, 0, p)
                    send(ref, ref, *first_sems(item, half, d, n), ring_device(half, 0, 1 - 2 * d))

    def first_forward(item):
        for half in range(2):
            for d in range(2):
                to = 1 - 2 * d
                ref = piece(item, half, -to, d)
                arrive(ref, *first_sems(item, half, d, 0), ring_device(half, 0, to))
                send(ref, ref, *first_sems(item, half, d, 2), ring_device(half, 0, to))

    def first_near(item):
        for half in range(2):
            for d in range(2):
                to = 1 - 2 * d
                arrive(piece(item, half, -to, 1 - d), *first_sems(item, half, d, 1), ring_device(half, 0, to))

    def first_far(item):
        for half in range(2):
            for d in range(2):
                arrive(piece(item, half, 2, d), *first_sems(item, half, d, 2), ring_device(half, 0, 1 - 2 * d))

    def second_block(item, half, step, d, n):
        across = ORDER[d][n]
        return block(item, half, step, across) if half == 0 else block(item, half, across, step)

    def second_sems(item, half, d, kind):
        k = ((item * 2 + half) * 2 + d) * 6 + kind
        return second_send.at[k], second_recv.at[k]

    def second_start(item, *which):
        for n in which:
            for half in range(2):
                for d in range(2):
                    ref = second_block(item, half, 0, d, n)
                    send(ref, ref, *second_sems(item, half, d, n), ring_device(half, 1, 1 - 2 * d))

    def second_near(item, *which):
        for n in which:
            for half in range(2):
                for d in range(2):
                    to = 1 - 2 * d
                    arrive(second_block(item, half, -to, d, n), *second_sems(item, half, d, n), ring_device(half, 1, to))

    def second_forward(item, *which):
        for n in which:
            for half in range(2):
                for d in range(2):
                    to = 1 - 2 * d
                    ref = second_block(item, half, -to, d, n)
                    arrive(ref, *second_sems(item, half, d, n), ring_device(half, 1, to))
                    send(ref, ref, *second_sems(item, half, d, 4 + n), ring_device(half, 1, to))

    def second_far(item, *which):
        for n in which:
            for half in range(2):
                for d in range(2):
                    ref = second_block(item, half, 2, d, n)
                    arrive(ref, *second_sems(item, half, d, 4 + n), ring_device(half, 1, 1 - 2 * d))

    def x_piece(which, t, p):
        if which == 0:
            return xall.at[t, pl.ds(p * 192, 192)]
        if which == 1:
            return wo.at[t, p]
        return ret.at[t, pl.ds(p * 96, 96)]

    def x_sems(which, kind):
        k = which * 14 + kind
        return x_send.at[k], x_recv.at[k]

    def hand_over(which, place, p):
        ref = x_piece(which, x_index((0, -1, 1, 2)[place]), p)
        send(ref, ref, *x_sems(which, 6 + 2 * place + p), partner)

    def x_start(which):
        for p in range(2):
            for d in range(2):
                q = p if d == 0 else 1 - p
                dst = x_piece(which, tp, q)
                src = attn.at[q, :, :, pl.ds(128, 32)] if which == 1 else dst
                send(src, dst, *x_sems(which, 2 * d + q), x_device(1 - 2 * d))
        for p in range(2):
            dst = x_piece(which, tp, p)
            src = attn.at[p, :, :, pl.ds(128, 32)] if which == 1 else dst
            send(src, dst, *x_sems(which, 6 + p), partner)

    def x_forward(which):
        for d in range(2):
            to = 1 - 2 * d
            ref = x_piece(which, x_index(-to), d)
            arrive(ref, *x_sems(which, 2 * d + d), x_device(to))
            send(ref, ref, *x_sems(which, 4 + d), x_device(to))
            hand_over(which, 1 + d, d)

    def x_near(which):
        for d in range(2):
            to = 1 - 2 * d
            arrive(x_piece(which, x_index(-to), 1 - d), *x_sems(which, 2 * d + 1 - d), x_device(to))
            hand_over(which, 1 + d, 1 - d)

    def x_far(which):
        for d in range(2):
            arrive(x_piece(which, x_index(2), d), *x_sems(which, 4 + d), x_device(1 - 2 * d))
            hand_over(which, 3, d)

    def x_partner(which):
        for place in range(4):
            t = x_index((0, -1, 1, 2)[place], 1 - core)
            for p in range(2):
                arrive(x_piece(which, t, p), *x_sems(which, 6 + 2 * place + p), partner)

    def norm_rows(source, gain):
        @pl.loop(0, ROWS // 16)
        def _(i):
            rows = pl.ds(pl.multiple_of(i * 16, 16), 16)
            blocks = [source[t, rows, :].astype(F32) for t in range(8)]
            squares = blocks[0] * blocks[0]
            for b in blocks[1:]:
                squares = squares + b * b
            scale = lax.rsqrt(jnp.sum(squares, axis=-1, keepdims=True) * (1.0 / D) + EPSILON)
            for t in range(8):
                columns = slice(256 * t, 256 * t + 256)
                wide[rows, columns] = (blocks[t] * scale * gains[gain, :, columns]).astype(BF)

    first_start(ATTN)
    x_start(0)
    first_start(UP)
    first_forward(ATTN)
    first_near(ATTN)
    x_forward(0)
    first_far(ATTN)
    second_start(ATTN, 0, 1, 2, 3)
    first_forward(UP)
    x_near(0)
    second_forward(ATTN, 0, 1)
    first_start(DOWN)
    x_far(0)
    first_near(UP)
    first_far(UP)
    second_start(UP, 0, 1, 2, 3)
    second_near(ATTN, 2, 3)
    second_far(ATTN, 0, 1)
    x_start(1)
    x_partner(0)
    norm_rows(xall, 0)
    first_forward(DOWN)

    weights = jnp.concatenate([attn[h, :, :, 0:128, :].reshape(D, 128) for h in range(2)], axis=1)
    qkvg[...] = jnp.dot(wide[...], weights, preferred_element_type=F32)
    log_gamma = jnp.float32(0.0)
    for h, value in enumerate(log_gammas()):
        log_gamma = jnp.where(tp == h, jnp.float32(value), log_gamma)
    square = (SEQ_LEN, SEQ_LEN)
    distance = (lax.broadcasted_iota(jnp.int32, square, 0) - lanes(square)).astype(F32)
    decay = jnp.where(distance >= 0, jnp.exp(jnp.maximum(distance, 0.0) * log_gamma), 0.0)
    lane = lanes(square)
    first, low = lax.rem(lane, 64) < 32, lane < 64
    for s in range(3):
        rows = slice(SEQ_LEN * s, SEQ_LEN * (s + 1))
        qk, vg = qkvg[rows, 0:128], qkvg[rows, 128:256]
        other = jnp.where(first, pltpu.roll(qk, 96, 1), pltpu.roll(qk, 32, 1))
        turned = (qk * tables[0] + other * tables[1]).astype(BF).astype(F32)
        queries = jnp.where(low, turned, 0.0).astype(BF)
        keys = pltpu.roll(turned, 64, 1).astype(BF)
        scores = lax.dot_general(queries, keys, (((1,), (1,)), ((), ())), preferred_element_type=F32)
        mixed = jnp.dot((scores * decay).astype(BF), vg.astype(BF), preferred_element_type=F32)
        mixed = jnp.where(low, mixed, 0.0)
        mean = jnp.sum(mixed, axis=-1, keepdims=True) * (1.0 / HEAD_DIM)
        centred = jnp.where(low, mixed - mean, 0.0)
        variance = jnp.sum(centred * centred, axis=-1, keepdims=True) * (1.0 / HEAD_DIM)
        gate = pltpu.roll(vg, 64, 1)
        gat[rows, :] = centred * lax.rsqrt(variance + EPSILON) * (gate / (1.0 + jnp.exp(-gate)))
    low = lanes((192, 128)) < 64
    ret[tp] = jnp.where(low, gat[0:192, :], pltpu.roll(gat[192:384, :], 64, 1)).astype(BF)
    x_start(2)
    for h in range(2):
        wo[tp, h] = attn[h, :, :, 128:160, :]
    x_forward(1)
    x_forward(2)
    x_near(2)
    x_near(1)
    x_far(2)
    second_forward(UP, 0, 1)
    x_far(1)
    first_near(DOWN)
    first_far(DOWN)
    second_start(DOWN, 0, 1, 2)
    x_partner(2)
    x_partner(1)

    for j in range(4):
        a, b = ret[2 * j].astype(F32), ret[2 * j + 1].astype(F32)
        lhs[0:192, 128 * j : 128 * j + 128] = jnp.where(low, a, pltpu.roll(b, 64, 1)).astype(BF)
        lhs[192:384, 128 * j : 128 * j + 128] = jnp.where(low, pltpu.roll(a, 64, 1), b).astype(BF)

    @pl.loop(0, 8)
    def _(t):
        z0, y0 = lax.div(t, 2), lax.rem(t, 2) * 2
        columns = [wo[:, :, z0, y0 + k].reshape(HEADS * HEAD_DIM, 128) for k in range(2)]
        branch = jnp.dot(lhs[...], jnp.concatenate(columns, axis=1), preferred_element_type=F32)
        mid[t] = (xall[t].astype(F32) + branch).astype(BF)

    norm_rows(mid, 1)
    second_near(UP, 2, 3)
    second_far(UP, 0, 1)
    second_forward(DOWN, 0)
    for h in range(2):
        raw = jnp.dot(wide[...], upb[h].reshape(D, 512), preferred_element_type=F32)
        raw = jnp.maximum(raw, 0.0)
        hid[:, 512 * h : 512 * h + 512] = (raw * raw).astype(BF)
    second_forward(DOWN, 1)
    second_start(DOWN, 3)

    def number(dz, dy):
        return (dz + 1) * 4 + dy + 1

    begun = set()

    def products(pairs):
        done = []
        for half, blocks in pairs:
            columns = jnp.concatenate([block(DOWN, half, dz, dy)[...] for dz, dy in blocks], axis=1)
            both = jnp.dot(hid[:, 512 * half : 512 * half + 512], columns, preferred_element_type=F32)
            for k, at in enumerate(blocks):
                value, n = both[:, 128 * k : 128 * k + 128], number(*at)
                if at in begun:
                    acc[n] += value
                    done.append(at)
                else:
                    acc[n] = value
                    begun.add(at)
        return done

    def rows_of(c):
        return pl.ds(pl.multiple_of(c * 192, 64), 192)

    def swap(blocks):
        for at in blocks:
            n = number(*at)
            pps[n] = acc[n, rows_of(1 - core), :].astype(BF)
            send(pps.at[n], ppr.at[n], p_send.at[n], p_recv.at[n], partner)

    def owner_of(at):
        z_to, y_to = lax.rem(zl + at[0] + 4, 4), lax.rem(y + at[1] + 4, 4)
        t = z_to * 2 + lax.div(y_to, 2)
        k = lax.rem(y_to, 2)
        n = number(*at)
        copy = pltpu.make_async_remote_copy(
            src_ref=rss.at[n], dst_ref=rsr.at[x, k, core], send_sem=r_send.at[n],
            recv_sem=r_recv.at[(x * 2 + k) * 2 + core], device_id={"tp": t}, device_id_type=MESH,
        )
        return t, k, copy

    def deliver(blocks):
        for at in blocks:
            n = number(*at)
            arrive(ppr.at[n], p_send.at[n], p_recv.at[n], partner)
            total = (acc[n, rows_of(core), :] + ppr[n].astype(F32)).astype(BF)
            t, k, copy = owner_of(at)

            @pl.when(t == tp)
            def _():
                rsr[x, k, core] = total

            @pl.when(t != tp)
            def _():
                rss[n] = total
                copy.start()

    def arrivals(n, far):
        step = (2, 2) if far else (-1, 1)
        rows = [(step[d], ORDER[d][n]) for d in range(2)]
        columns = [(ORDER[d][n], step[d]) for d in range(2)]
        return [(0, rows), (1, columns)]

    own = [(0, [(0, 0), (0, 1)]), (0, [(0, -1), (0, 2)]), (1, [(0, 0), (1, 0)]), (1, [(-1, 0), (2, 0)])]
    ready = products(own)
    swap(ready)
    more = products(arrivals(0, False))
    swap(more)
    deliver(ready)
    ready = products(arrivals(1, False))
    swap(ready)
    deliver(more)
    second_near(DOWN, 2)
    more = products(arrivals(2, False))
    swap(more)
    deliver(ready)
    second_far(DOWN, 0)
    ready = products(arrivals(0, True))
    swap(ready)
    deliver(more)
    second_far(DOWN, 1)
    more = products(arrivals(1, True))
    swap(more)
    deliver(ready)
    second_near(DOWN, 3)
    ready = products(arrivals(3, False))
    swap(ready)
    deliver(more)
    deliver(ready)

    def from_chip(step, k, half):
        other = lax.rem(x + step, 4)
        arrive(rsr.at[other, k, half], r_send.at[0], r_recv.at[(other * 2 + k) * 2 + half], x_device(1))

    for k in range(2):
        from_chip(0, k, 1 - core)
        for step in range(1, 4):
            for half in range(2):
                from_chip(step, k, half)
    for k in range(2):
        for half in range(2):
            rows, columns = slice(192 * half, 192 * half + 192), slice(128 * k, 128 * k + 128)
            total = mid[tp, rows, columns].astype(F32)
            for chip in range(4):
                total = total + rsr[chip, k, half].astype(F32)
            out_ref[rows, columns] = total.astype(BF)
    for at in sorted(begun):
        t, _, copy = owner_of(at)
        pl.when(t != tp)(copy.wait_send)
    for copy in started:
        copy.wait_send()


def local(activations, norm_gain, qw, kw, vw, gw, ow, mlp_gain, uw, dw):
    cosine, sine = rotary_tables()
    operands = (
        activations, norm_gain.reshape(1, D), qw.T, kw.T, vw.T, gw.T, ow, mlp_gain.reshape(1, D), uw, dw,
        jnp.asarray(cosine), jnp.asarray(sine),
    )
    dma = pltpu.SemaphoreType.DMA
    return pl.pallas_call(
        layer_kernel,
        out_shape=jax.ShapeDtypeStruct((ROWS, D // 8), BF),
        in_specs=[pl.BlockSpec(memory_space=pltpu.HBM)] * len(operands),
        out_specs=pl.BlockSpec(memory_space=pltpu.VMEM),
        scratch_shapes=[
            pltpu.VMEM((2, 4, 4, 160, 128), BF),
            pltpu.VMEM((2, 4, 4, 128, 512), BF),
            pltpu.VMEM((2, 4, 4, 512, 128), BF),
            pltpu.VMEM((8, ROWS, 256), BF),
            pltpu.VMEM((8, 2, 4, 4, 32, 128), BF),
            pltpu.VMEM((8, 192, 128), BF),
            pltpu.VMEM((ROWS, D), BF),
            pltpu.VMEM((8, ROWS, 256), BF),
            pltpu.VMEM((ROWS, 1024), BF),
            pltpu.VMEM((16, 192, 128), BF),
            pltpu.VMEM((16, 192, 128), BF),
            pltpu.VMEM((16, 192, 128), BF),
            pltpu.VMEM((4, 2, 2, 192, 128), BF),
            pltpu.VMEM((4, 64, 128), BF),
            pltpu.VMEM((2, 1, D), F32),
            pltpu.VMEM((2, 128, 128), F32),
            pltpu.VMEM((ROWS, 256), F32),
            pltpu.VMEM((ROWS, 128), F32),
            pltpu.VMEM((ROWS, 512), BF),
            pltpu.VMEM((16, ROWS, 128), F32),
            dma((15,)), dma((36,)), dma((36,)), dma((72,)), dma((72,)), dma((42,)), dma((42,)), dma((16,)), dma((16,)), dma((16,)), dma((16,)),
        ],
        compiler_params=pltpu.CompilerParams(
            collective_id=0, has_side_effects=True, vmem_limit_bytes=56 * 1024 * 1024
        ),
        name="layer",
    )(*operands)


def solution(mesh):
    in_specs = (
        P(("rep", "fs"), "tp"), P(), P("fs", "tp"), P("fs", "tp"), P("fs", "tp"), P("fs", "tp"), P("tp", "fs"), P(),
        P("fs", "tp"), P("tp", "fs"),
    )
    return jax.shard_map(local, mesh=mesh, in_specs=in_specs, out_specs=P(("rep", "fs"), "tp"), check_vma=False)
```

```python
import numpy as np
import jax
import jax.numpy as jnp
from jax import lax
from jax.experimental import pallas as pl
from jax.experimental.pallas import tpu as pltpu
from jax.sharding import PartitionSpec as P

HEADS = 8
HEAD_DIM = 64
SEQ_LEN = 128
EPSILON = 1e-06
ROWS = 384
D = 2048
NX = 4
BF = jnp.bfloat16
F32 = jnp.float32
MESH = pl.DeviceIdType.MESH
ATTN, UP, DOWN = 0, 1, 2
ORDER = ((0, 1, -1, 2), (-1, 2, 0, 1))


def rotary_tables():
    half = HEAD_DIM // 2
    position = np.arange(SEQ_LEN, dtype=np.float32)
    freqs = np.float32(10000.0) ** (-np.arange(half, dtype=np.float32) / np.float32(half))
    angle = position[:, None] * freqs[None, :].astype(np.float32)
    cosine, sine = np.cos(angle), np.sin(angle)
    scale = np.float32(HEAD_DIM**-0.5)
    c = np.concatenate([cosine, cosine, cosine * scale, cosine * scale], axis=1)
    s = np.concatenate([-sine, sine, -sine * scale, sine * scale], axis=1)
    return c.astype(np.float32), s.astype(np.float32)


def log_gammas():
    head = np.arange(HEADS, dtype=np.float32)
    exponent = np.float32(5.0) + np.float32(4.0) * head / np.float32(HEADS - 1)
    return np.log(1.0 - np.power(2.0, -exponent.astype(np.float64)))


def lanes(shape):
    return lax.broadcasted_iota(jnp.int32, shape, len(shape) - 1)


def layer_kernel(
    act_hbm, ng_hbm, qw_hbm, kw_hbm, vw_hbm, gw_hbm, ow_hbm, mg_hbm, uw_hbm, dw_hbm, cos_hbm, sin_hbm,
    out_ref,
    attn, upb, dnb, xall, wo, ret, wide, mid, hid, pps, ppr, rss, rsr,
    small, gains, tables, qkvg, gat, lhs, acc,
    relay, local_sem, ring_send, first_recv, second_recv, x_send, x_recv, p_send, p_recv, r_send, r_recv, relay_recv,
):
    rep, fs, tp = lax.axis_index("rep"), lax.axis_index("fs"), lax.axis_index("tp")
    zl, y = lax.div(fs, 4), lax.rem(fs, 4)
    x, core = lax.div(tp, 2), lax.rem(tp, 2)
    zg = rep * 4 + zl

    def y_device(step):
        return {"fs": zl * 4 + lax.rem(y + step + 4, 4)}

    def z_device(step):
        other = lax.rem(zg + step + 8, 8)
        return {"rep": lax.div(other, 4), "fs": lax.rem(other, 4) * 4 + y}

    def x_index(step, c=core):
        return lax.rem(x + step + 4, 4) * 2 + c

    def x_device(step):
        return {"tp": x_index(step)}

    partner = {"tp": x * 2 + (1 - core)}

    barrier = pltpu.get_barrier_semaphore()
    peers = [y_device(1), y_device(-1), z_device(1), z_device(-1), partner]
    peers += [{"tp": x_index(step, c)} for step in (1, -1, 2) for c in range(2)]
    for peer in peers:
        pl.semaphore_signal(barrier, inc=1, device_id=peer, device_id_type=MESH)

    loads = [
        pltpu.make_async_copy(qw_hbm, small.at[0], local_sem.at[0]),
        pltpu.make_async_copy(kw_hbm, small.at[1], local_sem.at[1]),
        pltpu.make_async_copy(vw_hbm, small.at[2], local_sem.at[2]),
        pltpu.make_async_copy(gw_hbm, small.at[3], local_sem.at[3]),
        pltpu.make_async_copy(ow_hbm.at[pl.ds(0, 32)], attn.at[0, zl, y, pl.ds(128, 32)], local_sem.at[4]),
        pltpu.make_async_copy(ow_hbm.at[pl.ds(32, 32)], attn.at[1, zl, y, pl.ds(128, 32)], local_sem.at[5]),
        pltpu.make_async_copy(act_hbm, xall.at[tp], local_sem.at[6]),
        pltpu.make_async_copy(uw_hbm.at[:, pl.ds(0, 512)], upb.at[0, zl, y], local_sem.at[7]),
        pltpu.make_async_copy(uw_hbm.at[:, pl.ds(512, 512)], upb.at[1, zl, y], local_sem.at[8]),
        pltpu.make_async_copy(dw_hbm.at[pl.ds(0, 512)], dnb.at[0, zl, y], local_sem.at[9]),
        pltpu.make_async_copy(dw_hbm.at[pl.ds(512, 512)], dnb.at[1, zl, y], local_sem.at[10]),
        pltpu.make_async_copy(ng_hbm, gains.at[0], local_sem.at[11]),
        pltpu.make_async_copy(mg_hbm, gains.at[1], local_sem.at[12]),
        pltpu.make_async_copy(cos_hbm, tables.at[0], local_sem.at[13]),
        pltpu.make_async_copy(sin_hbm, tables.at[1], local_sem.at[14]),
    ]
    for copy in loads:
        copy.start()
    for copy in loads[:6]:
        copy.wait()
    for h in range(2):
        attn[h, zl, y, 0:128, :] = small[2 * h : 2 * h + 2].reshape(128, 128).astype(F32).T.astype(BF)
    pl.semaphore_wait(barrier, len(peers))

    def remote(src, dst, send_sem, recv_sem, device):
        return pltpu.make_async_remote_copy(
            src_ref=src, dst_ref=dst, send_sem=send_sem, recv_sem=recv_sem, device_id=device, device_id_type=MESH
        )

    def send(src, dst, send_sem, recv_sem, device):
        remote(src, dst, send_sem, recv_sem, device).start()

    def arrive(region, recv_sem):
        remote(region, region, r_send.at[0], recv_sem, partner).wait_recv()

    def sent(region, send_sem):
        remote(region, region, send_sem, r_recv.at[0], partner).wait_send()

    bufs = (attn, upb, dnb)
    depth = (160, 128, 512)

    def block(item, half, dz, dy):
        return bufs[item].at[half, lax.rem(zl + dz + 4, 4), lax.rem(y + dy + 4, 4)]

    def along_y(half, phase):
        return (half + phase) % 2 == 0

    def piece(item, half, step, p):
        cut = depth[item] // 2
        dz, dy = (0, step) if half == 0 else (step, 0)
        return block(item, half, dz, dy).at[pl.ds(p * cut, cut)]

    def ring_device(half, phase, step):
        return y_device(step) if along_y(half, phase) else z_device(step)

    def first_sem(item, half=2, d=0):
        return first_recv.at[item * 5 + half * 2 + d]

    def first_start(item):
        for n in range(2):
            for half in range(2):
                for d in range(2):
                    ref = piece(item, half, 0, n if d == 0 else 1 - n)
                    sem = first_sem(item, half, d) if n == 0 else first_sem(item)
                    send(ref, ref, ring_send.at[item], sem, ring_device(half, 0, 1 - 2 * d))

    def first_forward(item):
        for half in range(2):
            for d in range(2):
                to = 1 - 2 * d
                ref = piece(item, half, -to, d)
                arrive(ref, first_sem(item, half, d))
                send(ref, ref, ring_send.at[item], first_sem(item), ring_device(half, 0, to))

    def first_rest(item):
        arrive(bufs[item].at[0, 0], first_sem(item))

    def second_block(item, half, step, d, n):
        across = ORDER[d][n]
        return block(item, half, step, across) if half == 0 else block(item, half, across, step)

    def second_sem(item, half, d, n, far):
        if n < 2 and not far:
            return second_recv.at[item * 8 + half * 4 + d * 2 + n]
        if item < DOWN:
            return second_recv.at[24 + item]
        return second_recv.at[26 + n]

    def second_start(item, *which):
        for n in which:
            for half in range(2):
                for d in range(2):
                    ref = second_block(item, half, 0, d, n)
                    sem = second_sem(item, half, d, n, False)
                    send(ref, ref, ring_send.at[3 + item], sem, ring_device(half, 1, 1 - 2 * d))

    def second_forward(item, *which):
        for n in which:
            for half in range(2):
                for d in range(2):
                    to = 1 - 2 * d
                    ref = second_block(item, half, -to, d, n)
                    arrive(ref, second_sem(item, half, d, n, False))
                    sem = second_sem(item, half, d, n, True)
                    send(ref, ref, ring_send.at[3 + item], sem, ring_device(half, 1, to))

    def second_rest(item):
        arrive(bufs[item].at[0], second_sem(item, 0, 0, 0, True))

    def second_four(item, n, far):
        arrive(bufs[item].at[0, 0], second_sem(item, 0, 0, n, far))

    def x_piece(which, t, p):
        if which == 0:
            return xall.at[t, pl.ds(p * 192, 192)]
        if which == 1:
            return wo.at[t, p]
        return ret.at[t, pl.ds(p * 96, 96)]

    whole = (xall, wo, ret)

    def x_sem(which, kind):
        return x_recv.at[which * 5 + kind]

    def hand_over(which, place, p):
        ref = x_piece(which, x_index((0, -1, 1, 2)[place]), p)
        send(ref, ref, x_send.at[which], x_sem(which, 4), partner)

    def x_start(which):
        for n in range(2):
            for d in range(2):
                p = n if d == 0 else 1 - n
                dst = x_piece(which, tp, p)
                src = attn.at[p, :, :, pl.ds(128, 32)] if which == 1 else dst
                send(src, dst, x_send.at[which], x_sem(which, d if n == 0 else 2), x_device(1 - 2 * d))
        for p in range(2):
            dst = x_piece(which, tp, p)
            src = attn.at[p, :, :, pl.ds(128, 32)] if which == 1 else dst
            send(src, dst, x_send.at[which], x_sem(which, 4), partner)

    def x_forward(which):
        for d in range(2):
            to = 1 - 2 * d
            ref = x_piece(which, x_index(-to), d)
            arrive(ref, x_sem(which, d))
            send(ref, ref, x_send.at[which], x_sem(which, 3), x_device(to))
            hand_over(which, 1 + d, d)

    def x_near(which):
        arrive(whole[which].at[0], x_sem(which, 2))
        for d in range(2):
            hand_over(which, 1 + d, 1 - d)

    def x_far(which):
        arrive(whole[which].at[0], x_sem(which, 3))
        for d in range(2):
            hand_over(which, 3, d)

    def x_partner(which):
        arrive(whole[which].at[pl.ds(0, 4)], x_sem(which, 4))

    def norm_rows(source, gain):
        @pl.loop(0, ROWS // 16)
        def _(i):
            rows = pl.ds(pl.multiple_of(i * 16, 16), 16)
            blocks = [source[t, rows, :].astype(F32) for t in range(8)]
            squares = blocks[0] * blocks[0]
            for b in blocks[1:]:
                squares = squares + b * b
            scale = lax.rsqrt(jnp.sum(squares, axis=-1, keepdims=True) * (1.0 / D) + EPSILON)
            for t in range(8):
                columns = slice(256 * t, 256 * t + 256)
                wide[rows, columns] = (blocks[t] * scale * gains[gain, :, columns]).astype(BF)

    first_start(ATTN)
    loads[6].wait()
    x_start(0)
    loads[7].wait()
    loads[8].wait()
    first_start(UP)
    for copy in loads[9:]:
        copy.wait()
    first_forward(ATTN)
    x_forward(0)
    first_forward(UP)
    first_rest(ATTN)
    second_start(ATTN, 0, 1, 2, 3)
    x_near(0)
    second_forward(ATTN, 0, 1)
    first_start(DOWN)
    x_far(0)
    x_partner(0)
    norm_rows(xall, 0)
    first_rest(UP)
    second_start(UP, 0)
    second_rest(ATTN)
    x_start(1)
    first_forward(DOWN)
    second_start(UP, 1, 2, 3)

    weights = jnp.concatenate([attn[h, :, :, 0:128, :].reshape(D, 128) for h in range(2)], axis=1)
    qkvg[...] = jnp.dot(wide[...], weights, preferred_element_type=F32)
    log_gamma = jnp.float32(0.0)
    for h, value in enumerate(log_gammas()):
        log_gamma = jnp.where(tp == h, jnp.float32(value), log_gamma)
    square = (SEQ_LEN, SEQ_LEN)
    distance = (lax.broadcasted_iota(jnp.int32, square, 0) - lanes(square)).astype(F32)
    decay = jnp.where(distance >= 0, jnp.exp(jnp.maximum(distance, 0.0) * log_gamma), 0.0)
    lane = lanes(square)
    first, low = lax.rem(lane, 64) < 32, lane < 64
    for s in range(3):
        rows = slice(SEQ_LEN * s, SEQ_LEN * (s + 1))
        qk, vg = qkvg[rows, 0:128], qkvg[rows, 128:256]
        other = jnp.where(first, pltpu.roll(qk, 96, 1), pltpu.roll(qk, 32, 1))
        turned = (qk * tables[0] + other * tables[1]).astype(BF).astype(F32)
        queries = jnp.where(low, turned, 0.0).astype(BF)
        keys = pltpu.roll(turned, 64, 1).astype(BF)
        scores = lax.dot_general(queries, keys, (((1,), (1,)), ((), ())), preferred_element_type=F32)
        mixed = jnp.dot((scores * decay).astype(BF), vg.astype(BF), preferred_element_type=F32)
        mixed = jnp.where(low, mixed, 0.0)
        mean = jnp.sum(mixed, axis=-1, keepdims=True) * (1.0 / HEAD_DIM)
        centred = jnp.where(low, mixed - mean, 0.0)
        variance = jnp.sum(centred * centred, axis=-1, keepdims=True) * (1.0 / HEAD_DIM)
        gate = pltpu.roll(vg, 64, 1)
        gat[rows, :] = centred * lax.rsqrt(variance + EPSILON) * (gate / (1.0 + jnp.exp(-gate)))
    low = lanes((192, 128)) < 64
    ret[tp] = jnp.where(low, gat[0:192, :], pltpu.roll(gat[192:384, :], 64, 1)).astype(BF)
    x_start(2)
    for h in range(2):
        wo[tp, h] = attn[h, :, :, 128:160, :]
    x_forward(1)
    x_forward(2)
    x_near(2)
    x_near(1)
    x_far(2)
    second_forward(UP, 0, 1)
    x_far(1)
    first_rest(DOWN)
    second_start(DOWN, 0, 1)
    x_partner(2)
    x_partner(1)

    for j in range(4):
        a, b = ret[2 * j].astype(F32), ret[2 * j + 1].astype(F32)
        lhs[0:192, 128 * j : 128 * j + 128] = jnp.where(low, a, pltpu.roll(b, 64, 1)).astype(BF)
        lhs[192:384, 128 * j : 128 * j + 128] = jnp.where(low, pltpu.roll(a, 64, 1), b).astype(BF)

    @pl.loop(0, 8)
    def _(t):
        z0, y0 = lax.div(t, 2), lax.rem(t, 2) * 2
        columns = [wo[:, :, z0, y0 + k].reshape(HEADS * HEAD_DIM, 128) for k in range(2)]
        branch = jnp.dot(lhs[...], jnp.concatenate(columns, axis=1), preferred_element_type=F32)
        mid[t] = (xall[t].astype(F32) + branch).astype(BF)

    norm_rows(mid, 1)
    second_rest(UP)
    for h in range(2):
        raw = jnp.dot(wide[...], upb[h].reshape(D, 512), preferred_element_type=F32)
        raw = jnp.maximum(raw, 0.0)
        hid[:, 512 * h : 512 * h + 512] = (raw * raw).astype(BF)
    second_forward(DOWN, 0)

    def number(dz, dy):
        return (dz + 1) * 4 + dy + 1

    begun = set()

    def products(pairs):
        done = []
        for half, blocks in pairs:
            columns = jnp.concatenate([block(DOWN, half, dz, dy)[...] for dz, dy in blocks], axis=1)
            both = jnp.dot(hid[:, 512 * half : 512 * half + 512], columns, preferred_element_type=F32)
            for k, at in enumerate(blocks):
                value, n = both[:, 128 * k : 128 * k + 128], number(*at)
                if at in begun:
                    acc[n] += value
                    done.append(at)
                else:
                    acc[n] = value
                    begun.add(at)
        return done

    def rows_of(c):
        return pl.ds(pl.multiple_of(c * 192, 64), 192)

    def swap(blocks, group):
        for at in blocks:
            n = number(*at)
            pps[n] = acc[n, rows_of(1 - core), :].astype(BF)
            send(pps.at[n], ppr.at[n], p_send.at[0], p_recv.at[group], partner)

    way = 1 - 2 * core

    def route(at):
        z_to, y_to = lax.rem(zl + at[0] + 4, 4), lax.rem(y + at[1] + 4, 4)
        c_to, k = lax.div(y_to, 2), lax.rem(y_to, 2)
        hops = lax.rem(way * (z_to - x) + 8, 4)
        return number(*at), {"tp": z_to * 2 + c_to}, c_to, k, hops

    def deliver(blocks, group):
        arrive(ppr.at[pl.ds(0, len(blocks))], p_recv.at[group])
        for at in blocks:
            n, owner, c_to, k, hops = route(at)
            total = (acc[n, rows_of(core), :] + ppr[n].astype(F32)).astype(BF)
            rss[n] = total

            if group < 5:

                @pl.when(hops == 2)
                def _():
                    send(rss.at[n], relay.at[at[1] + 1], r_send.at[0], relay_recv.at[at[1] + 1], x_device(way))

                @pl.when((hops == 3) | ((hops == 0) & (c_to != core)))
                def _():
                    send(rss.at[n], rsr.at[hops, k, core], r_send.at[0], r_recv.at[0], owner)

            else:

                @pl.when(hops == 2)
                def _():
                    send(rss.at[n], rsr.at[2, k, core], r_send.at[0], r_recv.at[1 + k], owner)

                @pl.when((hops % 2 == 1) | ((hops == 0) & (c_to != core)))
                def _():
                    send(rss.at[n], rsr.at[hops, k, core], r_send.at[0], r_recv.at[0], owner)

            @pl.when((hops == 0) & (c_to == core))
            def _():
                rsr[0, k, core] = total

    def pass_on(blocks):
        for at in blocks:
            n, owner, _, k, hops = route(at)

            @pl.when(hops == 1)
            def _():
                arrive(relay.at[at[1] + 1], relay_recv.at[at[1] + 1])
                total = acc[n, rows_of(core), :] + ppr[n].astype(F32) + relay[at[1] + 1].astype(F32)
                rss[n] = total.astype(BF)
                send(rss.at[n], rsr.at[1, k, core], r_send.at[0], r_recv.at[0], owner)

    def arrivals(n, far):
        step = (2, 2) if far else (-1, 1)
        rows = [(step[d], ORDER[d][n]) for d in range(2)]
        columns = [(ORDER[d][n], step[d]) for d in range(2)]
        return [(0, rows), (1, columns)]

    own = [(0, [(0, 0), (0, 1)]), (0, [(0, -1), (0, 2)]), (1, [(0, 0), (1, 0)]), (1, [(-1, 0), (2, 0)])]
    s0 = products(own)
    swap(s0, 0)
    s1 = products(arrivals(0, False))
    swap(s1, 1)
    deliver(s0, 0)
    second_forward(DOWN, 1)
    second_start(DOWN, 2, 3)
    s2 = products(arrivals(1, False))
    swap(s2, 2)
    deliver(s1, 1)
    deliver(s2, 2)
    second_four(DOWN, 0, True)
    s3 = products(arrivals(0, True))
    swap(s3, 3)
    pass_on(s0)
    deliver(s3, 3)
    second_four(DOWN, 1, True)
    s4 = products(arrivals(1, True))
    swap(s4, 4)
    pass_on(s1)
    pass_on(s2)
    deliver(s4, 4)
    second_four(DOWN, 2, False)
    s5 = products(arrivals(2, False))
    swap(s5, 5)
    pass_on(s3)
    deliver(s5, 5)
    second_four(DOWN, 3, False)
    s6 = products(arrivals(3, False))
    swap(s6, 6)
    deliver(s6, 6)
    pass_on(s4)

    def straight(k):
        dz, dy = lax.rem(x - zl + 4, 4), lax.rem(core * 2 + k - y + 4, 4)
        found = (dz == 0) & (dy < 0)
        for at in s5 + s6:
            found = found | ((dz == at[0] % 4) & (dy == at[1] % 4))
        return found

    for k in range(2):

        @pl.when(jnp.logical_not(straight(k)))
        def _():
            rsr[2, k] = jnp.zeros((2, 192, 128), BF)

    def collect():
        arrive(rss.at[pl.ds(0, 10)], r_recv.at[0])
        for k in range(2):

            @pl.when(straight(k))
            def _():
                arrive(rss.at[pl.ds(0, 2)], r_recv.at[1 + k])

    def finish():
        for k in range(2):
            for half in range(2):
                rows, columns = slice(192 * half, 192 * half + 192), slice(128 * k, 128 * k + 128)
                total = mid[tp, rows, columns].astype(F32)
                for hops in range(4):
                    total = total + rsr[hops, k, half].astype(F32)
                out_ref[rows, columns] = total.astype(BF)

    def drain():
        for item in range(3):
            sent(bufs[item].at[:, pl.ds(0, 3), 0], ring_send.at[item])
            sent(bufs[item].at[:, pl.ds(0, 3)], ring_send.at[3 + item])
        for which in range(3):
            sent(whole[which].at[pl.ds(0, 7)], x_send.at[which])
        sent(pps, p_send.at[0])
        sent(rss.at[pl.ds(0, 14)], r_send.at[0])

    collect()
    finish()
    drain()


def local(activations, norm_gain, qw, kw, vw, gw, ow, mlp_gain, uw, dw):
    cosine, sine = rotary_tables()
    operands = (
        activations, norm_gain.reshape(1, D), qw.T, kw.T, vw.T, gw.T, ow, mlp_gain.reshape(1, D), uw, dw,
        jnp.asarray(cosine), jnp.asarray(sine),
    )
    dma = pltpu.SemaphoreType.DMA
    rows = pl.pallas_call(
        layer_kernel,
        out_shape=pltpu.VMEM((ROWS, D // 8), BF),
        in_specs=[pl.BlockSpec(memory_space=pltpu.HBM)] * len(operands),
        out_specs=pl.BlockSpec(memory_space=pltpu.VMEM),
        scratch_shapes=[
            pltpu.VMEM((2, 4, 4, 160, 128), BF),
            pltpu.VMEM((2, 4, 4, 128, 512), BF),
            pltpu.VMEM((2, 4, 4, 512, 128), BF),
            pltpu.VMEM((8, ROWS, 256), BF),
            pltpu.VMEM((8, 2, 4, 4, 32, 128), BF),
            pltpu.VMEM((8, 192, 128), BF),
            pltpu.VMEM((ROWS, D), BF),
            pltpu.VMEM((8, ROWS, 256), BF),
            pltpu.VMEM((ROWS, 1024), BF),
            pltpu.VMEM((16, 192, 128), BF),
            pltpu.VMEM((16, 192, 128), BF),
            pltpu.VMEM((16, 192, 128), BF),
            pltpu.VMEM((4, 2, 2, 192, 128), BF),
            pltpu.VMEM((4, 64, 128), BF),
            pltpu.VMEM((2, 1, D), F32),
            pltpu.VMEM((2, 128, 128), F32),
            pltpu.VMEM((ROWS, 256), F32),
            pltpu.VMEM((ROWS, 128), F32),
            pltpu.VMEM((ROWS, 512), BF),
            pltpu.VMEM((16, ROWS, 128), F32),
            pltpu.VMEM((4, 192, 128), BF),
            dma((15,)), dma((6,)), dma((15,)), dma((30,)), dma((3,)), dma((15,)), dma((1,)), dma((7,)), dma((1,)), dma((3,)), dma((4,)),
        ],
        compiler_params=pltpu.CompilerParams(
            collective_id=0, has_side_effects=True, vmem_limit_bytes=56 * 1024 * 1024
        ),
        name="layer",
    )(*operands)
    return rows


def solution(mesh):
    in_specs = (
        P(("rep", "fs"), "tp"), P(), P("fs", "tp"), P("fs", "tp"), P("fs", "tp"), P("fs", "tp"), P("tp", "fs"), P(),
        P("fs", "tp"), P("tp", "fs"),
    )
    return jax.shard_map(local, mesh=mesh, in_specs=in_specs, out_specs=P(("rep", "fs"), "tp"), check_vma=False)
```

```python
import numpy as np
import jax
import jax.numpy as jnp
from jax import lax
from jax.experimental import pallas as pl
from jax.experimental.pallas import tpu as pltpu
from jax.sharding import PartitionSpec as P

HEADS = 8
HEAD_DIM = 64
SEQ_LEN = 128
EPSILON = 1e-06
ROWS = 384
D = 2048
NX = 4
BF = jnp.bfloat16
F32 = jnp.float32
MESH = pl.DeviceIdType.MESH
ATTN, UP, DOWN = 0, 1, 2
ORDER = ((0, 1, 2, -1), (-1, 2, 0, 1))


def rotary_tables():
    half = HEAD_DIM // 2
    position = np.arange(SEQ_LEN, dtype=np.float32)
    freqs = np.float32(10000.0) ** (-np.arange(half, dtype=np.float32) / np.float32(half))
    angle = position[:, None] * freqs[None, :].astype(np.float32)
    cosine, sine = np.cos(angle), np.sin(angle)
    scale = np.float32(HEAD_DIM**-0.5)
    c = np.concatenate([cosine, cosine, cosine * scale, cosine * scale], axis=1)
    s = np.concatenate([-sine, sine, -sine * scale, sine * scale], axis=1)
    return c.astype(np.float32), s.astype(np.float32)


def log_gammas():
    head = np.arange(HEADS, dtype=np.float32)
    exponent = np.float32(5.0) + np.float32(4.0) * head / np.float32(HEADS - 1)
    return np.log(1.0 - np.power(2.0, -exponent.astype(np.float64)))


def lanes(shape):
    return lax.broadcasted_iota(jnp.int32, shape, len(shape) - 1)


def layer_kernel(
    act_hbm, ng_hbm, qw_hbm, kw_hbm, vw_hbm, gw_hbm, ow_hbm, mg_hbm, uw_hbm, dw_hbm, cos_hbm, sin_hbm,
    out_ref,
    attn, upb, dnb, xall, wo, ret, wide, mid, hid, pps, ppr, rss, rsr,
    small, gains, tables, qkvg, gat, lhs, acc,
    local_sem, ring_send, first_recv, second_recv, x_send, x_recv, p_send, p_recv, r_send, r_recv,
):
    rep, fs, tp = lax.axis_index("rep"), lax.axis_index("fs"), lax.axis_index("tp")
    zl, y = lax.div(fs, 4), lax.rem(fs, 4)
    x, core = lax.div(tp, 2), lax.rem(tp, 2)
    zg = rep * 4 + zl

    def y_device(step):
        return {"fs": zl * 4 + lax.rem(y + step + 4, 4)}

    def z_device(step):
        other = lax.rem(zg + step + 8, 8)
        return {"rep": lax.div(other, 4), "fs": lax.rem(other, 4) * 4 + y}

    def x_index(step, c=core):
        return lax.rem(x + step + 4, 4) * 2 + c

    def x_device(step):
        return {"tp": x_index(step)}

    partner = {"tp": x * 2 + (1 - core)}

    barrier = pltpu.get_barrier_semaphore()
    peers = [y_device(1), y_device(-1), z_device(1), z_device(-1), partner]
    peers += [{"tp": x_index(step, c)} for step in (1, -1, 2) for c in range(2)]
    for peer in peers:
        pl.semaphore_signal(barrier, inc=1, device_id=peer, device_id_type=MESH)

    loads = (
        (qw_hbm, small.at[0], 0),
        (kw_hbm, small.at[1], 0),
        (vw_hbm, small.at[2], 0),
        (gw_hbm, small.at[3], 0),
        (ow_hbm.at[pl.ds(0, 32)], attn.at[0, zl, y, pl.ds(128, 32)], 1),
        (ow_hbm.at[pl.ds(32, 32)], attn.at[1, zl, y, pl.ds(128, 32)], 1),
        (act_hbm, xall.at[tp], 2),
        (uw_hbm.at[:, pl.ds(0, 512)], upb.at[0, zl, y], 3),
        (uw_hbm.at[:, pl.ds(512, 512)], upb.at[1, zl, y], 3),
        (dw_hbm.at[pl.ds(0, 512)], dnb.at[0, zl, y], 4),
        (dw_hbm.at[pl.ds(512, 512)], dnb.at[1, zl, y], 4),
        (ng_hbm, gains.at[0], 5),
        (mg_hbm, gains.at[1], 5),
        (cos_hbm, tables.at[0], 6),
        (sin_hbm, tables.at[1], 6),
    )
    for src, dst, n in loads:
        pltpu.make_async_copy(src, dst, local_sem.at[n]).start()

    def loaded(region, n):
        pltpu.make_async_copy(region, region, local_sem.at[n]).wait()

    loaded(small, 0)
    loaded(attn.at[0, 0, 0, pl.ds(0, 64)], 1)
    for h in range(2):
        attn[h, zl, y, 0:128, :] = small[2 * h : 2 * h + 2].reshape(128, 128).astype(F32).T.astype(BF)
    pl.semaphore_wait(barrier, len(peers))

    def remote(src, dst, send_sem, recv_sem, device):
        return pltpu.make_async_remote_copy(
            src_ref=src, dst_ref=dst, send_sem=send_sem, recv_sem=recv_sem, device_id=device, device_id_type=MESH
        )

    def send(src, dst, send_sem, recv_sem, device):
        remote(src, dst, send_sem, recv_sem, device).start()

    def arrive(region, recv_sem):
        remote(region, region, r_send.at[0], recv_sem, partner).wait_recv()

    def sent(region, send_sem):
        remote(region, region, send_sem, r_recv.at[0], partner).wait_send()

    bufs = (attn, upb, dnb)
    depth = (160, 128, 512)

    def block(item, half, dz, dy):
        return bufs[item].at[half, lax.rem(zl + dz + 4, 4), lax.rem(y + dy + 4, 4)]

    def along_y(half, phase):
        return (half + phase) % 2 == 0

    def piece(item, half, step, p):
        cut = depth[item] // 2
        dz, dy = (0, step) if half == 0 else (step, 0)
        return block(item, half, dz, dy).at[pl.ds(p * cut, cut)]

    def ring_device(half, phase, step):
        return y_device(step) if along_y(half, phase) else z_device(step)

    def first_start(item):
        for n in range(2):
            for half in range(2):
                for d in range(2):
                    ref = piece(item, half, 0, n if d == 0 else 1 - n)
                    send(ref, ref, ring_send.at[item], first_recv.at[2 * item + n], ring_device(half, 0, 1 - 2 * d))

    def first_forward(item):
        arrive(bufs[item].at[0, 0, pl.ds(0, 2)], first_recv.at[2 * item])
        for half in range(2):
            for d in range(2):
                to = 1 - 2 * d
                ref = piece(item, half, -to, d)
                send(ref, ref, ring_send.at[item], first_recv.at[2 * item + 1], ring_device(half, 0, to))

    def first_rest(item):
        arrive(bufs[item].at[0, 0], first_recv.at[2 * item + 1])

    def second_block(item, half, step, d, n):
        across = ORDER[d][n]
        return block(item, half, step, across) if half == 0 else block(item, half, across, step)

    def second_sem(item, n, far):
        if n < 2 and not far:
            return second_recv.at[2 * item + n]
        return second_recv.at[6 + item] if item < DOWN else second_recv.at[8 + n]

    def second_start(item, *which):
        for n in which:
            for half in range(2):
                for d in range(2):
                    ref = second_block(item, half, 0, d, n)
                    send(ref, ref, ring_send.at[3 + item], second_sem(item, n, False), ring_device(half, 1, 1 - 2 * d))

    def second_forward(item, *which):
        for n in which:
            arrive(bufs[item].at[0, 0], second_sem(item, n, False))
            for half in range(2):
                for d in range(2):
                    to = 1 - 2 * d
                    ref = second_block(item, half, -to, d, n)
                    send(ref, ref, ring_send.at[3 + item], second_sem(item, n, True), ring_device(half, 1, to))

    def second_rest(item):
        arrive(bufs[item].at[0], second_sem(item, 0, True))

    def second_four(item, n, far):
        arrive(bufs[item].at[0, 0], second_sem(item, n, far))

    def x_piece(which, t, p):
        if which == 0:
            return xall.at[t, pl.ds(p * 192, 192)]
        if which == 1:
            return wo.at[t, p]
        return ret.at[t, pl.ds(p * 96, 96)]

    whole = (xall, wo, ret)

    def x_sem(which, kind):
        return x_recv.at[which * 4 + kind]

    def hand_over(which, place, p):
        ref = x_piece(which, x_index((0, -1, 1, 2)[place]), p)
        send(ref, ref, x_send.at[which], x_sem(which, 3), partner)

    def x_start(which):
        for n in range(2):
            for d in range(2):
                p = n if d == 0 else 1 - n
                dst = x_piece(which, tp, p)
                src = attn.at[p, :, :, pl.ds(128, 32)] if which == 1 else dst
                send(src, dst, x_send.at[which], x_sem(which, n), x_device(1 - 2 * d))
        for p in range(2):
            dst = x_piece(which, tp, p)
            src = attn.at[p, :, :, pl.ds(128, 32)] if which == 1 else dst
            send(src, dst, x_send.at[which], x_sem(which, 3), partner)

    def x_forward(which):
        arrive(whole[which].at[0], x_sem(which, 0))
        for d in range(2):
            to = 1 - 2 * d
            ref = x_piece(which, x_index(-to), d)
            send(ref, ref, x_send.at[which], x_sem(which, 2), x_device(to))
            hand_over(which, 1 + d, d)

    def x_near(which):
        arrive(whole[which].at[0], x_sem(which, 1))
        for d in range(2):
            hand_over(which, 1 + d, 1 - d)

    def x_far(which):
        arrive(whole[which].at[0], x_sem(which, 2))
        for d in range(2):
            hand_over(which, 3, d)

    def x_partner(which):
        arrive(whole[which].at[pl.ds(0, 4)], x_sem(which, 3))

    def norm_rows(source, gain):
        @pl.loop(0, ROWS // 16)
        def _(i):
            rows = pl.ds(pl.multiple_of(i * 16, 16), 16)
            blocks = [source[t, rows, :].astype(F32) for t in range(8)]
            squares = blocks[0] * blocks[0]
            for b in blocks[1:]:
                squares = squares + b * b
            scale = lax.rsqrt(jnp.sum(squares, axis=-1, keepdims=True) * (1.0 / D) + EPSILON)
            for t in range(8):
                columns = slice(256 * t, 256 * t + 256)
                wide[rows, columns] = (blocks[t] * scale * gains[gain, :, columns]).astype(BF)

    first_start(ATTN)
    loaded(xall.at[0], 2)
    x_start(0)
    loaded(upb.at[0, 0, pl.ds(0, 2)], 3)
    first_start(UP)
    loaded(dnb.at[0, 0, pl.ds(0, 2)], 4)
    loaded(gains, 5)
    loaded(tables, 6)
    first_forward(ATTN)
    first_forward(UP)
    x_forward(0)
    first_rest(ATTN)
    second_start(ATTN, 0, 1, 2, 3)
    first_start(DOWN)
    x_near(0)
    second_forward(ATTN, 0, 1)
    x_far(0)
    x_partner(0)
    norm_rows(xall, 0)
    first_rest(UP)
    second_start(UP, 0)
    second_rest(ATTN)
    x_start(1)
    first_forward(DOWN)
    second_start(UP, 1, 2, 3)

    weights = jnp.concatenate([attn[h, :, :, 0:128, :].reshape(D, 128) for h in range(2)], axis=1)
    qkvg[...] = jnp.dot(wide[...], weights, preferred_element_type=F32)
    log_gamma = jnp.float32(0.0)
    for h, value in enumerate(log_gammas()):
        log_gamma = jnp.where(tp == h, jnp.float32(value), log_gamma)
    square = (SEQ_LEN, SEQ_LEN)
    distance = (lax.broadcasted_iota(jnp.int32, square, 0) - lanes(square)).astype(F32)
    decay = jnp.where(distance >= 0, jnp.exp(jnp.maximum(distance, 0.0) * log_gamma), 0.0)
    lane = lanes(square)
    first, low = lax.rem(lane, 64) < 32, lane < 64
    for s in range(3):
        rows = slice(SEQ_LEN * s, SEQ_LEN * (s + 1))
        qk, vg = qkvg[rows, 0:128], qkvg[rows, 128:256]
        other = jnp.where(first, pltpu.roll(qk, 96, 1), pltpu.roll(qk, 32, 1))
        turned = (qk * tables[0] + other * tables[1]).astype(BF).astype(F32)
        queries = jnp.where(low, turned, 0.0).astype(BF)
        keys = pltpu.roll(turned, 64, 1).astype(BF)
        scores = lax.dot_general(queries, keys, (((1,), (1,)), ((), ())), preferred_element_type=F32)
        mixed = jnp.dot((scores * decay).astype(BF), vg.astype(BF), preferred_element_type=F32)
        mixed = jnp.where(low, mixed, 0.0)
        mean = jnp.sum(mixed, axis=-1, keepdims=True) * (1.0 / HEAD_DIM)
        centred = jnp.where(low, mixed - mean, 0.0)
        variance = jnp.sum(centred * centred, axis=-1, keepdims=True) * (1.0 / HEAD_DIM)
        gate = pltpu.roll(vg, 64, 1)
        gat[rows, :] = centred * lax.rsqrt(variance + EPSILON) * (gate / (1.0 + jnp.exp(-gate)))
    low = lanes((192, 128)) < 64
    ret[tp] = jnp.where(low, gat[0:192, :], pltpu.roll(gat[192:384, :], 64, 1)).astype(BF)
    x_start(2)
    for h in range(2):
        wo[tp, h] = attn[h, :, :, 128:160, :]
    x_forward(1)
    x_forward(2)
    x_near(2)
    x_near(1)
    x_far(2)
    second_forward(UP, 0, 1)
    x_far(1)
    first_rest(DOWN)
    second_start(DOWN, 0, 1)
    x_partner(2)
    x_partner(1)

    for j in range(4):
        a, b = ret[2 * j].astype(F32), ret[2 * j + 1].astype(F32)
        lhs[0:192, 128 * j : 128 * j + 128] = jnp.where(low, a, pltpu.roll(b, 64, 1)).astype(BF)
        lhs[192:384, 128 * j : 128 * j + 128] = jnp.where(low, pltpu.roll(a, 64, 1), b).astype(BF)

    @pl.loop(0, 8)
    def _(t):
        z0, y0 = lax.div(t, 2), lax.rem(t, 2) * 2
        columns = [wo[:, :, z0, y0 + k].reshape(HEADS * HEAD_DIM, 128) for k in range(2)]
        branch = jnp.dot(lhs[...], jnp.concatenate(columns, axis=1), preferred_element_type=F32)
        mid[t] = (xall[t].astype(F32) + branch).astype(BF)

    norm_rows(mid, 1)
    second_rest(UP)
    for h in range(2):
        raw = jnp.dot(wide[...], upb[h].reshape(D, 512), preferred_element_type=F32)
        raw = jnp.maximum(raw, 0.0)
        hid[:, 512 * h : 512 * h + 512] = (raw * raw).astype(BF)
    second_forward(DOWN, 0)

    def number(dz, dy):
        return (dz + 1) * 4 + dy + 1

    begun = set()

    def products(pairs):
        done = []
        for half, blocks in pairs:
            columns = jnp.concatenate([block(DOWN, half, dz, dy)[...] for dz, dy in blocks], axis=1)
            both = jnp.dot(hid[:, 512 * half : 512 * half + 512], columns, preferred_element_type=F32)
            for k, at in enumerate(blocks):
                value, n = both[:, 128 * k : 128 * k + 128], number(*at)
                if at in begun:
                    acc[n] += value
                    done.append(at)
                else:
                    acc[n] = value
                    begun.add(at)
        return done

    def rows_of(c):
        return pl.ds(pl.multiple_of(c * 192, 64), 192)

    def swap(blocks, group):
        for at in blocks:
            n = number(*at)
            pps[n] = acc[n, rows_of(1 - core), :].astype(BF)
            send(pps.at[n], ppr.at[n], p_send.at[0], p_recv.at[group], partner)


    def route(at):
        z_to, y_to = lax.rem(zl + at[0] + 4, 4), lax.rem(y + at[1] + 4, 4)
        c_to, k = lax.div(y_to, 2), lax.rem(y_to, 2)
        hops = lax.rem(z_to - x + 4, 4)
        return number(*at), {"tp": z_to * 2 + c_to}, c_to, k, hops

    def deliver(blocks, group):
        arrive(ppr.at[pl.ds(0, len(blocks))], p_recv.at[group])
        for at in blocks:
            n, owner, c_to, k, hops = route(at)
            total = (acc[n, rows_of(core), :] + ppr[n].astype(F32)).astype(BF)
            rss[n] = total

            @pl.when((hops > 0) | (c_to != core))
            def _():
                send(rss.at[n], rsr.at[hops, k, core], r_send.at[0], r_recv.at[0], owner)

            @pl.when((hops == 0) & (c_to == core))
            def _():
                rsr[0, k, core] = total

    def arrivals(n, far):
        step = (2, 2) if far else (-1, 1)
        rows = [(step[d], ORDER[d][n]) for d in range(2)]
        columns = [(ORDER[d][n], step[d]) for d in range(2)]
        return [(0, rows), (1, columns)]

    own = [(0, [(0, 0), (0, 1)]), (0, [(0, -1), (0, 2)]), (1, [(0, 0), (1, 0)]), (1, [(-1, 0), (2, 0)])]
    def deliver_on(c, blocks, group):
        @pl.when(core == c)
        def _():
            deliver(blocks, group)

    s0 = products(own)
    swap(s0, 0)
    s1 = products(arrivals(0, False))
    swap(s1, 1)
    deliver(s0, 0)
    second_forward(DOWN, 1)
    second_start(DOWN, 2, 3)
    s2 = products(arrivals(1, False))
    swap(s2, 2)
    deliver(s1, 1)
    deliver_on(0, s2, 2)
    second_four(DOWN, 0, True)
    s3 = products(arrivals(0, True))
    swap(s3, 3)
    deliver_on(1, s2, 2)
    deliver_on(0, s3, 3)
    second_four(DOWN, 1, True)
    s4 = products(arrivals(1, True))
    swap(s4, 4)
    deliver_on(1, s3, 3)
    deliver_on(0, s4, 4)
    second_four(DOWN, 2, False)
    s5 = products(arrivals(2, False))
    swap(s5, 5)
    deliver_on(1, s4, 4)
    deliver(s5, 5)
    second_four(DOWN, 3, False)
    s6 = products(arrivals(3, False))
    swap(s6, 6)
    deliver(s6, 6)

    def collect():
        arrive(rss.at[pl.ds(0, 14)], r_recv.at[0])

    def finish():
        for k in range(2):
            for half in range(2):
                rows, columns = slice(192 * half, 192 * half + 192), slice(128 * k, 128 * k + 128)
                total = mid[tp, rows, columns].astype(F32)
                for hops in range(4):
                    total = total + rsr[hops, k, half].astype(F32)
                out_ref[rows, columns] = total.astype(BF)

    def drain():
        for item in range(3):
            sent(bufs[item].at[:, pl.ds(0, 3), 0], ring_send.at[item])
            sent(bufs[item].at[:, pl.ds(0, 3)], ring_send.at[3 + item])
        for which in range(3):
            sent(whole[which].at[pl.ds(0, 7)], x_send.at[which])
        sent(pps, p_send.at[0])
        sent(rss.at[pl.ds(0, 14)], r_send.at[0])

    collect()
    finish()
    drain()


def local(activations, norm_gain, qw, kw, vw, gw, ow, mlp_gain, uw, dw):
    cosine, sine = rotary_tables()
    operands = (
        activations, norm_gain.reshape(1, D), qw.T, kw.T, vw.T, gw.T, ow, mlp_gain.reshape(1, D), uw, dw,
        jnp.asarray(cosine), jnp.asarray(sine),
    )
    dma = pltpu.SemaphoreType.DMA
    rows = pl.pallas_call(
        layer_kernel,
        out_shape=pltpu.VMEM((ROWS, D // 8), BF),
        in_specs=[pl.BlockSpec(memory_space=pltpu.HBM)] * len(operands),
        out_specs=pl.BlockSpec(memory_space=pltpu.VMEM),
        scratch_shapes=[
            pltpu.VMEM((2, 4, 4, 160, 128), BF),
            pltpu.VMEM((2, 4, 4, 128, 512), BF),
            pltpu.VMEM((2, 4, 4, 512, 128), BF),
            pltpu.VMEM((8, ROWS, 256), BF),
            pltpu.VMEM((8, 2, 4, 4, 32, 128), BF),
            pltpu.VMEM((8, 192, 128), BF),
            pltpu.VMEM((ROWS, D), BF),
            pltpu.VMEM((8, ROWS, 256), BF),
            pltpu.VMEM((ROWS, 1024), BF),
            pltpu.VMEM((16, 192, 128), BF),
            pltpu.VMEM((16, 192, 128), BF),
            pltpu.VMEM((16, 192, 128), BF),
            pltpu.VMEM((4, 2, 2, 192, 128), BF),
            pltpu.VMEM((4, 64, 128), BF),
            pltpu.VMEM((2, 1, D), F32),
            pltpu.VMEM((2, 128, 128), F32),
            pltpu.VMEM((ROWS, 256), F32),
            pltpu.VMEM((ROWS, 128), F32),
            pltpu.VMEM((ROWS, 512), BF),
            pltpu.VMEM((16, ROWS, 128), F32),
            dma((7,)), dma((6,)), dma((6,)), dma((12,)), dma((3,)), dma((12,)), dma((1,)), dma((7,)), dma((1,)), dma((1,)),
        ],
        compiler_params=pltpu.CompilerParams(
            collective_id=0, has_side_effects=True, vmem_limit_bytes=56 * 1024 * 1024
        ),
        name="layer",
    )(*operands)
    return rows


def solution(mesh):
    in_specs = (
        P(("rep", "fs"), "tp"), P(), P("fs", "tp"), P("fs", "tp"), P("fs", "tp"), P("fs", "tp"), P("tp", "fs"), P(),
        P("fs", "tp"), P("tp", "fs"),
    )
    return jax.shard_map(local, mesh=mesh, in_specs=in_specs, out_specs=P(("rep", "fs"), "tp"), check_vma=False)
```

```python
import numpy as np
import jax
import jax.numpy as jnp
from jax import lax
from jax.experimental import pallas as pl
from jax.experimental.pallas import tpu as pltpu
from jax.sharding import PartitionSpec as P

HEADS = 8
HEAD_DIM = 64
SEQ_LEN = 128
EPSILON = 1e-06
ROWS = 384
D = 2048
NX = 4
BF = jnp.bfloat16
F32 = jnp.float32
MESH = pl.DeviceIdType.MESH
ATTN, UP, DOWN = 0, 1, 2
ORDER = ((0, 1, 2, -1), (-1, 2, 0, 1))


def rotary_tables():
    half = HEAD_DIM // 2
    position = np.arange(SEQ_LEN, dtype=np.float32)
    freqs = np.float32(10000.0) ** (-np.arange(half, dtype=np.float32) / np.float32(half))
    angle = position[:, None] * freqs[None, :].astype(np.float32)
    cosine, sine = np.cos(angle), np.sin(angle)
    scale = np.float32(HEAD_DIM**-0.5)
    c = np.concatenate([cosine, cosine, cosine * scale, cosine * scale], axis=1)
    s = np.concatenate([-sine, sine, -sine * scale, sine * scale], axis=1)
    return c.astype(np.float32), s.astype(np.float32)


def log_gammas():
    head = np.arange(HEADS, dtype=np.float32)
    exponent = np.float32(5.0) + np.float32(4.0) * head / np.float32(HEADS - 1)
    return np.log(1.0 - np.power(2.0, -exponent.astype(np.float64)))


def lanes(shape):
    return lax.broadcasted_iota(jnp.int32, shape, len(shape) - 1)


def layer_kernel(
    act_hbm, ng_hbm, qw_hbm, kw_hbm, vw_hbm, gw_hbm, ow_hbm, mg_hbm, uw_hbm, dw_hbm, cos_hbm, sin_hbm,
    out_ref,
    attn, upb, dnb, xall, wo, ret, wide, mid, hid, pps, ppr, rss, rsr,
    small, gains, tables, qkvg, gat, lhs, acc,
    local_sem, ring_send, first_recv, second_recv, x_send, x_recv, p_send, p_recv, r_send, r_recv,
):
    rep, fs, tp = lax.axis_index("rep"), lax.axis_index("fs"), lax.axis_index("tp")
    zl, y = lax.div(fs, 4), lax.rem(fs, 4)
    x, core = lax.div(tp, 2), lax.rem(tp, 2)
    zg = rep * 4 + zl

    def y_device(step):
        return {"fs": zl * 4 + lax.rem(y + step + 4, 4)}

    def z_device(step):
        other = lax.rem(zg + step + 8, 8)
        return {"rep": lax.div(other, 4), "fs": lax.rem(other, 4) * 4 + y}

    def x_index(step, c=core):
        return lax.rem(x + step + 4, 4) * 2 + c

    def x_device(step):
        return {"tp": x_index(step)}

    partner = {"tp": x * 2 + (1 - core)}

    barrier = pltpu.get_barrier_semaphore()
    peers = [y_device(1), y_device(-1), z_device(1), z_device(-1), partner]
    peers += [{"tp": x_index(step, c)} for step in (1, -1, 2) for c in range(2)]
    for peer in peers:
        pl.semaphore_signal(barrier, inc=1, device_id=peer, device_id_type=MESH)

    loads = (
        (qw_hbm, small.at[0], 0),
        (kw_hbm, small.at[1], 0),
        (vw_hbm, small.at[2], 0),
        (gw_hbm, small.at[3], 0),
        (ow_hbm.at[pl.ds(0, 32)], attn.at[0, zl, y, pl.ds(128, 32)], 1),
        (ow_hbm.at[pl.ds(32, 32)], attn.at[1, zl, y, pl.ds(128, 32)], 1),
        (act_hbm, xall.at[tp], 2),
        (uw_hbm.at[:, pl.ds(0, 512)], upb.at[0, zl, y], 3),
        (uw_hbm.at[:, pl.ds(512, 512)], upb.at[1, zl, y], 3),
        (dw_hbm.at[pl.ds(0, 512)], dnb.at[0, zl, y], 4),
        (dw_hbm.at[pl.ds(512, 512)], dnb.at[1, zl, y], 4),
        (ng_hbm, gains.at[0], 5),
        (mg_hbm, gains.at[1], 5),
        (cos_hbm, tables.at[0], 6),
        (sin_hbm, tables.at[1], 6),
    )
    for src, dst, n in loads:
        pltpu.make_async_copy(src, dst, local_sem.at[n]).start()

    def loaded(region, n):
        pltpu.make_async_copy(region, region, local_sem.at[n]).wait()

    loaded(small, 0)
    loaded(attn.at[0, 0, 0, pl.ds(0, 64)], 1)
    for h in range(2):
        attn[h, zl, y, 0:128, :] = small[2 * h : 2 * h + 2].reshape(128, 128).astype(F32).T.astype(BF)
    pl.semaphore_wait(barrier, len(peers))

    def remote(src, dst, send_sem, recv_sem, device):
        return pltpu.make_async_remote_copy(
            src_ref=src, dst_ref=dst, send_sem=send_sem, recv_sem=recv_sem, device_id=device, device_id_type=MESH
        )

    def send(src, dst, send_sem, recv_sem, device):
        remote(src, dst, send_sem, recv_sem, device).start()

    def arrive(region, recv_sem):
        remote(region, region, r_send.at[0], recv_sem, partner).wait_recv()

    def sent(region, send_sem):
        remote(region, region, send_sem, r_recv.at[0], partner).wait_send()

    bufs = (attn, upb, dnb)
    depth = (160, 128, 512)

    def block(item, half, dz, dy):
        return bufs[item].at[half, lax.rem(zl + dz + 4, 4), lax.rem(y + dy + 4, 4)]

    def along_y(half, phase):
        return (half + phase) % 2 == 0

    def piece(item, half, step, p):
        cut = depth[item] // 2
        dz, dy = (0, step) if half == 0 else (step, 0)
        return block(item, half, dz, dy).at[pl.ds(p * cut, cut)]

    def ring_device(half, phase, step):
        return y_device(step) if along_y(half, phase) else z_device(step)

    def first_start(item):
        for n in range(2):
            for half in range(2):
                for d in range(2):
                    ref = piece(item, half, 0, n if d == 0 else 1 - n)
                    send(ref, ref, ring_send.at[item], first_recv.at[2 * item + n], ring_device(half, 0, 1 - 2 * d))

    def first_forward(item):
        arrive(bufs[item].at[0, 0, pl.ds(0, 2)], first_recv.at[2 * item])
        for half in range(2):
            for d in range(2):
                to = 1 - 2 * d
                ref = piece(item, half, -to, d)
                send(ref, ref, ring_send.at[item], first_recv.at[2 * item + 1], ring_device(half, 0, to))

    def first_rest(item):
        arrive(bufs[item].at[0, 0], first_recv.at[2 * item + 1])

    def second_block(item, half, step, d, n):
        across = ORDER[d][n]
        return block(item, half, step, across) if half == 0 else block(item, half, across, step)

    def second_sem(item, n, far):
        if n < 2 and not far:
            return second_recv.at[2 * item + n]
        return second_recv.at[6 + item] if item < DOWN else second_recv.at[8 + n]

    def second_start(item, *which):
        for n in which:
            for half in range(2):
                for d in range(2):
                    ref = second_block(item, half, 0, d, n)
                    send(ref, ref, ring_send.at[3 + item], second_sem(item, n, False), ring_device(half, 1, 1 - 2 * d))

    def second_forward(item, *which):
        for n in which:
            arrive(bufs[item].at[0, 0], second_sem(item, n, False))
            for half in range(2):
                for d in range(2):
                    to = 1 - 2 * d
                    ref = second_block(item, half, -to, d, n)
                    send(ref, ref, ring_send.at[3 + item], second_sem(item, n, True), ring_device(half, 1, to))

    def second_rest(item):
        arrive(bufs[item].at[0], second_sem(item, 0, True))

    def second_four(item, n, far):
        arrive(bufs[item].at[0, 0], second_sem(item, n, far))

    def x_piece(which, t, p):
        if which == 0:
            return xall.at[t, pl.ds(p * 192, 192)]
        if which == 1:
            return wo.at[t, p]
        return ret.at[t, pl.ds(p * 96, 96)]

    whole = (xall, wo, ret)

    def x_sem(which, kind):
        return x_recv.at[which * 4 + kind]

    def hand_over(which, place, p):
        ref = x_piece(which, x_index((0, -1, 1, 2)[place]), p)
        send(ref, ref, x_send.at[which], x_sem(which, 3), partner)

    def x_start(which):
        for n in range(2):
            for d in range(2):
                p = n if d == 0 else 1 - n
                dst = x_piece(which, tp, p)
                src = attn.at[p, :, :, pl.ds(128, 32)] if which == 1 else dst
                send(src, dst, x_send.at[which], x_sem(which, n), x_device(1 - 2 * d))
        for p in range(2):
            dst = x_piece(which, tp, p)
            src = attn.at[p, :, :, pl.ds(128, 32)] if which == 1 else dst
            send(src, dst, x_send.at[which], x_sem(which, 3), partner)

    def x_forward(which):
        arrive(whole[which].at[0], x_sem(which, 0))
        for d in range(2):
            to = 1 - 2 * d
            ref = x_piece(which, x_index(-to), d)
            send(ref, ref, x_send.at[which], x_sem(which, 2), x_device(to))
            hand_over(which, 1 + d, d)

    def x_near(which):
        arrive(whole[which].at[0], x_sem(which, 1))
        for d in range(2):
            hand_over(which, 1 + d, 1 - d)

    def x_far(which):
        arrive(whole[which].at[0], x_sem(which, 2))
        for d in range(2):
            hand_over(which, 3, d)

    def x_partner(which):
        arrive(whole[which].at[pl.ds(0, 4)], x_sem(which, 3))

    def norm_rows(source, gain):
        @pl.loop(0, ROWS // 16)
        def _(i):
            rows = pl.ds(pl.multiple_of(i * 16, 16), 16)
            blocks = [source[t, rows, :].astype(F32) for t in range(8)]
            squares = blocks[0] * blocks[0]
            for b in blocks[1:]:
                squares = squares + b * b
            scale = lax.rsqrt(jnp.sum(squares, axis=-1, keepdims=True) * (1.0 / D) + EPSILON)
            for t in range(8):
                columns = slice(256 * t, 256 * t + 256)
                wide[rows, columns] = (blocks[t] * scale * gains[gain, :, columns]).astype(BF)

    first_start(ATTN)
    loaded(xall.at[0], 2)
    x_start(0)
    loaded(upb.at[0, 0, pl.ds(0, 2)], 3)
    first_start(UP)
    loaded(dnb.at[0, 0, pl.ds(0, 2)], 4)
    loaded(gains, 5)
    loaded(tables, 6)
    first_forward(ATTN)
    first_forward(UP)
    x_forward(0)
    first_rest(ATTN)
    second_start(ATTN, 0, 1, 2, 3)
    first_start(DOWN)
    x_near(0)
    second_forward(ATTN, 0, 1)
    first_rest(UP)
    second_start(UP, 0)
    x_far(0)
    x_partner(0)
    norm_rows(xall, 0)
    first_forward(DOWN)
    second_start(UP, 1, 2, 3)
    second_rest(ATTN)
    x_start(1)

    weights = jnp.concatenate([attn[h, :, :, 0:128, :].reshape(D, 128) for h in range(2)], axis=1)
    qkvg[...] = jnp.dot(wide[...], weights, preferred_element_type=F32)
    log_gamma = jnp.float32(0.0)
    for h, value in enumerate(log_gammas()):
        log_gamma = jnp.where(tp == h, jnp.float32(value), log_gamma)
    square = (SEQ_LEN, SEQ_LEN)
    distance = (lax.broadcasted_iota(jnp.int32, square, 0) - lanes(square)).astype(F32)
    decay = jnp.where(distance >= 0, jnp.exp(jnp.maximum(distance, 0.0) * log_gamma), 0.0)
    lane = lanes(square)
    first, low = lax.rem(lane, 64) < 32, lane < 64
    for s in range(3):
        rows = slice(SEQ_LEN * s, SEQ_LEN * (s + 1))
        qk, vg = qkvg[rows, 0:128], qkvg[rows, 128:256]
        other = jnp.where(first, pltpu.roll(qk, 96, 1), pltpu.roll(qk, 32, 1))
        turned = (qk * tables[0] + other * tables[1]).astype(BF).astype(F32)
        queries = jnp.where(low, turned, 0.0).astype(BF)
        keys = pltpu.roll(turned, 64, 1).astype(BF)
        scores = lax.dot_general(queries, keys, (((1,), (1,)), ((), ())), preferred_element_type=F32)
        mixed = jnp.dot((scores * decay).astype(BF), vg.astype(BF), preferred_element_type=F32)
        mixed = jnp.where(low, mixed, 0.0)
        mean = jnp.sum(mixed, axis=-1, keepdims=True) * (1.0 / HEAD_DIM)
        centred = jnp.where(low, mixed - mean, 0.0)
        variance = jnp.sum(centred * centred, axis=-1, keepdims=True) * (1.0 / HEAD_DIM)
        gate = pltpu.roll(vg, 64, 1)
        gat[rows, :] = centred * lax.rsqrt(variance + EPSILON) * (gate / (1.0 + jnp.exp(-gate)))
    low = lanes((192, 128)) < 64
    ret[tp] = jnp.where(low, gat[0:192, :], pltpu.roll(gat[192:384, :], 64, 1)).astype(BF)
    x_start(2)
    for h in range(2):
        wo[tp, h] = attn[h, :, :, 128:160, :]
    x_forward(1)
    second_forward(UP, 0)
    x_forward(2)
    second_forward(UP, 1)
    first_rest(DOWN)
    second_start(DOWN, 0, 1, 2)
    x_near(2)
    x_near(1)
    x_far(2)
    x_far(1)
    x_partner(2)
    x_partner(1)

    for j in range(4):
        a, b = ret[2 * j].astype(F32), ret[2 * j + 1].astype(F32)
        lhs[0:192, 128 * j : 128 * j + 128] = jnp.where(low, a, pltpu.roll(b, 64, 1)).astype(BF)
        lhs[192:384, 128 * j : 128 * j + 128] = jnp.where(low, pltpu.roll(a, 64, 1), b).astype(BF)

    @pl.loop(0, 8)
    def _(t):
        z0, y0 = lax.div(t, 2), lax.rem(t, 2) * 2
        columns = [wo[:, :, z0, y0 + k].reshape(HEADS * HEAD_DIM, 128) for k in range(2)]
        branch = jnp.dot(lhs[...], jnp.concatenate(columns, axis=1), preferred_element_type=F32)
        mid[t] = (xall[t].astype(F32) + branch).astype(BF)

    norm_rows(mid, 1)
    second_rest(UP)
    for h in range(2):
        raw = jnp.dot(wide[...], upb[h].reshape(D, 512), preferred_element_type=F32)
        raw = jnp.maximum(raw, 0.0)
        hid[:, 512 * h : 512 * h + 512] = (raw * raw).astype(BF)
    second_forward(DOWN, 0)

    def number(dz, dy):
        return (dz + 1) * 4 + dy + 1

    begun = set()

    def products(pairs):
        done = []
        for half, blocks in pairs:
            columns = jnp.concatenate([block(DOWN, half, dz, dy)[...] for dz, dy in blocks], axis=1)
            both = jnp.dot(hid[:, 512 * half : 512 * half + 512], columns, preferred_element_type=F32)
            for k, at in enumerate(blocks):
                value, n = both[:, 128 * k : 128 * k + 128], number(*at)
                if at in begun:
                    acc[n] += value
                    done.append(at)
                else:
                    acc[n] = value
                    begun.add(at)
        return done

    def rows_of(c):
        return pl.ds(pl.multiple_of(c * 192, 64), 192)

    def swap(blocks, group):
        for at in blocks:
            n = number(*at)
            pps[n] = acc[n, rows_of(1 - core), :].astype(BF)
            send(pps.at[n], ppr.at[n], p_send.at[0], p_recv.at[group], partner)


    def route(at):
        z_to, y_to = lax.rem(zl + at[0] + 4, 4), lax.rem(y + at[1] + 4, 4)
        c_to, k = lax.div(y_to, 2), lax.rem(y_to, 2)
        hops = lax.rem(z_to - x + 4, 4)
        return number(*at), {"tp": z_to * 2 + c_to}, c_to, k, hops

    def deliver(blocks, group):
        arrive(ppr.at[pl.ds(0, len(blocks))], p_recv.at[group])
        for at in blocks:
            n, owner, c_to, k, hops = route(at)
            total = (acc[n, rows_of(core), :] + ppr[n].astype(F32)).astype(BF)
            rss[n] = total

            @pl.when((hops > 0) | (c_to != core))
            def _():
                send(rss.at[n], rsr.at[hops, k, core], r_send.at[0], r_recv.at[0], owner)

            @pl.when((hops == 0) & (c_to == core))
            def _():
                rsr[0, k, core] = total

    def arrivals(n, far):
        step = (2, 2) if far else (-1, 1)
        rows = [(step[d], ORDER[d][n]) for d in range(2)]
        columns = [(ORDER[d][n], step[d]) for d in range(2)]
        return [(0, rows), (1, columns)]

    own = [(0, [(0, 0), (0, 1)]), (0, [(0, -1), (0, 2)]), (1, [(0, 0), (1, 0)]), (1, [(-1, 0), (2, 0)])]
    def deliver_on(c, blocks, group):
        @pl.when(core == c)
        def _():
            deliver(blocks, group)

    s0 = products(own)
    swap(s0, 0)
    s1 = products(arrivals(0, False))
    swap(s1, 1)
    second_forward(DOWN, 1)
    second_start(DOWN, 3)
    s2 = products(arrivals(1, False))
    swap(s2, 2)
    deliver_on(0, s0, 0)
    deliver_on(0, s1, 1)
    second_four(DOWN, 2, False)
    s3 = products(arrivals(2, False))
    swap(s3, 3)
    deliver_on(1, s0, 0)
    deliver_on(1, s1, 1)
    deliver(s2, 2)
    deliver_on(0, s3, 3)
    second_four(DOWN, 0, True)
    s4 = products(arrivals(0, True))
    swap(s4, 4)
    deliver_on(1, s3, 3)
    deliver_on(0, s4, 4)
    second_four(DOWN, 1, True)
    s5 = products(arrivals(1, True))
    swap(s5, 5)
    deliver_on(1, s4, 4)
    deliver(s5, 5)
    second_four(DOWN, 3, False)
    s6 = products(arrivals(3, False))
    swap(s6, 6)
    deliver(s6, 6)

    def collect():
        arrive(rss.at[pl.ds(0, 14)], r_recv.at[0])

    def finish():
        for k in range(2):
            for half in range(2):
                rows, columns = slice(192 * half, 192 * half + 192), slice(128 * k, 128 * k + 128)
                total = mid[tp, rows, columns].astype(F32)
                for hops in range(4):
                    total = total + rsr[hops, k, half].astype(F32)
                out_ref[rows, columns] = total.astype(BF)

    def drain():
        for item in range(3):
            sent(bufs[item].at[:, pl.ds(0, 3), 0], ring_send.at[item])
            sent(bufs[item].at[:, pl.ds(0, 3)], ring_send.at[3 + item])
        for which in range(3):
            sent(whole[which].at[pl.ds(0, 7)], x_send.at[which])
        sent(pps, p_send.at[0])
        sent(rss.at[pl.ds(0, 14)], r_send.at[0])

    collect()
    finish()
    drain()


def local(activations, norm_gain, qw, kw, vw, gw, ow, mlp_gain, uw, dw):
    cosine, sine = rotary_tables()
    operands = (
        activations, norm_gain.reshape(1, D), qw.T, kw.T, vw.T, gw.T, ow, mlp_gain.reshape(1, D), uw, dw,
        jnp.asarray(cosine), jnp.asarray(sine),
    )
    dma = pltpu.SemaphoreType.DMA
    rows = pl.pallas_call(
        layer_kernel,
        out_shape=pltpu.VMEM((ROWS, D // 8), BF),
        in_specs=[pl.BlockSpec(memory_space=pltpu.HBM)] * len(operands),
        out_specs=pl.BlockSpec(memory_space=pltpu.VMEM),
        scratch_shapes=[
            pltpu.VMEM((2, 4, 4, 160, 128), BF),
            pltpu.VMEM((2, 4, 4, 128, 512), BF),
            pltpu.VMEM((2, 4, 4, 512, 128), BF),
            pltpu.VMEM((8, ROWS, 256), BF),
            pltpu.VMEM((8, 2, 4, 4, 32, 128), BF),
            pltpu.VMEM((8, 192, 128), BF),
            pltpu.VMEM((ROWS, D), BF),
            pltpu.VMEM((8, ROWS, 256), BF),
            pltpu.VMEM((ROWS, 1024), BF),
            pltpu.VMEM((16, 192, 128), BF),
            pltpu.VMEM((16, 192, 128), BF),
            pltpu.VMEM((16, 192, 128), BF),
            pltpu.VMEM((4, 2, 2, 192, 128), BF),
            pltpu.VMEM((4, 64, 128), BF),
            pltpu.VMEM((2, 1, D), F32),
            pltpu.VMEM((2, 128, 128), F32),
            pltpu.VMEM((ROWS, 256), F32),
            pltpu.VMEM((ROWS, 128), F32),
            pltpu.VMEM((ROWS, 512), BF),
            pltpu.VMEM((16, ROWS, 128), F32),
            dma((7,)), dma((6,)), dma((6,)), dma((12,)), dma((3,)), dma((12,)), dma((1,)), dma((7,)), dma((1,)), dma((1,)),
        ],
        compiler_params=pltpu.CompilerParams(
            collective_id=0, has_side_effects=True, vmem_limit_bytes=56 * 1024 * 1024
        ),
        name="layer",
    )(*operands)
    return rows


def solution(mesh):
    in_specs = (
        P(("rep", "fs"), "tp"), P(), P("fs", "tp"), P("fs", "tp"), P("fs", "tp"), P("fs", "tp"), P("tp", "fs"), P(),
        P("fs", "tp"), P("tp", "fs"),
    )
    return jax.shard_map(local, mesh=mesh, in_specs=in_specs, out_specs=P(("rep", "fs"), "tp"), check_vma=False)
```

```python
import numpy as np
import jax
import jax.numpy as jnp
from jax import lax
from jax.experimental import pallas as pl
from jax.experimental.pallas import tpu as pltpu
from jax.sharding import PartitionSpec as P

HEADS = 8
HEAD_DIM = 64
SEQ_LEN = 128
EPSILON = 1e-06
ROWS = 384
D = 2048
NX = 4
BF = jnp.bfloat16
F32 = jnp.float32
MESH = pl.DeviceIdType.MESH
ATTN, UP, DOWN = 0, 1, 2
ORDER = ((0, 1, 2, -1), (-1, 2, 0, 1))


def rotary_tables():
    half = HEAD_DIM // 2
    position = np.arange(SEQ_LEN, dtype=np.float32)
    freqs = np.float32(10000.0) ** (-np.arange(half, dtype=np.float32) / np.float32(half))
    angle = position[:, None] * freqs[None, :].astype(np.float32)
    cosine, sine = np.cos(angle), np.sin(angle)
    scale = np.float32(HEAD_DIM**-0.5)
    c = np.concatenate([cosine, cosine, cosine * scale, cosine * scale], axis=1)
    s = np.concatenate([-sine, sine, -sine * scale, sine * scale], axis=1)
    return c.astype(np.float32), s.astype(np.float32)


def log_gammas():
    head = np.arange(HEADS, dtype=np.float32)
    exponent = np.float32(5.0) + np.float32(4.0) * head / np.float32(HEADS - 1)
    return np.log(1.0 - np.power(2.0, -exponent.astype(np.float64)))


def lanes(shape):
    return lax.broadcasted_iota(jnp.int32, shape, len(shape) - 1)


def layer_kernel(
    act_hbm, ng_hbm, qw_hbm, kw_hbm, vw_hbm, gw_hbm, ow_hbm, mg_hbm, uw_hbm, dw_hbm, cos_hbm, sin_hbm,
    out_ref,
    attn, upb, dnb, xall, wo, ret, wide, mid, hid, pps, ppr, rss, rsr,
    small, gains, tables, qkvg, gat, lhs, acc,
    local_sem, ring_send, first_recv, second_recv, x_send, x_recv, p_send, p_recv, r_send, r_recv,
):
    rep, fs, tp = lax.axis_index("rep"), lax.axis_index("fs"), lax.axis_index("tp")
    zl, y = lax.div(fs, 4), lax.rem(fs, 4)
    x, core = lax.div(tp, 2), lax.rem(tp, 2)
    zg = rep * 4 + zl

    def y_device(step):
        return {"fs": zl * 4 + lax.rem(y + step + 4, 4)}

    def z_device(step):
        other = lax.rem(zg + step + 8, 8)
        return {"rep": lax.div(other, 4), "fs": lax.rem(other, 4) * 4 + y}

    def x_index(step, c=core):
        return lax.rem(x + step + 4, 4) * 2 + c

    def x_device(step):
        return {"tp": x_index(step)}

    partner = {"tp": x * 2 + (1 - core)}

    barrier = pltpu.get_barrier_semaphore()
    peers = [y_device(1), y_device(-1), z_device(1), z_device(-1), x_device(1), x_device(-1), partner]
    for peer in peers:
        pl.semaphore_signal(barrier, inc=1, device_id=peer, device_id_type=MESH)

    loads = (
        (qw_hbm, small.at[0], 0),
        (kw_hbm, small.at[1], 0),
        (vw_hbm, small.at[2], 0),
        (gw_hbm, small.at[3], 0),
        (ow_hbm.at[pl.ds(0, 32)], attn.at[0, zl, y, pl.ds(128, 32)], 1),
        (ow_hbm.at[pl.ds(32, 32)], attn.at[1, zl, y, pl.ds(128, 32)], 1),
        (act_hbm, xall.at[tp], 2),
        (uw_hbm.at[:, pl.ds(0, 512)], upb.at[0, zl, y], 3),
        (uw_hbm.at[:, pl.ds(512, 512)], upb.at[1, zl, y], 3),
        (dw_hbm.at[pl.ds(0, 512)], dnb.at[0, zl, y], 4),
        (dw_hbm.at[pl.ds(512, 512)], dnb.at[1, zl, y], 4),
        (ng_hbm, gains.at[0], 5),
        (mg_hbm, gains.at[1], 5),
        (cos_hbm, tables.at[0], 6),
        (sin_hbm, tables.at[1], 6),
    )
    for src, dst, n in loads:
        pltpu.make_async_copy(src, dst, local_sem.at[n]).start()

    def loaded(region, n):
        pltpu.make_async_copy(region, region, local_sem.at[n]).wait()

    loaded(small, 0)
    loaded(attn.at[0, 0, 0, pl.ds(0, 64)], 1)
    for h in range(2):
        attn[h, zl, y, 0:128, :] = small[2 * h : 2 * h + 2].reshape(128, 128).astype(F32).T.astype(BF)
    pl.semaphore_wait(barrier, len(peers))

    def remote(src, dst, send_sem, recv_sem, device):
        return pltpu.make_async_remote_copy(
            src_ref=src, dst_ref=dst, send_sem=send_sem, recv_sem=recv_sem, device_id=device, device_id_type=MESH
        )

    def send(src, dst, send_sem, recv_sem, device):
        remote(src, dst, send_sem, recv_sem, device).start()

    def arrive(region, recv_sem):
        remote(region, region, r_send.at[0], recv_sem, partner).wait_recv()

    def sent(region, send_sem):
        remote(region, region, send_sem, r_recv.at[0], partner).wait_send()

    bufs = (attn, upb, dnb)
    depth = (160, 128, 512)

    def block(item, half, dz, dy):
        return bufs[item].at[half, lax.rem(zl + dz + 4, 4), lax.rem(y + dy + 4, 4)]

    def along_y(half, phase):
        return (half + phase) % 2 == 0

    def piece(item, half, step, p):
        cut = depth[item] // 2
        dz, dy = (0, step) if half == 0 else (step, 0)
        return block(item, half, dz, dy).at[pl.ds(p * cut, cut)]

    def ring_device(half, phase, step):
        return y_device(step) if along_y(half, phase) else z_device(step)

    def first_start(item):
        for n in range(2):
            for half in range(2):
                for d in range(2):
                    ref = piece(item, half, 0, n if d == 0 else 1 - n)
                    send(ref, ref, ring_send.at[item], first_recv.at[2 * item + n], ring_device(half, 0, 1 - 2 * d))

    def first_forward(item):
        arrive(bufs[item].at[0, 0, pl.ds(0, 2)], first_recv.at[2 * item])
        for half in range(2):
            for d in range(2):
                to = 1 - 2 * d
                ref = piece(item, half, -to, d)
                send(ref, ref, ring_send.at[item], first_recv.at[2 * item + 1], ring_device(half, 0, to))

    def first_rest(item):
        arrive(bufs[item].at[0, 0], first_recv.at[2 * item + 1])

    def second_block(item, half, step, d, n):
        across = ORDER[d][n]
        return block(item, half, step, across) if half == 0 else block(item, half, across, step)

    def second_sem(item, n, far):
        if n < 2 and not far:
            return second_recv.at[2 * item + n]
        return second_recv.at[6 + item] if item < DOWN else second_recv.at[8 + n]

    def second_start(item, *which):
        for n in which:
            for half in range(2):
                for d in range(2):
                    ref = second_block(item, half, 0, d, n)
                    send(ref, ref, ring_send.at[3 + item], second_sem(item, n, False), ring_device(half, 1, 1 - 2 * d))

    def second_forward(item, *which):
        for n in which:
            arrive(bufs[item].at[0, 0], second_sem(item, n, False))
            for half in range(2):
                for d in range(2):
                    to = 1 - 2 * d
                    ref = second_block(item, half, -to, d, n)
                    send(ref, ref, ring_send.at[3 + item], second_sem(item, n, True), ring_device(half, 1, to))

    def second_forward_on(c, item, n):
        @pl.when(core == c)
        def _():
            second_forward(item, n)

    def second_rest(item):
        arrive(bufs[item].at[0], second_sem(item, 0, True))

    def second_four(item, n, far):
        arrive(bufs[item].at[0, 0], second_sem(item, n, far))

    def x_piece(which, t, p):
        if which == 0:
            return xall.at[t, pl.ds(p * 192, 192)]
        if which == 1:
            return wo.at[t, p]
        return ret.at[t, pl.ds(p * 96, 96)]

    whole = (xall, wo, ret)

    def x_sem(which, kind):
        return x_recv.at[which * 4 + kind]

    def hand_over(which, place, p):
        ref = x_piece(which, x_index((0, -1, 1, 2)[place]), p)
        send(ref, ref, x_send.at[which], x_sem(which, 3), partner)

    def x_start(which):
        for n in range(2):
            for d in range(2):
                p = n if d == 0 else 1 - n
                dst = x_piece(which, tp, p)
                src = attn.at[p, :, :, pl.ds(128, 32)] if which == 1 else dst
                send(src, dst, x_send.at[which], x_sem(which, n), x_device(1 - 2 * d))
        for p in range(2):
            dst = x_piece(which, tp, p)
            src = attn.at[p, :, :, pl.ds(128, 32)] if which == 1 else dst
            send(src, dst, x_send.at[which], x_sem(which, 3), partner)

    def x_forward(which):
        arrive(whole[which].at[0], x_sem(which, 0))
        for d in range(2):
            to = 1 - 2 * d
            ref = x_piece(which, x_index(-to), d)
            send(ref, ref, x_send.at[which], x_sem(which, 2), x_device(to))
            hand_over(which, 1 + d, d)

    def x_near(which):
        arrive(whole[which].at[0], x_sem(which, 1))
        for d in range(2):
            hand_over(which, 1 + d, 1 - d)

    def x_far(which):
        arrive(whole[which].at[0], x_sem(which, 2))
        for d in range(2):
            hand_over(which, 3, d)

    def x_partner(which):
        arrive(whole[which].at[pl.ds(0, 4)], x_sem(which, 3))

    def norm_rows(source, gain):
        @pl.loop(0, ROWS // 16)
        def _(i):
            rows = pl.ds(pl.multiple_of(i * 16, 16), 16)
            blocks = [source[t, rows, :].astype(F32) for t in range(8)]
            squares = blocks[0] * blocks[0]
            for b in blocks[1:]:
                squares = squares + b * b
            scale = lax.rsqrt(jnp.sum(squares, axis=-1, keepdims=True) * (1.0 / D) + EPSILON)
            for t in range(8):
                columns = slice(256 * t, 256 * t + 256)
                wide[rows, columns] = (blocks[t] * scale * gains[gain, :, columns]).astype(BF)

    first_start(ATTN)
    loaded(xall.at[0], 2)
    x_start(0)
    loaded(upb.at[0, 0, pl.ds(0, 2)], 3)
    first_start(UP)
    loaded(dnb.at[0, 0, pl.ds(0, 2)], 4)
    loaded(gains, 5)
    loaded(tables, 6)
    first_forward(ATTN)
    first_forward(UP)
    x_forward(0)
    first_rest(ATTN)
    second_start(ATTN, 0, 1, 2, 3)
    first_start(DOWN)
    x_near(0)
    second_forward(ATTN, 0, 1)
    first_rest(UP)
    second_start(UP, 0)
    x_far(0)
    x_partner(0)
    norm_rows(xall, 0)
    first_forward(DOWN)
    second_start(UP, 1, 2, 3)
    second_rest(ATTN)
    x_start(1)

    weights = jnp.concatenate([attn[h, :, :, 0:128, :].reshape(D, 128) for h in range(2)], axis=1)
    qkvg[...] = jnp.dot(wide[...], weights, preferred_element_type=F32)
    log_gamma = jnp.float32(0.0)
    for h, value in enumerate(log_gammas()):
        log_gamma = jnp.where(tp == h, jnp.float32(value), log_gamma)
    square = (SEQ_LEN, SEQ_LEN)
    distance = (lax.broadcasted_iota(jnp.int32, square, 0) - lanes(square)).astype(F32)
    decay = jnp.where(distance >= 0, jnp.exp(jnp.maximum(distance, 0.0) * log_gamma), 0.0)
    lane = lanes(square)
    first, low = lax.rem(lane, 64) < 32, lane < 64
    for s in range(3):
        rows = slice(SEQ_LEN * s, SEQ_LEN * (s + 1))
        qk, vg = qkvg[rows, 0:128], qkvg[rows, 128:256]
        other = jnp.where(first, pltpu.roll(qk, 96, 1), pltpu.roll(qk, 32, 1))
        turned = (qk * tables[0] + other * tables[1]).astype(BF).astype(F32)
        queries = jnp.where(low, turned, 0.0).astype(BF)
        keys = pltpu.roll(turned, 64, 1).astype(BF)
        scores = lax.dot_general(queries, keys, (((1,), (1,)), ((), ())), preferred_element_type=F32)
        mixed = jnp.dot((scores * decay).astype(BF), vg.astype(BF), preferred_element_type=F32)
        mixed = jnp.where(low, mixed, 0.0)
        mean = jnp.sum(mixed, axis=-1, keepdims=True) * (1.0 / HEAD_DIM)
        centred = jnp.where(low, mixed - mean, 0.0)
        variance = jnp.sum(centred * centred, axis=-1, keepdims=True) * (1.0 / HEAD_DIM)
        gate = pltpu.roll(vg, 64, 1)
        gat[rows, :] = centred * lax.rsqrt(variance + EPSILON) * (gate / (1.0 + jnp.exp(-gate)))
    low = lanes((192, 128)) < 64
    ret[tp] = jnp.where(low, gat[0:192, :], pltpu.roll(gat[192:384, :], 64, 1)).astype(BF)
    x_start(2)
    for h in range(2):
        wo[tp, h] = attn[h, :, :, 128:160, :]
    x_forward(1)
    second_forward(UP, 0)
    x_forward(2)
    second_forward(UP, 1)
    first_rest(DOWN)
    second_start(DOWN, 0, 1)
    x_near(2)
    x_near(1)
    x_far(2)
    x_far(1)
    x_partner(2)
    x_partner(1)

    for j in range(4):
        a, b = ret[2 * j].astype(F32), ret[2 * j + 1].astype(F32)
        lhs[0:192, 128 * j : 128 * j + 128] = jnp.where(low, a, pltpu.roll(b, 64, 1)).astype(BF)
        lhs[192:384, 128 * j : 128 * j + 128] = jnp.where(low, pltpu.roll(a, 64, 1), b).astype(BF)

    @pl.loop(0, 8)
    def _(t):
        z0, y0 = lax.div(t, 2), lax.rem(t, 2) * 2
        columns = [wo[:, :, z0, y0 + k].reshape(HEADS * HEAD_DIM, 128) for k in range(2)]
        branch = jnp.dot(lhs[...], jnp.concatenate(columns, axis=1), preferred_element_type=F32)
        mid[t] = (xall[t].astype(F32) + branch).astype(BF)

    norm_rows(mid, 1)
    second_rest(UP)
    second_forward_on(1, DOWN, 0)
    for h in range(2):
        raw = jnp.dot(wide[...], upb[h].reshape(D, 512), preferred_element_type=F32)
        raw = jnp.maximum(raw, 0.0)
        hid[:, 512 * h : 512 * h + 512] = (raw * raw).astype(BF)
    second_forward_on(0, DOWN, 0)

    def number(dz, dy):
        return (dz + 1) * 4 + dy + 1

    begun = set()

    def products(pairs):
        done = []
        for half, blocks in pairs:
            columns = jnp.concatenate([block(DOWN, half, dz, dy)[...] for dz, dy in blocks], axis=1)
            both = jnp.dot(hid[:, 512 * half : 512 * half + 512], columns, preferred_element_type=F32)
            for k, at in enumerate(blocks):
                value, n = both[:, 128 * k : 128 * k + 128], number(*at)
                if at in begun:
                    acc[n] += value
                    done.append(at)
                else:
                    acc[n] = value
                    begun.add(at)
        return done

    def rows_of(c):
        return pl.ds(pl.multiple_of(c * 192, 64), 192)

    def swap(blocks, group):
        for at in blocks:
            n = number(*at)
            pps[n] = acc[n, rows_of(1 - core), :].astype(BF)
            send(pps.at[n], ppr.at[n], p_send.at[0], p_recv.at[group], partner)


    def route(at):
        z_to, y_to = lax.rem(zl + at[0] + 4, 4), lax.rem(y + at[1] + 4, 4)
        c_to, k = lax.div(y_to, 2), lax.rem(y_to, 2)
        hops = lax.rem(z_to - x + 4, 4)
        return number(*at), {"tp": z_to * 2 + c_to}, c_to, k, hops

    def deliver(blocks, group):
        arrive(ppr.at[pl.ds(0, len(blocks))], p_recv.at[group])
        for at in blocks:
            n, owner, c_to, k, hops = route(at)
            total = (acc[n, rows_of(core), :] + ppr[n].astype(F32)).astype(BF)
            rss[n] = total

            @pl.when((hops > 0) | (c_to != core))
            def _():
                send(rss.at[n], rsr.at[hops, k, core], r_send.at[0], r_recv.at[0], owner)

            @pl.when((hops == 0) & (c_to == core))
            def _():
                rsr[0, k, core] = total

    def arrivals(n, far):
        step = (2, 2) if far else (-1, 1)
        rows = [(step[d], ORDER[d][n]) for d in range(2)]
        columns = [(ORDER[d][n], step[d]) for d in range(2)]
        return [(0, rows), (1, columns)]

    own = [(0, [(0, 0), (0, 1)]), (0, [(0, -1), (0, 2)]), (1, [(0, 0), (1, 0)]), (1, [(-1, 0), (2, 0)])]
    def deliver_on(c, blocks, group):
        @pl.when(core == c)
        def _():
            deliver(blocks, group)

    s0 = products(own)
    swap(s0, 0)
    s1 = products(arrivals(0, False))
    swap(s1, 1)
    second_forward(DOWN, 1)
    second_start(DOWN, 2, 3)
    s2 = products(arrivals(1, False))
    swap(s2, 2)
    deliver_on(0, s0, 0)
    deliver_on(0, s1, 1)
    second_four(DOWN, 0, True)
    s3 = products(arrivals(0, True))
    swap(s3, 3)
    deliver_on(1, s0, 0)
    deliver_on(1, s1, 1)
    deliver(s2, 2)
    deliver_on(0, s3, 3)
    second_four(DOWN, 1, True)
    s4 = products(arrivals(1, True))
    swap(s4, 4)
    deliver_on(1, s3, 3)
    deliver_on(0, s4, 4)
    second_four(DOWN, 2, False)
    s5 = products(arrivals(2, False))
    swap(s5, 5)
    deliver_on(1, s4, 4)
    deliver(s5, 5)
    second_four(DOWN, 3, False)
    s6 = products(arrivals(3, False))
    swap(s6, 6)
    deliver(s6, 6)

    def collect():
        arrive(rss.at[pl.ds(0, 14)], r_recv.at[0])

    def finish():
        for k in range(2):
            for half in range(2):
                rows, columns = slice(192 * half, 192 * half + 192), slice(128 * k, 128 * k + 128)
                total = mid[tp, rows, columns].astype(F32)
                for hops in range(4):
                    total = total + rsr[hops, k, half].astype(F32)
                out_ref[rows, columns] = total.astype(BF)

    def drain():
        for item in range(3):
            sent(bufs[item].at[:, pl.ds(0, 3), 0], ring_send.at[item])
            sent(bufs[item].at[:, pl.ds(0, 3)], ring_send.at[3 + item])
        for which in range(3):
            sent(whole[which].at[pl.ds(0, 7)], x_send.at[which])
        sent(pps, p_send.at[0])
        sent(rss.at[pl.ds(0, 14)], r_send.at[0])

    collect()
    finish()
    drain()


def local(activations, norm_gain, qw, kw, vw, gw, ow, mlp_gain, uw, dw):
    cosine, sine = rotary_tables()
    operands = (
        activations, norm_gain.reshape(1, D), qw.T, kw.T, vw.T, gw.T, ow, mlp_gain.reshape(1, D), uw, dw,
        jnp.asarray(cosine), jnp.asarray(sine),
    )
    dma = pltpu.SemaphoreType.DMA
    rows = pl.pallas_call(
        layer_kernel,
        out_shape=pltpu.VMEM((ROWS, D // 8), BF),
        in_specs=[pl.BlockSpec(memory_space=pltpu.HBM)] * len(operands),
        out_specs=pl.BlockSpec(memory_space=pltpu.VMEM),
        scratch_shapes=[
            pltpu.VMEM((2, 4, 4, 160, 128), BF),
            pltpu.VMEM((2, 4, 4, 128, 512), BF),
            pltpu.VMEM((2, 4, 4, 512, 128), BF),
            pltpu.VMEM((8, ROWS, 256), BF),
            pltpu.VMEM((8, 2, 4, 4, 32, 128), BF),
            pltpu.VMEM((8, 192, 128), BF),
            pltpu.VMEM((ROWS, D), BF),
            pltpu.VMEM((8, ROWS, 256), BF),
            pltpu.VMEM((ROWS, 1024), BF),
            pltpu.VMEM((16, 192, 128), BF),
            pltpu.VMEM((16, 192, 128), BF),
            pltpu.VMEM((16, 192, 128), BF),
            pltpu.VMEM((4, 2, 2, 192, 128), BF),
            pltpu.VMEM((4, 64, 128), BF),
            pltpu.VMEM((2, 1, D), F32),
            pltpu.VMEM((2, 128, 128), F32),
            pltpu.VMEM((ROWS, 256), F32),
            pltpu.VMEM((ROWS, 128), F32),
            pltpu.VMEM((ROWS, 512), BF),
            pltpu.VMEM((16, ROWS, 128), F32),
            dma((7,)), dma((6,)), dma((6,)), dma((12,)), dma((3,)), dma((12,)), dma((1,)), dma((7,)), dma((1,)), dma((1,)),
        ],
        compiler_params=pltpu.CompilerParams(
            collective_id=0, has_side_effects=True, vmem_limit_bytes=56 * 1024 * 1024
        ),
        name="layer",
    )(*operands)
    return rows


def solution(mesh):
    in_specs = (
        P(("rep", "fs"), "tp"), P(), P("fs", "tp"), P("fs", "tp"), P("fs", "tp"), P("fs", "tp"), P("tp", "fs"), P(),
        P("fs", "tp"), P("tp", "fs"),
    )
    return jax.shard_map(local, mesh=mesh, in_specs=in_specs, out_specs=P(("rep", "fs"), "tp"), check_vma=False)
```

```python
import numpy as np
import jax
import jax.numpy as jnp
from jax import lax
from jax.experimental import pallas as pl
from jax.experimental.pallas import tpu as pltpu
from jax.sharding import PartitionSpec as P

HEADS = 8
HEAD_DIM = 64
SEQ_LEN = 128
EPSILON = 1e-06
ROWS = 384
D = 2048
NX = 4
BF = jnp.bfloat16
F32 = jnp.float32
MESH = pl.DeviceIdType.MESH
ATTN, UP, DOWN = 0, 1, 2
ORDER = ((0, 1, 2, -1), (2, -1, 0, 1))


def rotary_tables():
    half = HEAD_DIM // 2
    position = np.arange(SEQ_LEN, dtype=np.float32)
    freqs = np.float32(10000.0) ** (-np.arange(half, dtype=np.float32) / np.float32(half))
    angle = position[:, None] * freqs[None, :].astype(np.float32)
    cosine, sine = np.cos(angle), np.sin(angle)
    scale = np.float32(HEAD_DIM**-0.5)
    c = np.concatenate([cosine, cosine, cosine * scale, cosine * scale], axis=1)
    s = np.concatenate([-sine, sine, -sine * scale, sine * scale], axis=1)
    return c.astype(np.float32), s.astype(np.float32)


def log_gammas():
    head = np.arange(HEADS, dtype=np.float32)
    exponent = np.float32(5.0) + np.float32(4.0) * head / np.float32(HEADS - 1)
    return np.log(1.0 - np.power(2.0, -exponent.astype(np.float64)))


def lanes(shape):
    return lax.broadcasted_iota(jnp.int32, shape, len(shape) - 1)


def layer_kernel(
    act_hbm, ng_hbm, qw_hbm, kw_hbm, vw_hbm, gw_hbm, ow_hbm, mg_hbm, uw_hbm, dw_hbm, cos_hbm, sin_hbm,
    out_ref,
    attn, upb, dnb, xall, wo, ret, wide, mid, hid, pps, ppr, rss, rsr,
    small, gains, tables, qkvg, gat, lhs, acc,
    hid2, ext, last, local_sem, ring_send, first_recv, second_recv, x_send, x_recv, p_send, p_recv, r_send, r_recv, h_send, h_recv,
):
    rep, fs, tp = lax.axis_index("rep"), lax.axis_index("fs"), lax.axis_index("tp")
    zl, y = lax.div(fs, 4), lax.rem(fs, 4)
    x, core = lax.div(tp, 2), lax.rem(tp, 2)
    zg = rep * 4 + zl

    def y_device(step):
        return {"fs": zl * 4 + lax.rem(y + step + 4, 4)}

    def z_device(step):
        other = lax.rem(zg + step + 8, 8)
        return {"rep": lax.div(other, 4), "fs": lax.rem(other, 4) * 4 + y}

    def x_index(step, c=core):
        return lax.rem(x + step + 4, 4) * 2 + c

    def x_device(step):
        return {"tp": x_index(step)}

    partner = {"tp": x * 2 + (1 - core)}

    barrier = pltpu.get_barrier_semaphore()
    peers = [y_device(1), y_device(-1), z_device(1), z_device(-1), x_device(1), x_device(-1), partner]
    for peer in peers:
        pl.semaphore_signal(barrier, inc=1, device_id=peer, device_id_type=MESH)

    loads = (
        (qw_hbm, small.at[0], 0),
        (kw_hbm, small.at[1], 0),
        (vw_hbm, small.at[2], 0),
        (gw_hbm, small.at[3], 0),
        (ow_hbm.at[pl.ds(0, 32)], attn.at[0, zl, y, pl.ds(128, 32)], 1),
        (ow_hbm.at[pl.ds(32, 32)], attn.at[1, zl, y, pl.ds(128, 32)], 1),
        (act_hbm, xall.at[tp], 2),
        (uw_hbm.at[:, pl.ds(0, 512)], upb.at[0, zl, y], 3),
        (uw_hbm.at[:, pl.ds(512, 512)], upb.at[1, zl, y], 3),
        (dw_hbm.at[pl.ds(0, 512)], dnb.at[0, zl, y], 4),
        (dw_hbm.at[pl.ds(512, 512)], dnb.at[1, zl, y], 4),
        (ng_hbm, gains.at[0], 5),
        (mg_hbm, gains.at[1], 5),
        (cos_hbm, tables.at[0], 6),
        (sin_hbm, tables.at[1], 6),
    )
    for src, dst, n in loads:
        pltpu.make_async_copy(src, dst, local_sem.at[n]).start()

    def loaded(region, n):
        pltpu.make_async_copy(region, region, local_sem.at[n]).wait()

    loaded(small, 0)
    loaded(attn.at[0, 0, 0, pl.ds(0, 64)], 1)
    for h in range(2):
        attn[h, zl, y, 0:128, :] = small[2 * h : 2 * h + 2].reshape(128, 128).astype(F32).T.astype(BF)
    pl.semaphore_wait(barrier, len(peers))

    def remote(src, dst, send_sem, recv_sem, device):
        return pltpu.make_async_remote_copy(
            src_ref=src, dst_ref=dst, send_sem=send_sem, recv_sem=recv_sem, device_id=device, device_id_type=MESH
        )

    def send(src, dst, send_sem, recv_sem, device):
        remote(src, dst, send_sem, recv_sem, device).start()

    def arrive(region, recv_sem):
        remote(region, region, r_send.at[0], recv_sem, partner).wait_recv()

    def sent(region, send_sem):
        remote(region, region, send_sem, r_recv.at[0], partner).wait_send()

    bufs = (attn, upb, dnb)
    depth = (160, 128, 512)

    def block(item, half, dz, dy):
        return bufs[item].at[half, lax.rem(zl + dz + 4, 4), lax.rem(y + dy + 4, 4)]

    def along_y(half, phase):
        return (half + phase) % 2 == 0

    def piece(item, half, step, p):
        cut = depth[item] // 2
        dz, dy = (0, step) if half == 0 else (step, 0)
        return block(item, half, dz, dy).at[pl.ds(p * cut, cut)]

    def ring_device(half, phase, step):
        return y_device(step) if along_y(half, phase) else z_device(step)

    def first_start(item):
        for n in range(2):
            for half in range(2):
                for d in range(2):
                    ref = piece(item, half, 0, n if d == 0 else 1 - n)
                    send(ref, ref, ring_send.at[item], first_recv.at[2 * item + n], ring_device(half, 0, 1 - 2 * d))

    def first_forward(item):
        arrive(bufs[item].at[0, 0, pl.ds(0, 2)], first_recv.at[2 * item])
        for half in range(2):
            for d in range(2):
                to = 1 - 2 * d
                ref = piece(item, half, -to, d)
                send(ref, ref, ring_send.at[item], first_recv.at[2 * item + 1], ring_device(half, 0, to))

    def first_rest(item):
        arrive(bufs[item].at[0, 0], first_recv.at[2 * item + 1])

    def second_block(item, half, step, d, n):
        across = ORDER[d][n]
        return block(item, half, step, across) if half == 0 else block(item, half, across, step)

    def second_sem(item, n, far):
        if n < 2 and not far:
            return second_recv.at[2 * item + n]
        return second_recv.at[6 + item] if item < DOWN else second_recv.at[8 + n]

    def second_start(item, *which):
        for n in which:
            for half in range(2):
                for d in range(2):
                    ref = second_block(item, half, 0, d, n)
                    send(ref, ref, ring_send.at[3 + item], second_sem(item, n, False), ring_device(half, 1, 1 - 2 * d))

    def second_forward(item, *which):
        for n in which:
            arrive(bufs[item].at[0, 0], second_sem(item, n, False))
            for half in range(2):
                for d in range(2):
                    to = 1 - 2 * d
                    ref = second_block(item, half, -to, d, n)
                    send(ref, ref, ring_send.at[3 + item], second_sem(item, n, True), ring_device(half, 1, to))

    def second_forward_on(c, item, n):
        @pl.when(core == c)
        def _():
            second_forward(item, n)

    def second_rest(item):
        arrive(bufs[item].at[0], second_sem(item, 0, True))

    def second_four(item, n, far):
        arrive(bufs[item].at[0, 0], second_sem(item, n, far))

    def x_piece(which, t, p):
        if which == 0:
            return xall.at[t, pl.ds(p * 192, 192)]
        if which == 1:
            return wo.at[t, p]
        return ret.at[t, pl.ds(p * 96, 96)]

    whole = (xall, wo, ret)

    def x_sem(which, kind):
        return x_recv.at[which * 4 + kind]

    def hand_over(which, place, p):
        ref = x_piece(which, x_index((0, -1, 1, 2)[place]), p)
        send(ref, ref, x_send.at[which], x_sem(which, 3), partner)

    def x_start(which):
        for n in range(2):
            for d in range(2):
                p = n if d == 0 else 1 - n
                dst = x_piece(which, tp, p)
                src = attn.at[p, :, :, pl.ds(128, 32)] if which == 1 else dst
                send(src, dst, x_send.at[which], x_sem(which, n), x_device(1 - 2 * d))
        for p in range(2):
            dst = x_piece(which, tp, p)
            src = attn.at[p, :, :, pl.ds(128, 32)] if which == 1 else dst
            send(src, dst, x_send.at[which], x_sem(which, 3), partner)

    def x_forward(which):
        arrive(whole[which].at[0], x_sem(which, 0))
        for d in range(2):
            to = 1 - 2 * d
            ref = x_piece(which, x_index(-to), d)
            send(ref, ref, x_send.at[which], x_sem(which, 2), x_device(to))
            hand_over(which, 1 + d, d)

    def x_near(which):
        arrive(whole[which].at[0], x_sem(which, 1))
        for d in range(2):
            hand_over(which, 1 + d, 1 - d)

    def x_far(which):
        arrive(whole[which].at[0], x_sem(which, 2))
        for d in range(2):
            hand_over(which, 3, d)

    def x_partner(which):
        arrive(whole[which].at[pl.ds(0, 4)], x_sem(which, 3))

    def norm_rows(source, gain):
        @pl.loop(0, ROWS // 16)
        def _(i):
            rows = pl.ds(pl.multiple_of(i * 16, 16), 16)
            blocks = [source[t, rows, :].astype(F32) for t in range(8)]
            squares = blocks[0] * blocks[0]
            for b in blocks[1:]:
                squares = squares + b * b
            scale = lax.rsqrt(jnp.sum(squares, axis=-1, keepdims=True) * (1.0 / D) + EPSILON)
            for t in range(8):
                columns = slice(256 * t, 256 * t + 256)
                wide[rows, columns] = (blocks[t] * scale * gains[gain, :, columns]).astype(BF)

    first_start(ATTN)
    loaded(xall.at[0], 2)
    x_start(0)
    loaded(upb.at[0, 0, pl.ds(0, 2)], 3)
    first_start(UP)
    loaded(dnb.at[0, 0, pl.ds(0, 2)], 4)
    loaded(gains, 5)
    loaded(tables, 6)
    first_forward(ATTN)
    first_forward(UP)
    x_forward(0)
    first_rest(ATTN)
    second_start(ATTN, 0, 1, 2, 3)
    first_start(DOWN)
    x_near(0)
    second_forward(ATTN, 0, 1)
    first_rest(UP)
    second_start(UP, 0)
    x_far(0)
    x_partner(0)
    norm_rows(xall, 0)
    first_forward(DOWN)
    second_start(UP, 1, 2, 3)
    second_rest(ATTN)
    x_start(1)

    weights = jnp.concatenate([attn[h, :, :, 0:128, :].reshape(D, 128) for h in range(2)], axis=1)
    qkvg[...] = jnp.dot(wide[...], weights, preferred_element_type=F32)
    log_gamma = jnp.float32(0.0)
    for h, value in enumerate(log_gammas()):
        log_gamma = jnp.where(tp == h, jnp.float32(value), log_gamma)
    square = (SEQ_LEN, SEQ_LEN)
    distance = (lax.broadcasted_iota(jnp.int32, square, 0) - lanes(square)).astype(F32)
    decay = jnp.where(distance >= 0, jnp.exp(jnp.maximum(distance, 0.0) * log_gamma), 0.0)
    lane = lanes(square)
    first, low = lax.rem(lane, 64) < 32, lane < 64
    for s in range(3):
        rows = slice(SEQ_LEN * s, SEQ_LEN * (s + 1))
        qk, vg = qkvg[rows, 0:128], qkvg[rows, 128:256]
        other = jnp.where(first, pltpu.roll(qk, 96, 1), pltpu.roll(qk, 32, 1))
        turned = (qk * tables[0] + other * tables[1]).astype(BF).astype(F32)
        queries = jnp.where(low, turned, 0.0).astype(BF)
        keys = pltpu.roll(turned, 64, 1).astype(BF)
        scores = lax.dot_general(queries, keys, (((1,), (1,)), ((), ())), preferred_element_type=F32)
        mixed = jnp.dot((scores * decay).astype(BF), vg.astype(BF), preferred_element_type=F32)
        mixed = jnp.where(low, mixed, 0.0)
        mean = jnp.sum(mixed, axis=-1, keepdims=True) * (1.0 / HEAD_DIM)
        centred = jnp.where(low, mixed - mean, 0.0)
        variance = jnp.sum(centred * centred, axis=-1, keepdims=True) * (1.0 / HEAD_DIM)
        gate = pltpu.roll(vg, 64, 1)
        gat[rows, :] = centred * lax.rsqrt(variance + EPSILON) * (gate / (1.0 + jnp.exp(-gate)))
    low = lanes((192, 128)) < 64
    ret[tp] = jnp.where(low, gat[0:192, :], pltpu.roll(gat[192:384, :], 64, 1)).astype(BF)
    x_start(2)
    for h in range(2):
        wo[tp, h] = attn[h, :, :, 128:160, :]
    x_forward(1)
    second_forward(UP, 0)
    x_forward(2)
    second_forward(UP, 1)
    first_rest(DOWN)
    second_start(DOWN, 0, 1)
    x_near(2)
    x_near(1)
    x_far(2)
    x_far(1)
    x_partner(2)
    x_partner(1)

    for j in range(4):
        a, b = ret[2 * j].astype(F32), ret[2 * j + 1].astype(F32)
        lhs[0:192, 128 * j : 128 * j + 128] = jnp.where(low, a, pltpu.roll(b, 64, 1)).astype(BF)
        lhs[192:384, 128 * j : 128 * j + 128] = jnp.where(low, pltpu.roll(a, 64, 1), b).astype(BF)

    @pl.loop(0, 8)
    def _(t):
        z0, y0 = lax.div(t, 2), lax.rem(t, 2) * 2
        columns = [wo[:, :, z0, y0 + k].reshape(HEADS * HEAD_DIM, 128) for k in range(2)]
        branch = jnp.dot(lhs[...], jnp.concatenate(columns, axis=1), preferred_element_type=F32)
        mid[t] = (xall[t].astype(F32) + branch).astype(BF)

    norm_rows(mid, 1)
    second_rest(UP)
    second_forward_on(1, DOWN, 0)
    for h in range(2):
        raw = jnp.dot(wide[...], upb[h].reshape(D, 512), preferred_element_type=F32)
        raw = jnp.maximum(raw, 0.0)
        hid[:, 512 * h : 512 * h + 512] = (raw * raw).astype(BF)
    second_forward_on(0, DOWN, 0)
    send(hid, hid2, h_send.at[0], h_recv.at[0], partner)

    def number(dz, dy):
        return (dz + 1) * 4 + dy + 1

    def last_start():
        for half in range(2):
            for d in range(2):
                ref, sem = second_block(DOWN, half, 0, d, 3), second_sem(DOWN, 3, False)
                there = ring_device(half, 1, 1 - 2 * d)

                @pl.when(core == d)
                def _():
                    send(ref, ref, ring_send.at[3 + DOWN], sem, there)

                @pl.when(core != d)
                def _():
                    send(ref, ext.at[half], ring_send.at[3 + DOWN], sem, {**there, "tp": x * 2 + d})

    begun = set()

    def products(pairs):
        done = []
        for half, blocks in pairs:
            columns = jnp.concatenate([block(DOWN, half, dz, dy)[...] for dz, dy in blocks], axis=1)
            both = jnp.dot(hid[:, 512 * half : 512 * half + 512], columns, preferred_element_type=F32)
            for k, at in enumerate(blocks):
                value, n = both[:, 128 * k : 128 * k + 128], number(*at)
                if at in begun:
                    acc[n] += value
                    done.append(at)
                else:
                    acc[n] = value
                    begun.add(at)
        return done

    def rows_of(c):
        return pl.ds(pl.multiple_of(c * 192, 64), 192)

    def swap(blocks, group):
        for at in blocks:
            n = number(*at)
            pps[n] = acc[n, rows_of(1 - core), :].astype(BF)
            send(pps.at[n], ppr.at[n], p_send.at[0], p_recv.at[group], partner)


    def route(dz, dy):
        z_to, y_to = lax.rem(zl + dz + 4, 4), lax.rem(y + dy + 4, 4)
        c_to, k = lax.div(y_to, 2), lax.rem(y_to, 2)
        hops = lax.rem(z_to - x + 4, 4)
        return {"tp": z_to * 2 + c_to}, k, hops, (hops == 0) & (c_to == core), lax.div(3 - hops, 3) * (1 + k)

    def deliver(blocks, group):
        arrive(ppr.at[pl.ds(0, len(blocks))], p_recv.at[group])
        for at in blocks:
            n = number(*at)
            owner, k, hops, own, sem = route(*at)
            total = (acc[n, rows_of(core), :] + ppr[n].astype(F32)).astype(BF)
            rss[n] = total

            @pl.when(jnp.logical_not(own))
            def _():
                send(rss.at[n], rsr.at[hops, k, core], r_send.at[0], r_recv.at[sem], owner)

            @pl.when(own)
            def _():
                rsr[0, k, core] = total

    step = 2 * core - 1

    def deliver_last():
        owner, k, hops, own, sem = route(step, step)
        z_from, y_from = lax.rem(zl + step + 4, 4), lax.rem(y + step + 4, 4)
        mine = jnp.concatenate([dnb[0, z_from, y_from], dnb[1, z_from, y_from]], axis=0)
        other = ext[...].reshape(1024, 128)
        for half in range(2):
            rows = slice(192 * half, 192 * half + 192)
            total = jnp.dot(hid[rows, :], mine, preferred_element_type=F32)
            total = (total + jnp.dot(hid2[rows, :], other, preferred_element_type=F32)).astype(BF)
            last[half] = total

            @pl.when(jnp.logical_not(own))
            def _():
                send(last.at[half], rsr.at[hops, k, half], r_send.at[1], r_recv.at[sem], owner)

            @pl.when(own)
            def _():
                rsr[0, k, half] = total

    def arrivals(n, far):
        step = (2, 2) if far else (-1, 1)
        rows = [(step[d], ORDER[d][n]) for d in range(2)]
        columns = [(ORDER[d][n], step[d]) for d in range(2)]
        return [(0, rows), (1, columns)]

    own = [(0, [(0, 0), (0, 1)]), (0, [(0, -1), (0, 2)]), (1, [(0, 0), (1, 0)]), (1, [(-1, 0), (2, 0)])]
    def deliver_on(c, blocks, group):
        @pl.when(core == c)
        def _():
            deliver(blocks, group)

    s0 = products(own)
    swap(s0, 0)
    s1 = products(arrivals(0, False))
    swap(s1, 1)
    second_forward(DOWN, 1)
    second_start(DOWN, 2)
    last_start()
    s2 = products(arrivals(1, False))
    swap(s2, 2)
    deliver_on(0, s0, 0)
    deliver_on(0, s1, 1)
    second_four(DOWN, 0, True)
    s3 = products(arrivals(0, True))
    swap(s3, 3)
    deliver_on(1, s0, 0)
    deliver_on(1, s1, 1)
    deliver(s2, 2)
    deliver_on(0, s3, 3)
    second_four(DOWN, 1, True)
    s4 = products(arrivals(1, True))
    swap(s4, 4)
    deliver_on(1, s3, 3)
    deliver_on(0, s4, 4)
    second_four(DOWN, 2, False)
    s5 = products(arrivals(2, False))
    swap(s5, 5)
    deliver_on(1, s4, 4)
    deliver(s5, 5)
    arrive(hid2, h_recv.at[0])
    second_four(DOWN, 3, False)
    deliver_last()

    def late(k, c):
        dz, dy = lax.rem(x - zl + 4, 4), lax.rem(core * 2 + k - y + 4, 4)
        return (dz == (2 * c + 3) % 4) & (dy == (2 * c + 3) % 4)

    def collect():
        arrive(rss.at[pl.ds(0, 12)], r_recv.at[0])
        for k in range(2):
            first, second = late(k, 0), late(k, 1)

            @pl.when((first & (core == 1)) | (second & (core == 0)))
            def _():
                arrive(rsr.at[0, k], r_recv.at[1 + k])

            @pl.when(jnp.logical_not(first | second))
            def _():
                arrive(rsr.at[0, k, 1 - core], r_recv.at[1 + k])

    def finish():
        for k in range(2):
            for half in range(2):
                rows, columns = slice(192 * half, 192 * half + 192), slice(128 * k, 128 * k + 128)
                total = mid[tp, rows, columns].astype(F32)
                for hops in range(4):
                    total = total + rsr[hops, k, half].astype(F32)
                out_ref[rows, columns] = total.astype(BF)

    def drain():
        for item in range(3):
            sent(bufs[item].at[:, pl.ds(0, 3), 0], ring_send.at[item])
            sent(bufs[item].at[:, pl.ds(0, 3)], ring_send.at[3 + item])
        for which in range(3):
            sent(whole[which].at[pl.ds(0, 7)], x_send.at[which])
        sent(hid, h_send.at[0])
        sent(pps.at[pl.ds(0, 14)], p_send.at[0])
        some = late(0, 0) | late(0, 1) | late(1, 0) | late(1, 1)
        pl.when(some)(lambda: sent(rss.at[pl.ds(0, 13)], r_send.at[0]))
        pl.when(jnp.logical_not(some))(lambda: sent(rss.at[pl.ds(0, 12)], r_send.at[0]))
        pl.when(jnp.logical_not(route(step, step)[3]))(lambda: sent(last, r_send.at[1]))

    collect()
    finish()
    drain()


def local(activations, norm_gain, qw, kw, vw, gw, ow, mlp_gain, uw, dw):
    cosine, sine = rotary_tables()
    operands = (
        activations, norm_gain.reshape(1, D), qw.T, kw.T, vw.T, gw.T, ow, mlp_gain.reshape(1, D), uw, dw,
        jnp.asarray(cosine), jnp.asarray(sine),
    )
    dma = pltpu.SemaphoreType.DMA
    rows = pl.pallas_call(
        layer_kernel,
        out_shape=pltpu.VMEM((ROWS, D // 8), BF),
        in_specs=[pl.BlockSpec(memory_space=pltpu.HBM)] * len(operands),
        out_specs=pl.BlockSpec(memory_space=pltpu.VMEM),
        scratch_shapes=[
            pltpu.VMEM((2, 4, 4, 160, 128), BF),
            pltpu.VMEM((2, 4, 4, 128, 512), BF),
            pltpu.VMEM((2, 4, 4, 512, 128), BF),
            pltpu.VMEM((8, ROWS, 256), BF),
            pltpu.VMEM((8, 2, 4, 4, 32, 128), BF),
            pltpu.VMEM((8, 192, 128), BF),
            pltpu.VMEM((ROWS, D), BF),
            pltpu.VMEM((8, ROWS, 256), BF),
            pltpu.VMEM((ROWS, 1024), BF),
            pltpu.VMEM((16, 192, 128), BF),
            pltpu.VMEM((16, 192, 128), BF),
            pltpu.VMEM((16, 192, 128), BF),
            pltpu.VMEM((4, 2, 2, 192, 128), BF),
            pltpu.VMEM((4, 64, 128), BF),
            pltpu.VMEM((2, 1, D), F32),
            pltpu.VMEM((2, 128, 128), F32),
            pltpu.VMEM((ROWS, 256), F32),
            pltpu.VMEM((ROWS, 128), F32),
            pltpu.VMEM((ROWS, 512), BF),
            pltpu.VMEM((16, ROWS, 128), F32),
            pltpu.VMEM((ROWS, 1024), BF),
            pltpu.VMEM((2, 512, 128), BF),
            pltpu.VMEM((2, 192, 128), BF),
            dma((7,)), dma((6,)), dma((6,)), dma((12,)), dma((3,)), dma((12,)), dma((1,)), dma((6,)), dma((2,)), dma((3,)), dma((1,)), dma((1,)),
        ],
        compiler_params=pltpu.CompilerParams(
            collective_id=0, has_side_effects=True, vmem_limit_bytes=56 * 1024 * 1024
        ),
        name="layer",
    )(*operands)
    return rows


def solution(mesh):
    in_specs = (
        P(("rep", "fs"), "tp"), P(), P("fs", "tp"), P("fs", "tp"), P("fs", "tp"), P("fs", "tp"), P("tp", "fs"), P(),
        P("fs", "tp"), P("tp", "fs"),
    )
    return jax.shard_map(local, mesh=mesh, in_specs=in_specs, out_specs=P(("rep", "fs"), "tp"), check_vma=False)
```

```python
import numpy as np
import jax
import jax.numpy as jnp
from jax import lax
from jax.experimental import pallas as pl
from jax.experimental.pallas import tpu as pltpu
from jax.sharding import PartitionSpec as P

HEADS = 8
HEAD_DIM = 64
SEQ_LEN = 128
EPSILON = 1e-06
ROWS = 384
D = 2048
NX = 4
BF = jnp.bfloat16
F32 = jnp.float32
MESH = pl.DeviceIdType.MESH
ATTN, UP, DOWN = 0, 1, 2
ORDER = ((0, 1, 2, -1), (2, -1, 0, 1))


def rotary_tables():
    half = HEAD_DIM // 2
    position = np.arange(SEQ_LEN, dtype=np.float32)
    freqs = np.float32(10000.0) ** (-np.arange(half, dtype=np.float32) / np.float32(half))
    angle = position[:, None] * freqs[None, :].astype(np.float32)
    cosine, sine = np.cos(angle), np.sin(angle)
    scale = np.float32(HEAD_DIM**-0.5)
    c = np.concatenate([cosine, cosine, cosine * scale, cosine * scale], axis=1)
    s = np.concatenate([-sine, sine, -sine * scale, sine * scale], axis=1)
    return c.astype(np.float32), s.astype(np.float32)


def log_gammas():
    head = np.arange(HEADS, dtype=np.float32)
    exponent = np.float32(5.0) + np.float32(4.0) * head / np.float32(HEADS - 1)
    return np.log(1.0 - np.power(2.0, -exponent.astype(np.float64)))


def lanes(shape):
    return lax.broadcasted_iota(jnp.int32, shape, len(shape) - 1)


def layer_kernel(
    act_hbm, ng_hbm, qw_hbm, kw_hbm, vw_hbm, gw_hbm, ow_hbm, mg_hbm, uw_hbm, dw_hbm, cos_hbm, sin_hbm,
    out_ref,
    attn, upb, dnb, xall, wo, ret, wide, mid, hid, pps, ppr, rss, rsr,
    small, gains, tables, qkvg, gat, lhs, acc,
    hid2, ext, last, local_sem, ring_send, first_recv, second_recv, x_send, x_recv, p_send, p_recv, r_send, r_recv, h_send, h_recv,
):
    rep, fs, tp = lax.axis_index("rep"), lax.axis_index("fs"), lax.axis_index("tp")
    zl, y = lax.div(fs, 4), lax.rem(fs, 4)
    x, core = lax.div(tp, 2), lax.rem(tp, 2)
    zg = rep * 4 + zl

    def y_device(step):
        return {"fs": zl * 4 + lax.rem(y + step + 4, 4)}

    def z_device(step):
        other = lax.rem(zg + step + 8, 8)
        return {"rep": lax.div(other, 4), "fs": lax.rem(other, 4) * 4 + y}

    def x_index(step, c=core):
        return lax.rem(x + step + 4, 4) * 2 + c

    def x_device(step):
        return {"tp": x_index(step)}

    partner = {"tp": x * 2 + (1 - core)}

    barrier = pltpu.get_barrier_semaphore()
    peers = [y_device(1), y_device(-1), z_device(1), z_device(-1), x_device(1), x_device(-1), partner]
    for peer in peers:
        pl.semaphore_signal(barrier, inc=1, device_id=peer, device_id_type=MESH)

    loads = (
        (qw_hbm, small.at[0], 0),
        (kw_hbm, small.at[1], 0),
        (vw_hbm, small.at[2], 0),
        (gw_hbm, small.at[3], 0),
        (ow_hbm.at[pl.ds(0, 32)], attn.at[0, zl, y, pl.ds(128, 32)], 1),
        (ow_hbm.at[pl.ds(32, 32)], attn.at[1, zl, y, pl.ds(128, 32)], 1),
        (act_hbm, xall.at[tp], 2),
        (uw_hbm.at[:, pl.ds(0, 512)], upb.at[0, zl, y], 3),
        (uw_hbm.at[:, pl.ds(512, 512)], upb.at[1, zl, y], 3),
        (dw_hbm.at[pl.ds(0, 512)], dnb.at[0, zl, y], 4),
        (dw_hbm.at[pl.ds(512, 512)], dnb.at[1, zl, y], 4),
        (ng_hbm, gains.at[0], 5),
        (mg_hbm, gains.at[1], 5),
        (cos_hbm, tables.at[0], 6),
        (sin_hbm, tables.at[1], 6),
    )
    for src, dst, n in loads:
        pltpu.make_async_copy(src, dst, local_sem.at[n]).start()

    def loaded(region, n):
        pltpu.make_async_copy(region, region, local_sem.at[n]).wait()

    loaded(small, 0)
    loaded(attn.at[0, 0, 0, pl.ds(0, 64)], 1)
    for h in range(2):
        attn[h, zl, y, 0:128, :] = small[2 * h : 2 * h + 2].reshape(128, 128).astype(F32).T.astype(BF)
    pl.semaphore_wait(barrier, len(peers))

    def remote(src, dst, send_sem, recv_sem, device):
        return pltpu.make_async_remote_copy(
            src_ref=src, dst_ref=dst, send_sem=send_sem, recv_sem=recv_sem, device_id=device, device_id_type=MESH
        )

    def send(src, dst, send_sem, recv_sem, device):
        remote(src, dst, send_sem, recv_sem, device).start()

    def arrive(region, recv_sem):
        remote(region, region, r_send.at[0], recv_sem, partner).wait_recv()

    def sent(region, send_sem):
        remote(region, region, send_sem, r_recv.at[0], partner).wait_send()

    bufs = (attn, upb, dnb)
    depth = (160, 128, 512)

    def block(item, half, dz, dy):
        return bufs[item].at[half, lax.rem(zl + dz + 4, 4), lax.rem(y + dy + 4, 4)]

    def along_y(half, phase):
        return (half + phase) % 2 == 0

    def piece(item, half, step, p):
        cut = depth[item] // 2
        dz, dy = (0, step) if half == 0 else (step, 0)
        return block(item, half, dz, dy).at[pl.ds(p * cut, cut)]

    def ring_device(half, phase, step):
        return y_device(step) if along_y(half, phase) else z_device(step)

    def first_start(item):
        for n in range(2):
            for half in range(2):
                for d in range(2):
                    ref = piece(item, half, 0, n if d == 0 else 1 - n)
                    send(ref, ref, ring_send.at[item], first_recv.at[2 * item + n], ring_device(half, 0, 1 - 2 * d))

    def first_forward(item):
        arrive(bufs[item].at[0, 0, pl.ds(0, 2)], first_recv.at[2 * item])
        for half in range(2):
            for d in range(2):
                to = 1 - 2 * d
                ref = piece(item, half, -to, d)
                send(ref, ref, ring_send.at[item], first_recv.at[2 * item + 1], ring_device(half, 0, to))

    def first_rest(item):
        arrive(bufs[item].at[0, 0], first_recv.at[2 * item + 1])

    def second_block(item, half, step, d, n):
        across = ORDER[d][n]
        return block(item, half, step, across) if half == 0 else block(item, half, across, step)

    def second_sem(item, n, far):
        if n < 2 and not far:
            return second_recv.at[2 * item + n]
        return second_recv.at[6 + item] if item < DOWN else second_recv.at[8 + n]

    def second_start(item, *which):
        for n in which:
            for half in range(2):
                for d in range(2):
                    ref = second_block(item, half, 0, d, n)
                    send(ref, ref, ring_send.at[3 + item], second_sem(item, n, False), ring_device(half, 1, 1 - 2 * d))

    def second_forward(item, *which):
        for n in which:
            arrive(bufs[item].at[0, 0], second_sem(item, n, False))
            for half in range(2):
                for d in range(2):
                    to = 1 - 2 * d
                    ref = second_block(item, half, -to, d, n)
                    send(ref, ref, ring_send.at[3 + item], second_sem(item, n, True), ring_device(half, 1, to))

    def second_forward_on(c, item, n):
        @pl.when(core == c)
        def _():
            second_forward(item, n)

    def second_rest(item):
        arrive(bufs[item].at[0], second_sem(item, 0, True))

    def second_four(item, n, far):
        arrive(bufs[item].at[0, 0], second_sem(item, n, far))

    def x_piece(which, t, p):
        if which == 0:
            return xall.at[t, pl.ds(p * 192, 192)]
        if which == 1:
            return wo.at[t, p]
        return ret.at[t, pl.ds(p * 96, 96)]

    whole = (xall, wo, ret)

    def x_sem(which, kind):
        return x_recv.at[which * 4 + kind]

    def hand_over(which, place, p):
        ref = x_piece(which, x_index((0, -1, 1, 2)[place]), p)
        send(ref, ref, x_send.at[which], x_sem(which, 3), partner)

    def x_start(which):
        for n in range(2):
            for d in range(2):
                p = n if d == 0 else 1 - n
                dst = x_piece(which, tp, p)
                src = attn.at[p, :, :, pl.ds(128, 32)] if which == 1 else dst
                send(src, dst, x_send.at[which], x_sem(which, n), x_device(1 - 2 * d))
        for p in range(2):
            dst = x_piece(which, tp, p)
            src = attn.at[p, :, :, pl.ds(128, 32)] if which == 1 else dst
            send(src, dst, x_send.at[which], x_sem(which, 3), partner)

    def x_forward(which):
        arrive(whole[which].at[0], x_sem(which, 0))
        for d in range(2):
            to = 1 - 2 * d
            ref = x_piece(which, x_index(-to), d)
            send(ref, ref, x_send.at[which], x_sem(which, 2), x_device(to))
            hand_over(which, 1 + d, d)

    def x_near(which):
        arrive(whole[which].at[0], x_sem(which, 1))
        for d in range(2):
            hand_over(which, 1 + d, 1 - d)

    def x_far(which):
        arrive(whole[which].at[0], x_sem(which, 2))
        for d in range(2):
            hand_over(which, 3, d)

    def x_partner(which):
        arrive(whole[which].at[pl.ds(0, 4)], x_sem(which, 3))

    def norm_rows(source, gain):
        @pl.loop(0, ROWS // 16)
        def _(i):
            rows = pl.ds(pl.multiple_of(i * 16, 16), 16)
            blocks = [source[t, rows, :].astype(F32) for t in range(8)]
            squares = blocks[0] * blocks[0]
            for b in blocks[1:]:
                squares = squares + b * b
            scale = lax.rsqrt(jnp.sum(squares, axis=-1, keepdims=True) * (1.0 / D) + EPSILON)
            for t in range(8):
                columns = slice(256 * t, 256 * t + 256)
                wide[rows, columns] = (blocks[t] * scale * gains[gain, :, columns]).astype(BF)

    first_start(ATTN)
    loaded(xall.at[0], 2)
    x_start(0)
    loaded(upb.at[0, 0, pl.ds(0, 2)], 3)
    first_start(UP)
    loaded(dnb.at[0, 0, pl.ds(0, 2)], 4)
    loaded(gains, 5)
    loaded(tables, 6)
    first_forward(ATTN)
    first_forward(UP)
    x_forward(0)
    first_rest(ATTN)
    second_start(ATTN, 0, 1, 2, 3)
    first_start(DOWN)
    x_near(0)
    second_forward(ATTN, 0, 1)
    first_rest(UP)
    second_start(UP, 0)
    x_far(0)
    x_partner(0)
    norm_rows(xall, 0)
    first_forward(DOWN)
    second_start(UP, 1, 2, 3)
    second_rest(ATTN)
    x_start(1)

    weights = jnp.concatenate([attn[h, :, :, 0:128, :].reshape(D, 128) for h in range(2)], axis=1)
    qkvg[...] = jnp.dot(wide[...], weights, preferred_element_type=F32)
    log_gamma = jnp.float32(0.0)
    for h, value in enumerate(log_gammas()):
        log_gamma = jnp.where(tp == h, jnp.float32(value), log_gamma)
    square = (SEQ_LEN, SEQ_LEN)
    distance = (lax.broadcasted_iota(jnp.int32, square, 0) - lanes(square)).astype(F32)
    decay = jnp.where(distance >= 0, jnp.exp(jnp.maximum(distance, 0.0) * log_gamma), 0.0)
    lane = lanes(square)
    first, low = lax.rem(lane, 64) < 32, lane < 64
    for s in range(3):
        rows = slice(SEQ_LEN * s, SEQ_LEN * (s + 1))
        qk, vg = qkvg[rows, 0:128], qkvg[rows, 128:256]
        other = jnp.where(first, pltpu.roll(qk, 96, 1), pltpu.roll(qk, 32, 1))
        turned = (qk * tables[0] + other * tables[1]).astype(BF).astype(F32)
        queries = jnp.where(low, turned, 0.0).astype(BF)
        keys = pltpu.roll(turned, 64, 1).astype(BF)
        scores = lax.dot_general(queries, keys, (((1,), (1,)), ((), ())), preferred_element_type=F32)
        mixed = jnp.dot((scores * decay).astype(BF), vg.astype(BF), preferred_element_type=F32)
        mixed = jnp.where(low, mixed, 0.0)
        mean = jnp.sum(mixed, axis=-1, keepdims=True) * (1.0 / HEAD_DIM)
        centred = jnp.where(low, mixed - mean, 0.0)
        variance = jnp.sum(centred * centred, axis=-1, keepdims=True) * (1.0 / HEAD_DIM)
        gate = pltpu.roll(vg, 64, 1)
        gat[rows, :] = centred * lax.rsqrt(variance + EPSILON) * (gate / (1.0 + jnp.exp(-gate)))
    low = lanes((192, 128)) < 64
    ret[tp] = jnp.where(low, gat[0:192, :], pltpu.roll(gat[192:384, :], 64, 1)).astype(BF)
    x_start(2)
    for h in range(2):
        wo[tp, h] = attn[h, :, :, 128:160, :]
    x_forward(1)
    second_forward(UP, 0)
    x_forward(2)
    second_forward(UP, 1)
    first_rest(DOWN)
    second_start(DOWN, 0, 1)
    x_near(2)
    x_near(1)
    x_far(2)
    x_far(1)
    x_partner(2)
    x_partner(1)

    for j in range(4):
        a, b = ret[2 * j].astype(F32), ret[2 * j + 1].astype(F32)
        lhs[0:192, 128 * j : 128 * j + 128] = jnp.where(low, a, pltpu.roll(b, 64, 1)).astype(BF)
        lhs[192:384, 128 * j : 128 * j + 128] = jnp.where(low, pltpu.roll(a, 64, 1), b).astype(BF)

    @pl.loop(0, 8)
    def _(t):
        z0, y0 = lax.div(t, 2), lax.rem(t, 2) * 2
        columns = [wo[:, :, z0, y0 + k].reshape(HEADS * HEAD_DIM, 128) for k in range(2)]
        branch = jnp.dot(lhs[...], jnp.concatenate(columns, axis=1), preferred_element_type=F32)
        mid[t] = (xall[t].astype(F32) + branch).astype(BF)

    norm_rows(mid, 1)
    second_rest(UP)
    second_forward_on(1, DOWN, 0)
    for h in range(2):
        raw = jnp.dot(wide[...], upb[h].reshape(D, 512), preferred_element_type=F32)
        raw = jnp.maximum(raw, 0.0)
        hid[:, 512 * h : 512 * h + 512] = (raw * raw).astype(BF)
    second_forward_on(0, DOWN, 0)
    send(hid, hid2, h_send.at[0], h_recv.at[0], partner)

    def number(dz, dy):
        return (dz + 1) * 4 + dy + 1

    def last_start():
        for half in range(2):
            for d in range(2):
                ref, sem = second_block(DOWN, half, 0, d, 3), second_sem(DOWN, 3, False)
                there = ring_device(half, 1, 1 - 2 * d)

                @pl.when(core == d)
                def _():
                    send(ref, ref, ring_send.at[3 + DOWN], sem, there)

                @pl.when(core != d)
                def _():
                    send(ref, ext.at[half], ring_send.at[3 + DOWN], sem, {**there, "tp": x * 2 + d})

    def on_core(c, step):
        pl.when(core == c)(step)

    begun = set()

    def products(pairs):
        done = []
        for half, blocks in pairs:
            columns = jnp.concatenate([block(DOWN, half, dz, dy)[...] for dz, dy in blocks], axis=1)
            both = jnp.dot(hid[:, 512 * half : 512 * half + 512], columns, preferred_element_type=F32)
            for k, at in enumerate(blocks):
                value, n = both[:, 128 * k : 128 * k + 128], number(*at)
                if at in begun:
                    acc[n] += value
                    done.append(at)
                else:
                    acc[n] = value
                    begun.add(at)
        return done

    def rows_of(c):
        return pl.ds(pl.multiple_of(c * 192, 64), 192)

    def swap(blocks, group):
        for at in blocks:
            n = number(*at)
            pps[n] = acc[n, rows_of(1 - core), :].astype(BF)
            send(pps.at[n], ppr.at[n], p_send.at[0], p_recv.at[group], partner)


    def route(dz, dy):
        z_to, y_to = lax.rem(zl + dz + 4, 4), lax.rem(y + dy + 4, 4)
        c_to, k = lax.div(y_to, 2), lax.rem(y_to, 2)
        hops = lax.rem(z_to - x + 4, 4)
        return {"tp": z_to * 2 + c_to}, k, hops, (hops == 0) & (c_to == core), lax.div(3 - hops, 3) * (1 + k)

    def deliver(blocks, group):
        arrive(ppr.at[pl.ds(0, len(blocks))], p_recv.at[group])
        for at in blocks:
            n = number(*at)
            owner, k, hops, own, sem = route(*at)
            total = (acc[n, rows_of(core), :] + ppr[n].astype(F32)).astype(BF)
            rss[n] = total

            @pl.when(jnp.logical_not(own))
            def _():
                send(rss.at[n], rsr.at[hops, k, core], r_send.at[0], r_recv.at[sem], owner)

            @pl.when(own)
            def _():
                rsr[0, k, core] = total

    step = 2 * core - 1

    def deliver_last():
        owner, k, hops, own, sem = route(step, step)
        z_from, y_from = lax.rem(zl + step + 4, 4), lax.rem(y + step + 4, 4)
        mine = jnp.concatenate([dnb[0, z_from, y_from], dnb[1, z_from, y_from]], axis=0)
        other = ext[...].reshape(1024, 128)
        for half in range(2):
            rows = slice(192 * half, 192 * half + 192)
            total = jnp.dot(hid[rows, :], mine, preferred_element_type=F32)
            total = (total + jnp.dot(hid2[rows, :], other, preferred_element_type=F32)).astype(BF)
            last[half] = total

            @pl.when(jnp.logical_not(own))
            def _():
                send(last.at[half], rsr.at[hops, k, half], r_send.at[1], r_recv.at[sem], owner)

            @pl.when(own)
            def _():
                rsr[0, k, half] = total

    def arrivals(n, far):
        step = (2, 2) if far else (-1, 1)
        rows = [(step[d], ORDER[d][n]) for d in range(2)]
        columns = [(ORDER[d][n], step[d]) for d in range(2)]
        return [(0, rows), (1, columns)]

    own = [(0, [(0, 0), (0, 1)]), (0, [(0, -1), (0, 2)]), (1, [(0, 0), (1, 0)]), (1, [(-1, 0), (2, 0)])]
    def deliver_on(c, blocks, group):
        @pl.when(core == c)
        def _():
            deliver(blocks, group)

    s0 = products(own)
    swap(s0, 0)
    s1 = products(arrivals(0, False))
    swap(s1, 1)
    second_forward(DOWN, 1)
    on_core(0, lambda: second_start(DOWN, 2))
    s2 = products(arrivals(1, False))
    swap(s2, 2)
    deliver_on(0, s0, 0)
    deliver_on(0, s1, 1)
    second_four(DOWN, 0, True)
    on_core(1, lambda: second_start(DOWN, 2))
    on_core(0, last_start)
    s3 = products(arrivals(0, True))
    swap(s3, 3)
    deliver_on(1, s0, 0)
    deliver_on(1, s1, 1)
    deliver(s2, 2)
    deliver_on(0, s3, 3)
    second_four(DOWN, 1, True)
    on_core(1, last_start)
    s4 = products(arrivals(1, True))
    swap(s4, 4)
    deliver_on(1, s3, 3)
    deliver_on(0, s4, 4)
    second_four(DOWN, 2, False)
    s5 = products(arrivals(2, False))
    swap(s5, 5)
    deliver_on(1, s4, 4)
    deliver_on(0, s5, 5)
    arrive(hid2, h_recv.at[0])
    second_four(DOWN, 3, False)
    deliver_last()
    deliver_on(1, s5, 5)

    def late(k, c):
        dz, dy = lax.rem(x - zl + 4, 4), lax.rem(core * 2 + k - y + 4, 4)
        return (dz == (2 * c + 3) % 4) & (dy == (2 * c + 3) % 4)

    def collect():
        arrive(rss.at[pl.ds(0, 12)], r_recv.at[0])
        for k in range(2):
            first, second = late(k, 0), late(k, 1)

            @pl.when((first & (core == 1)) | (second & (core == 0)))
            def _():
                arrive(rsr.at[0, k], r_recv.at[1 + k])

            @pl.when(jnp.logical_not(first | second))
            def _():
                arrive(rsr.at[0, k, 1 - core], r_recv.at[1 + k])

    def finish():
        for k in range(2):
            for half in range(2):
                rows, columns = slice(192 * half, 192 * half + 192), slice(128 * k, 128 * k + 128)
                total = mid[tp, rows, columns].astype(F32)
                for hops in range(4):
                    total = total + rsr[hops, k, half].astype(F32)
                out_ref[rows, columns] = total.astype(BF)

    def drain():
        for item in range(3):
            sent(bufs[item].at[:, pl.ds(0, 3), 0], ring_send.at[item])
            sent(bufs[item].at[:, pl.ds(0, 3)], ring_send.at[3 + item])
        for which in range(3):
            sent(whole[which].at[pl.ds(0, 7)], x_send.at[which])
        sent(hid, h_send.at[0])
        sent(pps.at[pl.ds(0, 14)], p_send.at[0])
        some = late(0, 0) | late(0, 1) | late(1, 0) | late(1, 1)
        pl.when(some)(lambda: sent(rss.at[pl.ds(0, 13)], r_send.at[0]))
        pl.when(jnp.logical_not(some))(lambda: sent(rss.at[pl.ds(0, 12)], r_send.at[0]))
        pl.when(jnp.logical_not(route(step, step)[3]))(lambda: sent(last, r_send.at[1]))

    collect()
    finish()
    drain()


def local(activations, norm_gain, qw, kw, vw, gw, ow, mlp_gain, uw, dw):
    cosine, sine = rotary_tables()
    operands = (
        activations, norm_gain.reshape(1, D), qw.T, kw.T, vw.T, gw.T, ow, mlp_gain.reshape(1, D), uw, dw,
        jnp.asarray(cosine), jnp.asarray(sine),
    )
    dma = pltpu.SemaphoreType.DMA
    rows = pl.pallas_call(
        layer_kernel,
        out_shape=pltpu.VMEM((ROWS, D // 8), BF),
        in_specs=[pl.BlockSpec(memory_space=pltpu.HBM)] * len(operands),
        out_specs=pl.BlockSpec(memory_space=pltpu.VMEM),
        scratch_shapes=[
            pltpu.VMEM((2, 4, 4, 160, 128), BF),
            pltpu.VMEM((2, 4, 4, 128, 512), BF),
            pltpu.VMEM((2, 4, 4, 512, 128), BF),
            pltpu.VMEM((8, ROWS, 256), BF),
            pltpu.VMEM((8, 2, 4, 4, 32, 128), BF),
            pltpu.VMEM((8, 192, 128), BF),
            pltpu.VMEM((ROWS, D), BF),
            pltpu.VMEM((8, ROWS, 256), BF),
            pltpu.VMEM((ROWS, 1024), BF),
            pltpu.VMEM((16, 192, 128), BF),
            pltpu.VMEM((16, 192, 128), BF),
            pltpu.VMEM((16, 192, 128), BF),
            pltpu.VMEM((4, 2, 2, 192, 128), BF),
            pltpu.VMEM((4, 64, 128), BF),
            pltpu.VMEM((2, 1, D), F32),
            pltpu.VMEM((2, 128, 128), F32),
            pltpu.VMEM((ROWS, 256), F32),
            pltpu.VMEM((ROWS, 128), F32),
            pltpu.VMEM((ROWS, 512), BF),
            pltpu.VMEM((16, ROWS, 128), F32),
            pltpu.VMEM((ROWS, 1024), BF),
            pltpu.VMEM((2, 512, 128), BF),
            pltpu.VMEM((2, 192, 128), BF),
            dma((7,)), dma((6,)), dma((6,)), dma((12,)), dma((3,)), dma((12,)), dma((1,)), dma((6,)), dma((2,)), dma((3,)), dma((1,)), dma((1,)),
        ],
        compiler_params=pltpu.CompilerParams(
            collective_id=0, has_side_effects=True, vmem_limit_bytes=56 * 1024 * 1024
        ),
        name="layer",
    )(*operands)
    return rows


def solution(mesh):
    in_specs = (
        P(("rep", "fs"), "tp"), P(), P("fs", "tp"), P("fs", "tp"), P("fs", "tp"), P("fs", "tp"), P("tp", "fs"), P(),
        P("fs", "tp"), P("tp", "fs"),
    )
    return jax.shard_map(local, mesh=mesh, in_specs=in_specs, out_specs=P(("rep", "fs"), "tp"), check_vma=False)
```

```python
import numpy as np
import jax
import jax.numpy as jnp
from jax import lax
from jax.experimental import pallas as pl
from jax.experimental.pallas import tpu as pltpu
from jax.sharding import PartitionSpec as P

HEADS = 8
HEAD_DIM = 64
SEQ_LEN = 128
EPSILON = 1e-06
ROWS = 384
D = 2048
NX = 4
BF = jnp.bfloat16
F32 = jnp.float32
MESH = pl.DeviceIdType.MESH
ATTN, UP, DOWN = 0, 1, 2
ORDER = ((0, 1, 2, -1), (2, -1, 0, 1))


def rotary_tables():
    half = HEAD_DIM // 2
    position = np.arange(SEQ_LEN, dtype=np.float32)
    freqs = np.float32(10000.0) ** (-np.arange(half, dtype=np.float32) / np.float32(half))
    angle = position[:, None] * freqs[None, :].astype(np.float32)
    cosine, sine = np.cos(angle), np.sin(angle)
    scale = np.float32(HEAD_DIM**-0.5)
    c = np.concatenate([cosine, cosine, cosine * scale, cosine * scale], axis=1)
    s = np.concatenate([-sine, sine, -sine * scale, sine * scale], axis=1)
    return c.astype(np.float32), s.astype(np.float32)


def log_gammas():
    head = np.arange(HEADS, dtype=np.float32)
    exponent = np.float32(5.0) + np.float32(4.0) * head / np.float32(HEADS - 1)
    return np.log(1.0 - np.power(2.0, -exponent.astype(np.float64)))


def lanes(shape):
    return lax.broadcasted_iota(jnp.int32, shape, len(shape) - 1)


def layer_kernel(
    act_hbm, ng_hbm, qw_hbm, kw_hbm, vw_hbm, gw_hbm, ow_hbm, mg_hbm, uw_hbm, dw_hbm, cos_hbm, sin_hbm,
    out_ref,
    attn, upb, dnb, xall, wo, ret, wide, mid, hid, pps, ppr, rss, rsr,
    small, gains, tables, qkvg, gat, lhs, acc,
    hid2, ext, last, local_sem, ring_send, first_recv, second_recv, x_send, x_recv, p_send, p_recv, r_send, r_recv, h_send, h_recv,
):
    rep, fs, tp = lax.axis_index("rep"), lax.axis_index("fs"), lax.axis_index("tp")
    zl, y = lax.div(fs, 4), lax.rem(fs, 4)
    x, core = lax.div(tp, 2), lax.rem(tp, 2)
    zg = rep * 4 + zl

    def y_device(step):
        return {"fs": zl * 4 + lax.rem(y + step + 4, 4)}

    def z_device(step):
        other = lax.rem(zg + step + 8, 8)
        return {"rep": lax.div(other, 4), "fs": lax.rem(other, 4) * 4 + y}

    def x_index(step, c=core):
        return lax.rem(x + step + 4, 4) * 2 + c

    def x_device(step):
        return {"tp": x_index(step)}

    partner = {"tp": x * 2 + (1 - core)}

    barrier = pltpu.get_barrier_semaphore()
    peers = [y_device(1), y_device(-1), z_device(1), z_device(-1), x_device(1), x_device(-1), partner]
    for peer in peers:
        pl.semaphore_signal(barrier, inc=1, device_id=peer, device_id_type=MESH)

    loads = (
        (qw_hbm, small.at[0], 0),
        (kw_hbm, small.at[1], 0),
        (vw_hbm, small.at[2], 0),
        (gw_hbm, small.at[3], 0),
        (ow_hbm.at[pl.ds(0, 32)], attn.at[0, zl, y, pl.ds(128, 32)], 1),
        (ow_hbm.at[pl.ds(32, 32)], attn.at[1, zl, y, pl.ds(128, 32)], 1),
        (act_hbm, xall.at[tp], 2),
        (uw_hbm.at[:, pl.ds(0, 512)], upb.at[0, zl, y], 3),
        (uw_hbm.at[:, pl.ds(512, 512)], upb.at[1, zl, y], 3),
        (dw_hbm.at[pl.ds(0, 512)], dnb.at[0, zl, y], 4),
        (dw_hbm.at[pl.ds(512, 512)], dnb.at[1, zl, y], 4),
        (ng_hbm, gains.at[0], 5),
        (mg_hbm, gains.at[1], 5),
        (cos_hbm, tables.at[0], 6),
        (sin_hbm, tables.at[1], 6),
    )
    for src, dst, n in loads:
        pltpu.make_async_copy(src, dst, local_sem.at[n]).start()

    def loaded(region, n):
        pltpu.make_async_copy(region, region, local_sem.at[n]).wait()

    loaded(small, 0)
    loaded(attn.at[0, 0, 0, pl.ds(0, 64)], 1)
    for h in range(2):
        attn[h, zl, y, 0:128, :] = small[2 * h : 2 * h + 2].reshape(128, 128).astype(F32).T.astype(BF)
    pl.semaphore_wait(barrier, len(peers))

    def remote(src, dst, send_sem, recv_sem, device):
        return pltpu.make_async_remote_copy(
            src_ref=src, dst_ref=dst, send_sem=send_sem, recv_sem=recv_sem, device_id=device, device_id_type=MESH
        )

    def send(src, dst, send_sem, recv_sem, device):
        remote(src, dst, send_sem, recv_sem, device).start()

    def arrive(region, recv_sem):
        remote(region, region, r_send.at[0], recv_sem, partner).wait_recv()

    def sent(region, send_sem):
        remote(region, region, send_sem, r_recv.at[0], partner).wait_send()

    bufs = (attn, upb, dnb)
    depth = (160, 128, 512)

    def block(item, half, dz, dy):
        return bufs[item].at[half, lax.rem(zl + dz + 4, 4), lax.rem(y + dy + 4, 4)]

    def along_y(half, phase):
        return (half + phase) % 2 == 0

    def piece(item, half, step, p):
        cut = depth[item] // 2
        dz, dy = (0, step) if half == 0 else (step, 0)
        return block(item, half, dz, dy).at[pl.ds(p * cut, cut)]

    def ring_device(half, phase, step):
        return y_device(step) if along_y(half, phase) else z_device(step)

    def first_start(item):
        for n in range(2):
            for half in range(2):
                for d in range(2):
                    ref = piece(item, half, 0, n if d == 0 else 1 - n)
                    send(ref, ref, ring_send.at[item], first_recv.at[2 * item + n], ring_device(half, 0, 1 - 2 * d))

    def first_forward(item):
        arrive(bufs[item].at[0, 0, pl.ds(0, 2)], first_recv.at[2 * item])
        for half in range(2):
            for d in range(2):
                to = 1 - 2 * d
                ref = piece(item, half, -to, d)
                send(ref, ref, ring_send.at[item], first_recv.at[2 * item + 1], ring_device(half, 0, to))

    def first_rest(item):
        arrive(bufs[item].at[0, 0], first_recv.at[2 * item + 1])

    def second_block(item, half, step, d, n):
        across = ORDER[d][n]
        return block(item, half, step, across) if half == 0 else block(item, half, across, step)

    def second_sem(item, n, far):
        if n < 2 and not far:
            return second_recv.at[2 * item + n]
        return second_recv.at[6 + item] if item < DOWN else second_recv.at[8 + n]

    def second_start(item, *which):
        for n in which:
            for half in range(2):
                for d in range(2):
                    ref = second_block(item, half, 0, d, n)
                    send(ref, ref, ring_send.at[3 + item], second_sem(item, n, False), ring_device(half, 1, 1 - 2 * d))

    def second_forward(item, *which):
        for n in which:
            arrive(bufs[item].at[0, 0], second_sem(item, n, False))
            for half in range(2):
                for d in range(2):
                    to = 1 - 2 * d
                    ref = second_block(item, half, -to, d, n)
                    send(ref, ref, ring_send.at[3 + item], second_sem(item, n, True), ring_device(half, 1, to))

    def second_forward_on(c, item, n):
        @pl.when(core == c)
        def _():
            second_forward(item, n)

    def second_rest(item):
        arrive(bufs[item].at[0], second_sem(item, 0, True))

    def second_four(item, n, far):
        arrive(bufs[item].at[0, 0], second_sem(item, n, far))

    def x_piece(which, t, p):
        if which == 0:
            return xall.at[t, pl.ds(p * 192, 192)]
        if which == 1:
            return wo.at[t, p]
        return ret.at[t, pl.ds(p * 96, 96)]

    whole = (xall, wo, ret)

    def x_sem(which, kind):
        return x_recv.at[which * 4 + kind]

    def hand_over(which, place, p):
        ref = x_piece(which, x_index((0, -1, 1, 2)[place]), p)
        send(ref, ref, x_send.at[which], x_sem(which, 3), partner)

    def x_start(which):
        for n in range(2):
            for d in range(2):
                p = n if d == 0 else 1 - n
                dst = x_piece(which, tp, p)
                src = attn.at[p, :, :, pl.ds(128, 32)] if which == 1 else dst
                send(src, dst, x_send.at[which], x_sem(which, n), x_device(1 - 2 * d))
        for p in range(2):
            dst = x_piece(which, tp, p)
            src = attn.at[p, :, :, pl.ds(128, 32)] if which == 1 else dst
            send(src, dst, x_send.at[which], x_sem(which, 3), partner)

    def x_forward(which):
        arrive(whole[which].at[0], x_sem(which, 0))
        for d in range(2):
            to = 1 - 2 * d
            ref = x_piece(which, x_index(-to), d)
            send(ref, ref, x_send.at[which], x_sem(which, 2), x_device(to))
            hand_over(which, 1 + d, d)

    def x_near(which):
        arrive(whole[which].at[0], x_sem(which, 1))
        for d in range(2):
            hand_over(which, 1 + d, 1 - d)

    def x_far(which):
        arrive(whole[which].at[0], x_sem(which, 2))
        for d in range(2):
            hand_over(which, 3, d)

    def x_partner(which):
        arrive(whole[which].at[pl.ds(0, 4)], x_sem(which, 3))

    def norm_rows(source, gain):
        @pl.loop(0, ROWS // 16)
        def _(i):
            rows = pl.ds(pl.multiple_of(i * 16, 16), 16)
            blocks = [source[t, rows, :].astype(F32) for t in range(8)]
            squares = blocks[0] * blocks[0]
            for b in blocks[1:]:
                squares = squares + b * b
            scale = lax.rsqrt(jnp.sum(squares, axis=-1, keepdims=True) * (1.0 / D) + EPSILON)
            for t in range(8):
                columns = slice(256 * t, 256 * t + 256)
                wide[rows, columns] = (blocks[t] * scale * gains[gain, :, columns]).astype(BF)

    first_start(ATTN)
    loaded(xall.at[0], 2)
    x_start(0)
    loaded(upb.at[0, 0, pl.ds(0, 2)], 3)
    first_start(UP)
    loaded(dnb.at[0, 0, pl.ds(0, 2)], 4)
    loaded(gains, 5)
    loaded(tables, 6)
    first_forward(ATTN)
    first_forward(UP)
    x_forward(0)
    first_rest(ATTN)
    second_start(ATTN, 0, 1, 2, 3)
    first_start(DOWN)
    x_near(0)
    second_forward(ATTN, 0, 1)
    first_rest(UP)
    second_start(UP, 0)
    x_far(0)
    x_partner(0)
    norm_rows(xall, 0)
    first_forward(DOWN)
    second_start(UP, 1, 2, 3)
    second_rest(ATTN)
    x_start(1)

    weights = jnp.concatenate([attn[h, :, :, 0:128, :].reshape(D, 128) for h in range(2)], axis=1)
    qkvg[...] = jnp.dot(wide[...], weights, preferred_element_type=F32)
    log_gamma = jnp.float32(0.0)
    for h, value in enumerate(log_gammas()):
        log_gamma = jnp.where(tp == h, jnp.float32(value), log_gamma)
    square = (SEQ_LEN, SEQ_LEN)
    distance = (lax.broadcasted_iota(jnp.int32, square, 0) - lanes(square)).astype(F32)
    decay = jnp.where(distance >= 0, jnp.exp(jnp.maximum(distance, 0.0) * log_gamma), 0.0)
    lane = lanes(square)
    first, low = lax.rem(lane, 64) < 32, lane < 64
    for s in range(3):
        rows = slice(SEQ_LEN * s, SEQ_LEN * (s + 1))
        qk, vg = qkvg[rows, 0:128], qkvg[rows, 128:256]
        other = jnp.where(first, pltpu.roll(qk, 96, 1), pltpu.roll(qk, 32, 1))
        turned = (qk * tables[0] + other * tables[1]).astype(BF).astype(F32)
        queries = jnp.where(low, turned, 0.0).astype(BF)
        keys = pltpu.roll(turned, 64, 1).astype(BF)
        scores = lax.dot_general(queries, keys, (((1,), (1,)), ((), ())), preferred_element_type=F32)
        mixed = jnp.dot((scores * decay).astype(BF), vg.astype(BF), preferred_element_type=F32)
        mixed = jnp.where(low, mixed, 0.0)
        mean = jnp.sum(mixed, axis=-1, keepdims=True) * (1.0 / HEAD_DIM)
        centred = jnp.where(low, mixed - mean, 0.0)
        variance = jnp.sum(centred * centred, axis=-1, keepdims=True) * (1.0 / HEAD_DIM)
        gate = pltpu.roll(vg, 64, 1)
        gat[rows, :] = centred * lax.rsqrt(variance + EPSILON) * (gate / (1.0 + jnp.exp(-gate)))
    low = lanes((192, 128)) < 64
    ret[tp] = jnp.where(low, gat[0:192, :], pltpu.roll(gat[192:384, :], 64, 1)).astype(BF)
    x_start(2)
    for h in range(2):
        wo[tp, h] = attn[h, :, :, 128:160, :]
    x_forward(1)
    second_forward(UP, 0)
    x_forward(2)
    second_forward(UP, 1)
    first_rest(DOWN)
    second_start(DOWN, 0, 1)
    x_near(2)
    x_near(1)
    x_far(2)
    x_far(1)
    x_partner(2)
    x_partner(1)

    for j in range(4):
        a, b = ret[2 * j].astype(F32), ret[2 * j + 1].astype(F32)
        lhs[0:192, 128 * j : 128 * j + 128] = jnp.where(low, a, pltpu.roll(b, 64, 1)).astype(BF)
        lhs[192:384, 128 * j : 128 * j + 128] = jnp.where(low, pltpu.roll(a, 64, 1), b).astype(BF)

    @pl.loop(0, 8)
    def _(t):
        z0, y0 = lax.div(t, 2), lax.rem(t, 2) * 2
        columns = [wo[:, :, z0, y0 + k].reshape(HEADS * HEAD_DIM, 128) for k in range(2)]
        branch = jnp.dot(lhs[...], jnp.concatenate(columns, axis=1), preferred_element_type=F32)
        mid[t] = (xall[t].astype(F32) + branch).astype(BF)

    norm_rows(mid, 1)
    second_rest(UP)
    second_forward_on(1, DOWN, 0)
    for h in range(2):
        raw = jnp.dot(wide[...], upb[h].reshape(D, 512), preferred_element_type=F32)
        raw = jnp.maximum(raw, 0.0)
        hid[:, 512 * h : 512 * h + 512] = (raw * raw).astype(BF)
    second_forward_on(0, DOWN, 0)
    send(hid, hid2, h_send.at[0], h_recv.at[0], partner)

    def number(dz, dy):
        return (dz + 1) * 4 + dy + 1

    def last_start():
        for half in range(2):
            for d in range(2):
                ref, sem = second_block(DOWN, half, 0, d, 3), second_sem(DOWN, 3, False)
                there = ring_device(half, 1, 1 - 2 * d)

                @pl.when(core == d)
                def _():
                    send(ref, ref, ring_send.at[3 + DOWN], sem, there)

                @pl.when(core != d)
                def _():
                    send(ref, ext.at[half], ring_send.at[3 + DOWN], sem, {**there, "tp": x * 2 + d})

    def on_core(c, step):
        pl.when(core == c)(step)

    begun = set()

    def products(pairs):
        done = []
        for half, blocks in pairs:
            columns = jnp.concatenate([block(DOWN, half, dz, dy)[...] for dz, dy in blocks], axis=1)
            both = jnp.dot(hid[:, 512 * half : 512 * half + 512], columns, preferred_element_type=F32)
            for k, at in enumerate(blocks):
                value, n = both[:, 128 * k : 128 * k + 128], number(*at)
                if at in begun:
                    acc[n] += value
                    done.append(at)
                else:
                    acc[n] = value
                    begun.add(at)
        return done

    def rows_of(c):
        return pl.ds(pl.multiple_of(c * 192, 64), 192)

    def swap(blocks, group):
        for at in blocks:
            n = number(*at)
            pps[n, 0] = acc[n, rows_of(1 - core), :].astype(BF)
            send(pps.at[n, 0], ppr.at[n, 0], p_send.at[0], p_recv.at[group], partner)

    def give(blocks, group):
        @pl.when(core == 1)
        def _():
            for at in blocks:
                n = number(*at)
                pps[n] = acc[n].astype(BF).reshape(2, 192, 128)
                send(pps.at[n], ppr.at[n], p_send.at[1], p_recv.at[group], partner)


    def route(dz, dy):
        z_to, y_to = lax.rem(zl + dz + 4, 4), lax.rem(y + dy + 4, 4)
        c_to, k = lax.div(y_to, 2), lax.rem(y_to, 2)
        hops = lax.rem(z_to - x + 4, 4)
        return {"tp": z_to * 2 + c_to}, k, hops, (hops == 0) & (c_to == core), lax.div(3 - hops, 3) * (1 + k)

    def deliver(blocks, group):
        arrive(ppr.at[pl.ds(0, len(blocks)), 0], p_recv.at[group])
        for at in blocks:
            n = number(*at)
            owner, k, hops, own, sem = route(*at)
            total = (acc[n, rows_of(core), :] + ppr[n, 0].astype(F32)).astype(BF)
            rss[n, 0] = total

            @pl.when(jnp.logical_not(own))
            def _():
                send(rss.at[n, 0], rsr.at[hops, k, core], r_send.at[0], r_recv.at[sem], owner)

            @pl.when(own)
            def _():
                rsr[0, k, core] = total

    def deliver_whole(blocks, group):
        @pl.when(core == 0)
        def _():
            arrive(ppr.at[pl.ds(0, len(blocks))], p_recv.at[group])
            for at in blocks:
                n = number(*at)
                owner, k, hops, own, sem = route(*at)
                total = (acc[n].reshape(2, 192, 128) + ppr[n].astype(F32)).astype(BF)
                rss[n] = total

                @pl.when(jnp.logical_not(own))
                def _():
                    send(rss.at[n], rsr.at[hops, k], r_send.at[2], r_recv.at[sem], owner)

                @pl.when(own)
                def _():
                    rsr[0, k] = total

    step = 2 * core - 1

    def deliver_last():
        owner, k, hops, own, sem = route(step, step)
        z_from, y_from = lax.rem(zl + step + 4, 4), lax.rem(y + step + 4, 4)
        mine = jnp.concatenate([dnb[0, z_from, y_from], dnb[1, z_from, y_from]], axis=0)
        other = ext[...].reshape(1024, 128)
        for half in range(2):
            rows = slice(192 * half, 192 * half + 192)
            total = jnp.dot(hid[rows, :], mine, preferred_element_type=F32)
            total = (total + jnp.dot(hid2[rows, :], other, preferred_element_type=F32)).astype(BF)
            last[half] = total

            @pl.when(jnp.logical_not(own))
            def _():
                send(last.at[half], rsr.at[hops, k, half], r_send.at[1], r_recv.at[sem], owner)

            @pl.when(own)
            def _():
                rsr[0, k, half] = total

    def arrivals(n, far):
        step = (2, 2) if far else (-1, 1)
        rows = [(step[d], ORDER[d][n]) for d in range(2)]
        columns = [(ORDER[d][n], step[d]) for d in range(2)]
        return [(0, rows), (1, columns)]

    own = [(0, [(0, 0), (0, 1)]), (0, [(0, -1), (0, 2)]), (1, [(0, 0), (1, 0)]), (1, [(-1, 0), (2, 0)])]
    def deliver_on(c, blocks, group):
        @pl.when(core == c)
        def _():
            deliver(blocks, group)

    s0 = products(own)
    swap(s0, 0)
    s1 = products(arrivals(0, False))
    swap(s1, 1)
    second_forward(DOWN, 1)
    on_core(0, lambda: second_start(DOWN, 2))
    s2 = products(arrivals(1, False))
    swap(s2, 2)
    deliver_on(0, s0, 0)
    deliver_on(0, s1, 1)
    second_four(DOWN, 0, True)
    on_core(1, lambda: second_start(DOWN, 2))
    on_core(0, last_start)
    s3 = products(arrivals(0, True))
    give(s3, 3)
    deliver_on(1, s0, 0)
    deliver_on(1, s1, 1)
    deliver(s2, 2)
    deliver_whole(s3, 3)
    second_four(DOWN, 1, True)
    on_core(1, last_start)
    s4 = products(arrivals(1, True))
    give(s4, 4)
    deliver_whole(s4, 4)
    second_four(DOWN, 2, False)
    s5 = products(arrivals(2, False))
    give(s5, 5)
    deliver_whole(s5, 5)
    arrive(hid2, h_recv.at[0])
    second_four(DOWN, 3, False)
    deliver_last()

    def among(k, blocks):
        dz, dy = lax.rem(x - zl + 4, 4), lax.rem(core * 2 + k - y + 4, 4)
        found = None
        for at in blocks:
            here = (dz == at[0] % 4) & (dy == at[1] % 4)
            found = here if found is None else found | here
        return found

    halves = [among(k, s0 + s1 + s2) for k in range(2)]
    on_one = [among(k, [(1, 1)]) for k in range(2)]
    on_zero = [jnp.logical_not(halves[k] | on_one[k]) for k in range(2)]
    whole_sums = [among(k, s3 + s4 + s5) for k in range(2)]

    def collect():
        arrive(rss.at[pl.ds(0, 6)], r_recv.at[0])
        for k in range(2):

            @pl.when((on_zero[k] & (core == 1)) | (on_one[k] & (core == 0)))
            def _():
                arrive(rsr.at[0, k], r_recv.at[1 + k])

            @pl.when(halves[k])
            def _():
                arrive(rsr.at[0, k, 1 - core], r_recv.at[1 + k])

    def count(pair):
        both, some = pair[0] & pair[1], pair[0] | pair[1]
        return [jnp.logical_not(some), some & jnp.logical_not(both), both]

    def finish():
        for k in range(2):
            for half in range(2):
                rows, columns = slice(192 * half, 192 * half + 192), slice(128 * k, 128 * k + 128)
                total = mid[tp, rows, columns].astype(F32)
                for hops in range(4):
                    total = total + rsr[hops, k, half].astype(F32)
                out_ref[rows, columns] = total.astype(BF)

    def drain():
        for item in range(3):
            sent(bufs[item].at[:, pl.ds(0, 3), 0], ring_send.at[item])
            sent(bufs[item].at[:, pl.ds(0, 3)], ring_send.at[3 + item])
        for which in range(3):
            sent(whole[which].at[pl.ds(0, 7)], x_send.at[which])
        sent(hid, h_send.at[0])
        sent(pps.at[pl.ds(0, 5), 0], p_send.at[0])
        pl.when(core == 1)(lambda: sent(pps.at[pl.ds(0, 9)], p_send.at[1]))
        for own, here in enumerate(count(halves)):
            pl.when(here)(lambda: sent(rss.at[pl.ds(0, 5 - own), 0], r_send.at[0]))
        for own, here in enumerate(count(whole_sums)):
            pl.when(here & (core == 0))(lambda: sent(rss.at[pl.ds(0, 9 - own)], r_send.at[2]))
        pl.when(jnp.logical_not(route(step, step)[3]))(lambda: sent(last, r_send.at[1]))

    collect()
    finish()
    drain()


def local(activations, norm_gain, qw, kw, vw, gw, ow, mlp_gain, uw, dw):
    cosine, sine = rotary_tables()
    operands = (
        activations, norm_gain.reshape(1, D), qw.T, kw.T, vw.T, gw.T, ow, mlp_gain.reshape(1, D), uw, dw,
        jnp.asarray(cosine), jnp.asarray(sine),
    )
    dma = pltpu.SemaphoreType.DMA
    rows = pl.pallas_call(
        layer_kernel,
        out_shape=pltpu.VMEM((ROWS, D // 8), BF),
        in_specs=[pl.BlockSpec(memory_space=pltpu.HBM)] * len(operands),
        out_specs=pl.BlockSpec(memory_space=pltpu.VMEM),
        scratch_shapes=[
            pltpu.VMEM((2, 4, 4, 160, 128), BF),
            pltpu.VMEM((2, 4, 4, 128, 512), BF),
            pltpu.VMEM((2, 4, 4, 512, 128), BF),
            pltpu.VMEM((8, ROWS, 256), BF),
            pltpu.VMEM((8, 2, 4, 4, 32, 128), BF),
            pltpu.VMEM((8, 192, 128), BF),
            pltpu.VMEM((ROWS, D), BF),
            pltpu.VMEM((8, ROWS, 256), BF),
            pltpu.VMEM((ROWS, 1024), BF),
            pltpu.VMEM((16, 2, 192, 128), BF),
            pltpu.VMEM((16, 2, 192, 128), BF),
            pltpu.VMEM((16, 2, 192, 128), BF),
            pltpu.VMEM((4, 2, 2, 192, 128), BF),
            pltpu.VMEM((4, 64, 128), BF),
            pltpu.VMEM((2, 1, D), F32),
            pltpu.VMEM((2, 128, 128), F32),
            pltpu.VMEM((ROWS, 256), F32),
            pltpu.VMEM((ROWS, 128), F32),
            pltpu.VMEM((ROWS, 512), BF),
            pltpu.VMEM((16, ROWS, 128), F32),
            pltpu.VMEM((ROWS, 1024), BF),
            pltpu.VMEM((2, 512, 128), BF),
            pltpu.VMEM((2, 192, 128), BF),
            dma((7,)), dma((6,)), dma((6,)), dma((12,)), dma((3,)), dma((12,)), dma((2,)), dma((6,)), dma((3,)), dma((3,)), dma((1,)), dma((1,)),
        ],
        compiler_params=pltpu.CompilerParams(
            collective_id=0, has_side_effects=True, vmem_limit_bytes=56 * 1024 * 1024
        ),
        name="layer",
    )(*operands)
    return rows


def solution(mesh):
    in_specs = (
        P(("rep", "fs"), "tp"), P(), P("fs", "tp"), P("fs", "tp"), P("fs", "tp"), P("fs", "tp"), P("tp", "fs"), P(),
        P("fs", "tp"), P("tp", "fs"),
    )
    return jax.shard_map(local, mesh=mesh, in_specs=in_specs, out_specs=P(("rep", "fs"), "tp"), check_vma=False)
```

```python
import numpy as np
import jax
import jax.numpy as jnp
from jax import lax
from jax.experimental import pallas as pl
from jax.experimental.pallas import tpu as pltpu
from jax.sharding import PartitionSpec as P

HEADS = 8
HEAD_DIM = 64
SEQ_LEN = 128
EPSILON = 1e-06
ROWS = 384
D = 2048
NX = 4
BF = jnp.bfloat16
F32 = jnp.float32
MESH = pl.DeviceIdType.MESH
ATTN, UP, DOWN = 0, 1, 2
ORDER = ((0, 1, 2, -1), (2, -1, 0, 1))


def rotary_tables():
    half = HEAD_DIM // 2
    position = np.arange(SEQ_LEN, dtype=np.float32)
    freqs = np.float32(10000.0) ** (-np.arange(half, dtype=np.float32) / np.float32(half))
    angle = position[:, None] * freqs[None, :].astype(np.float32)
    cosine, sine = np.cos(angle), np.sin(angle)
    scale = np.float32(HEAD_DIM**-0.5)
    c = np.concatenate([cosine, cosine, cosine * scale, cosine * scale], axis=1)
    s = np.concatenate([-sine, sine, -sine * scale, sine * scale], axis=1)
    return c.astype(np.float32), s.astype(np.float32)


def log_gammas():
    head = np.arange(HEADS, dtype=np.float32)
    exponent = np.float32(5.0) + np.float32(4.0) * head / np.float32(HEADS - 1)
    return np.log(1.0 - np.power(2.0, -exponent.astype(np.float64)))


def lanes(shape):
    return lax.broadcasted_iota(jnp.int32, shape, len(shape) - 1)


def layer_kernel(
    act_hbm, ng_hbm, qw_hbm, kw_hbm, vw_hbm, gw_hbm, ow_hbm, mg_hbm, uw_hbm, dw_hbm, cos_hbm, sin_hbm,
    out_ref,
    attn, upb, dnb, xall, wo, ret, wide, mid, hid, pps, ppr, rss, rsr,
    small, gains, tables, qkvg, gat, lhs, acc,
    hid2, ext, last, local_sem, ring_send, first_recv, second_recv, x_send, x_recv, p_send, p_recv, r_send, r_recv, h_send, h_recv,
):
    rep, fs, tp = lax.axis_index("rep"), lax.axis_index("fs"), lax.axis_index("tp")
    zl, y = lax.div(fs, 4), lax.rem(fs, 4)
    x, core = lax.div(tp, 2), lax.rem(tp, 2)
    zg = rep * 4 + zl

    def y_device(step):
        return {"fs": zl * 4 + lax.rem(y + step + 4, 4)}

    def z_device(step):
        other = lax.rem(zg + step + 8, 8)
        return {"rep": lax.div(other, 4), "fs": lax.rem(other, 4) * 4 + y}

    def x_index(step, c=core):
        return lax.rem(x + step + 4, 4) * 2 + c

    def x_device(step):
        return {"tp": x_index(step)}

    partner = {"tp": x * 2 + (1 - core)}

    barrier = pltpu.get_barrier_semaphore()
    peers = [y_device(1), y_device(-1), z_device(1), z_device(-1), x_device(1), x_device(-1), partner]
    for peer in peers:
        pl.semaphore_signal(barrier, inc=1, device_id=peer, device_id_type=MESH)

    loads = (
        (qw_hbm, small.at[0], 0),
        (kw_hbm, small.at[1], 0),
        (vw_hbm, small.at[2], 0),
        (gw_hbm, small.at[3], 0),
        (ow_hbm.at[pl.ds(0, 32)], attn.at[0, zl, y, pl.ds(128, 32)], 1),
        (ow_hbm.at[pl.ds(32, 32)], attn.at[1, zl, y, pl.ds(128, 32)], 1),
        (act_hbm, xall.at[tp], 2),
        (uw_hbm.at[:, pl.ds(0, 512)], upb.at[0, zl, y], 3),
        (uw_hbm.at[:, pl.ds(512, 512)], upb.at[1, zl, y], 3),
        (dw_hbm.at[pl.ds(0, 512)], dnb.at[0, zl, y], 4),
        (dw_hbm.at[pl.ds(512, 512)], dnb.at[1, zl, y], 4),
        (ng_hbm, gains.at[0], 5),
        (mg_hbm, gains.at[1], 5),
        (cos_hbm, tables.at[0], 6),
        (sin_hbm, tables.at[1], 6),
    )
    for src, dst, n in loads:
        pltpu.make_async_copy(src, dst, local_sem.at[n]).start()

    def loaded(region, n):
        pltpu.make_async_copy(region, region, local_sem.at[n]).wait()

    loaded(small, 0)
    loaded(attn.at[0, 0, 0, pl.ds(0, 64)], 1)
    for h in range(2):
        attn[h, zl, y, 0:128, :] = small[2 * h : 2 * h + 2].reshape(128, 128).astype(F32).T.astype(BF)
    pl.semaphore_wait(barrier, len(peers))

    def remote(src, dst, send_sem, recv_sem, device):
        return pltpu.make_async_remote_copy(
            src_ref=src, dst_ref=dst, send_sem=send_sem, recv_sem=recv_sem, device_id=device, device_id_type=MESH
        )

    def send(src, dst, send_sem, recv_sem, device):
        remote(src, dst, send_sem, recv_sem, device).start()

    def arrive(region, recv_sem):
        remote(region, region, r_send.at[0], recv_sem, partner).wait_recv()

    def sent(region, send_sem):
        remote(region, region, send_sem, r_recv.at[0], partner).wait_send()

    bufs = (attn, upb, dnb)
    depth = (160, 128, 512)

    def block(item, half, dz, dy):
        return bufs[item].at[half, lax.rem(zl + dz + 4, 4), lax.rem(y + dy + 4, 4)]

    def along_y(half, phase):
        return (half + phase) % 2 == 0

    def piece(item, half, step, p):
        cut = depth[item] // 2
        dz, dy = (0, step) if half == 0 else (step, 0)
        return block(item, half, dz, dy).at[pl.ds(p * cut, cut)]

    def ring_device(half, phase, step):
        return y_device(step) if along_y(half, phase) else z_device(step)

    def first_start(item):
        for n in range(2):
            for half in range(2):
                for d in range(2):
                    ref = piece(item, half, 0, n if d == 0 else 1 - n)
                    send(ref, ref, ring_send.at[item], first_recv.at[2 * item + n], ring_device(half, 0, 1 - 2 * d))

    def first_forward(item):
        arrive(bufs[item].at[0, 0, pl.ds(0, 2)], first_recv.at[2 * item])
        for half in range(2):
            for d in range(2):
                to = 1 - 2 * d
                ref = piece(item, half, -to, d)
                send(ref, ref, ring_send.at[item], first_recv.at[2 * item + 1], ring_device(half, 0, to))

    def first_rest(item):
        arrive(bufs[item].at[0, 0], first_recv.at[2 * item + 1])

    def second_block(item, half, step, d, n):
        across = ORDER[d][n]
        return block(item, half, step, across) if half == 0 else block(item, half, across, step)

    def second_sem(item, n, far):
        if n < 2 and not far:
            return second_recv.at[2 * item + n]
        return second_recv.at[6 + item] if item < DOWN else second_recv.at[8 + n]

    def second_start(item, *which):
        for n in which:
            for half in range(2):
                for d in range(2):
                    ref = second_block(item, half, 0, d, n)
                    send(ref, ref, ring_send.at[3 + item], second_sem(item, n, False), ring_device(half, 1, 1 - 2 * d))

    def second_forward(item, *which):
        for n in which:
            arrive(bufs[item].at[0, 0], second_sem(item, n, False))
            for half in range(2):
                for d in range(2):
                    to = 1 - 2 * d
                    ref = second_block(item, half, -to, d, n)
                    send(ref, ref, ring_send.at[3 + item], second_sem(item, n, True), ring_device(half, 1, to))

    def second_forward_on(c, item, n):
        @pl.when(core == c)
        def _():
            second_forward(item, n)

    def second_rest(item):
        arrive(bufs[item].at[0], second_sem(item, 0, True))

    def second_four(item, n, far):
        arrive(bufs[item].at[0, 0], second_sem(item, n, far))

    def x_piece(which, t, p):
        if which == 0:
            return xall.at[t, pl.ds(p * 192, 192)]
        if which == 1:
            return wo.at[t, p]
        return ret.at[t, pl.ds(p * 96, 96)]

    whole = (xall, wo, ret)

    def x_sem(which, kind):
        return x_recv.at[which * 4 + kind]

    def hand_over(which, place, p):
        ref = x_piece(which, x_index((0, -1, 1, 2)[place]), p)
        send(ref, ref, x_send.at[which], x_sem(which, 3), partner)

    def x_start(which):
        for n in range(2):
            for d in range(2):
                p = n if d == 0 else 1 - n
                dst = x_piece(which, tp, p)
                src = attn.at[p, :, :, pl.ds(128, 32)] if which == 1 else dst
                send(src, dst, x_send.at[which], x_sem(which, n), x_device(1 - 2 * d))
        for p in range(2):
            dst = x_piece(which, tp, p)
            src = attn.at[p, :, :, pl.ds(128, 32)] if which == 1 else dst
            send(src, dst, x_send.at[which], x_sem(which, 3), partner)

    def x_forward(which):
        arrive(whole[which].at[0], x_sem(which, 0))
        for d in range(2):
            to = 1 - 2 * d
            ref = x_piece(which, x_index(-to), d)
            send(ref, ref, x_send.at[which], x_sem(which, 2), x_device(to))
            hand_over(which, 1 + d, d)

    def x_near(which):
        arrive(whole[which].at[0], x_sem(which, 1))
        for d in range(2):
            hand_over(which, 1 + d, 1 - d)

    def x_far(which):
        arrive(whole[which].at[0], x_sem(which, 2))
        for d in range(2):
            hand_over(which, 3, d)

    def x_partner(which):
        arrive(whole[which].at[pl.ds(0, 4)], x_sem(which, 3))

    def norm_rows(source, gain):
        @pl.loop(0, ROWS // 16)
        def _(i):
            rows = pl.ds(pl.multiple_of(i * 16, 16), 16)
            blocks = [source[t, rows, :].astype(F32) for t in range(8)]
            squares = blocks[0] * blocks[0]
            for b in blocks[1:]:
                squares = squares + b * b
            scale = lax.rsqrt(jnp.sum(squares, axis=-1, keepdims=True) * (1.0 / D) + EPSILON)
            for t in range(8):
                columns = slice(256 * t, 256 * t + 256)
                wide[rows, columns] = (blocks[t] * scale * gains[gain, :, columns]).astype(BF)

    first_start(ATTN)
    loaded(xall.at[0], 2)
    x_start(0)
    loaded(upb.at[0, 0, pl.ds(0, 2)], 3)
    first_start(UP)
    loaded(dnb.at[0, 0, pl.ds(0, 2)], 4)
    loaded(gains, 5)
    loaded(tables, 6)
    first_forward(ATTN)
    first_forward(UP)
    x_forward(0)
    first_rest(ATTN)
    second_start(ATTN, 0, 1, 2, 3)
    first_start(DOWN)
    x_near(0)
    second_forward(ATTN, 0, 1)
    first_rest(UP)
    second_start(UP, 0)
    x_far(0)
    x_partner(0)
    norm_rows(xall, 0)
    first_forward(DOWN)
    second_start(UP, 1, 2, 3)
    second_rest(ATTN)
    x_start(1)

    weights = jnp.concatenate([attn[h, :, :, 0:128, :].reshape(D, 128) for h in range(2)], axis=1)
    qkvg[...] = jnp.dot(wide[...], weights, preferred_element_type=F32)
    log_gamma = jnp.float32(0.0)
    for h, value in enumerate(log_gammas()):
        log_gamma = jnp.where(tp == h, jnp.float32(value), log_gamma)
    square = (SEQ_LEN, SEQ_LEN)
    distance = (lax.broadcasted_iota(jnp.int32, square, 0) - lanes(square)).astype(F32)
    decay = jnp.where(distance >= 0, jnp.exp(jnp.maximum(distance, 0.0) * log_gamma), 0.0)
    lane = lanes(square)
    first, low = lax.rem(lane, 64) < 32, lane < 64
    for s in range(3):
        rows = slice(SEQ_LEN * s, SEQ_LEN * (s + 1))
        qk, vg = qkvg[rows, 0:128], qkvg[rows, 128:256]
        other = jnp.where(first, pltpu.roll(qk, 96, 1), pltpu.roll(qk, 32, 1))
        turned = (qk * tables[0] + other * tables[1]).astype(BF).astype(F32)
        queries = jnp.where(low, turned, 0.0).astype(BF)
        keys = pltpu.roll(turned, 64, 1).astype(BF)
        scores = lax.dot_general(queries, keys, (((1,), (1,)), ((), ())), preferred_element_type=F32)
        mixed = jnp.dot((scores * decay).astype(BF), vg.astype(BF), preferred_element_type=F32)
        mixed = jnp.where(low, mixed, 0.0)
        mean = jnp.sum(mixed, axis=-1, keepdims=True) * (1.0 / HEAD_DIM)
        centred = jnp.where(low, mixed - mean, 0.0)
        variance = jnp.sum(centred * centred, axis=-1, keepdims=True) * (1.0 / HEAD_DIM)
        gate = pltpu.roll(vg, 64, 1)
        gat[rows, :] = centred * lax.rsqrt(variance + EPSILON) * (gate / (1.0 + jnp.exp(-gate)))
    low = lanes((192, 128)) < 64
    ret[tp] = jnp.where(low, gat[0:192, :], pltpu.roll(gat[192:384, :], 64, 1)).astype(BF)
    x_start(2)
    for h in range(2):
        wo[tp, h] = attn[h, :, :, 128:160, :]
    x_forward(1)
    second_forward(UP, 0)
    x_forward(2)
    second_forward(UP, 1)
    first_rest(DOWN)
    second_start(DOWN, 0, 1)
    x_near(2)
    x_near(1)
    x_far(2)
    x_far(1)
    x_partner(2)
    x_partner(1)

    for j in range(4):
        a, b = ret[2 * j].astype(F32), ret[2 * j + 1].astype(F32)
        lhs[0:192, 128 * j : 128 * j + 128] = jnp.where(low, a, pltpu.roll(b, 64, 1)).astype(BF)
        lhs[192:384, 128 * j : 128 * j + 128] = jnp.where(low, pltpu.roll(a, 64, 1), b).astype(BF)

    @pl.loop(0, 8)
    def _(t):
        z0, y0 = lax.div(t, 2), lax.rem(t, 2) * 2
        columns = [wo[:, :, z0, y0 + k].reshape(HEADS * HEAD_DIM, 128) for k in range(2)]
        branch = jnp.dot(lhs[...], jnp.concatenate(columns, axis=1), preferred_element_type=F32)
        mid[t] = (xall[t].astype(F32) + branch).astype(BF)

    norm_rows(mid, 1)
    second_rest(UP)
    second_forward_on(1, DOWN, 0)
    for h in range(2):
        raw = jnp.dot(wide[...], upb[h].reshape(D, 512), preferred_element_type=F32)
        raw = jnp.maximum(raw, 0.0)
        hid[:, 512 * h : 512 * h + 512] = (raw * raw).astype(BF)
    second_forward_on(0, DOWN, 0)
    send(hid, hid2, h_send.at[0], h_recv.at[0], partner)

    def number(dz, dy):
        return (dz + 1) * 4 + dy + 1

    def last_start():
        for half in range(2):
            for d in range(2):
                ref, sem = second_block(DOWN, half, 0, d, 3), second_sem(DOWN, 3, False)
                there = ring_device(half, 1, 1 - 2 * d)

                @pl.when(core == d)
                def _():
                    send(ref, ref, ring_send.at[3 + DOWN], sem, there)

                @pl.when(core != d)
                def _():
                    send(ref, ext.at[half], ring_send.at[3 + DOWN], sem, {**there, "tp": x * 2 + d})

    def on_core(c, step):
        pl.when(core == c)(step)

    begun = set()

    def products(pairs):
        done = []
        for half, blocks in pairs:
            columns = jnp.concatenate([block(DOWN, half, dz, dy)[...] for dz, dy in blocks], axis=1)
            both = jnp.dot(hid[:, 512 * half : 512 * half + 512], columns, preferred_element_type=F32)
            for k, at in enumerate(blocks):
                value, n = both[:, 128 * k : 128 * k + 128], number(*at)
                if at in begun:
                    acc[n] += value
                    done.append(at)
                else:
                    acc[n] = value
                    begun.add(at)
        return done

    def rows_of(c):
        return pl.ds(pl.multiple_of(c * 192, 64), 192)

    def swap(blocks, group):
        for at in blocks:
            n = number(*at)
            pps[n, 0] = acc[n, rows_of(1 - core), :].astype(BF)
            send(pps.at[n, 0], ppr.at[n, 0], p_send.at[0], p_recv.at[group], partner)

    def give(blocks, group):
        @pl.when(core == 1)
        def _():
            for at in blocks:
                n = number(*at)
                pps[n] = acc[n].astype(BF).reshape(2, 192, 128)
                send(pps.at[n], ppr.at[n], p_send.at[1], p_recv.at[group], partner)


    def route(dz, dy):
        z_to, y_to = lax.rem(zl + dz + 4, 4), lax.rem(y + dy + 4, 4)
        c_to, k = lax.div(y_to, 2), lax.rem(y_to, 2)
        hops = lax.rem(z_to - x + 4, 4)
        return {"tp": z_to * 2 + c_to}, k, hops, (hops == 0) & (c_to == core), lax.div(3 - hops, 3) * (1 + k)

    def deliver(blocks, group):
        arrive(ppr.at[pl.ds(0, len(blocks)), 0], p_recv.at[group])
        for at in blocks:
            n = number(*at)
            owner, k, hops, own, sem = route(*at)
            total = (acc[n, rows_of(core), :] + ppr[n, 0].astype(F32)).astype(BF)
            rss[n, 0] = total

            @pl.when(jnp.logical_not(own))
            def _():
                send(rss.at[n, 0], rsr.at[hops, k, core], r_send.at[0], r_recv.at[sem], owner)

            @pl.when(own)
            def _():
                rsr[0, k, core] = total

    def deliver_whole(blocks, group):
        @pl.when(core == 0)
        def _():
            arrive(ppr.at[pl.ds(0, len(blocks))], p_recv.at[group])
            for at in blocks:
                n = number(*at)
                owner, k, hops, own, sem = route(*at)
                total = (acc[n].reshape(2, 192, 128) + ppr[n].astype(F32)).astype(BF)
                rss[n] = total

                @pl.when(jnp.logical_not(own))
                def _():
                    send(rss.at[n], rsr.at[hops, k], r_send.at[2], r_recv.at[sem], owner)

                @pl.when(own)
                def _():
                    rsr[0, k] = total

    step = 2 * core - 1

    def deliver_last():
        owner, k, hops, own, sem = route(step, step)
        z_from, y_from = lax.rem(zl + step + 4, 4), lax.rem(y + step + 4, 4)
        mine = jnp.concatenate([dnb[0, z_from, y_from], dnb[1, z_from, y_from]], axis=0)
        other = ext[...].reshape(1024, 128)
        for half in range(2):
            rows = slice(192 * half, 192 * half + 192)
            total = jnp.dot(hid[rows, :], mine, preferred_element_type=F32)
            total = (total + jnp.dot(hid2[rows, :], other, preferred_element_type=F32)).astype(BF)
            last[half] = total

            @pl.when(jnp.logical_not(own))
            def _():
                send(last.at[half], rsr.at[hops, k, half], r_send.at[1], r_recv.at[sem], owner)

            @pl.when(own)
            def _():
                rsr[0, k, half] = total

    def arrivals(n, far):
        step = (2, 2) if far else (-1, 1)
        rows = [(step[d], ORDER[d][n]) for d in range(2)]
        columns = [(ORDER[d][n], step[d]) for d in range(2)]
        return [(0, rows), (1, columns)]

    own = [(0, [(0, 0), (0, 1)]), (0, [(0, -1), (0, 2)]), (1, [(0, 0), (1, 0)]), (1, [(-1, 0), (2, 0)])]
    def deliver_on(c, blocks, group):
        @pl.when(core == c)
        def _():
            deliver(blocks, group)

    s0 = products(own)
    swap(s0, 0)
    s1 = products(arrivals(0, False))
    swap(s1, 1)
    second_forward(DOWN, 1)
    on_core(0, lambda: second_start(DOWN, 2))
    on_core(0, last_start)
    s2 = products(arrivals(1, False))
    swap(s2, 2)
    deliver_on(0, s0, 0)
    deliver_on(0, s1, 1)
    second_four(DOWN, 0, True)
    on_core(1, lambda: second_start(DOWN, 2))
    s3 = products(arrivals(0, True))
    give(s3, 3)
    deliver_on(1, s0, 0)
    deliver_on(1, s1, 1)
    deliver(s2, 2)
    deliver_whole(s3, 3)
    second_four(DOWN, 1, True)
    on_core(1, last_start)
    s4 = products(arrivals(1, True))
    give(s4, 4)
    deliver_whole(s4, 4)
    second_four(DOWN, 2, False)
    s5 = products(arrivals(2, False))
    give(s5, 5)
    deliver_whole(s5, 5)
    arrive(hid2, h_recv.at[0])
    second_four(DOWN, 3, False)
    deliver_last()

    def among(k, blocks):
        dz, dy = lax.rem(x - zl + 4, 4), lax.rem(core * 2 + k - y + 4, 4)
        found = None
        for at in blocks:
            here = (dz == at[0] % 4) & (dy == at[1] % 4)
            found = here if found is None else found | here
        return found

    halves = [among(k, s0 + s1 + s2) for k in range(2)]
    on_one = [among(k, [(1, 1)]) for k in range(2)]
    on_zero = [jnp.logical_not(halves[k] | on_one[k]) for k in range(2)]
    whole_sums = [among(k, s3 + s4 + s5) for k in range(2)]

    def collect():
        arrive(rss.at[pl.ds(0, 6)], r_recv.at[0])
        for k in range(2):

            @pl.when((on_zero[k] & (core == 1)) | (on_one[k] & (core == 0)))
            def _():
                arrive(rsr.at[0, k], r_recv.at[1 + k])

            @pl.when(halves[k])
            def _():
                arrive(rsr.at[0, k, 1 - core], r_recv.at[1 + k])

    def count(pair):
        both, some = pair[0] & pair[1], pair[0] | pair[1]
        return [jnp.logical_not(some), some & jnp.logical_not(both), both]

    def finish():
        for k in range(2):
            for half in range(2):
                rows, columns = slice(192 * half, 192 * half + 192), slice(128 * k, 128 * k + 128)
                total = mid[tp, rows, columns].astype(F32)
                for hops in range(4):
                    total = total + rsr[hops, k, half].astype(F32)
                out_ref[rows, columns] = total.astype(BF)

    def drain():
        for item in range(3):
            sent(bufs[item].at[:, pl.ds(0, 3), 0], ring_send.at[item])
            sent(bufs[item].at[:, pl.ds(0, 3)], ring_send.at[3 + item])
        for which in range(3):
            sent(whole[which].at[pl.ds(0, 7)], x_send.at[which])
        sent(hid, h_send.at[0])
        sent(pps.at[pl.ds(0, 5), 0], p_send.at[0])
        pl.when(core == 1)(lambda: sent(pps.at[pl.ds(0, 9)], p_send.at[1]))
        for own, here in enumerate(count(halves)):
            pl.when(here)(lambda: sent(rss.at[pl.ds(0, 5 - own), 0], r_send.at[0]))
        for own, here in enumerate(count(whole_sums)):
            pl.when(here & (core == 0))(lambda: sent(rss.at[pl.ds(0, 9 - own)], r_send.at[2]))
        pl.when(jnp.logical_not(route(step, step)[3]))(lambda: sent(last, r_send.at[1]))

    collect()
    finish()
    drain()


def local(activations, norm_gain, qw, kw, vw, gw, ow, mlp_gain, uw, dw):
    cosine, sine = rotary_tables()
    operands = (
        activations, norm_gain.reshape(1, D), qw.T, kw.T, vw.T, gw.T, ow, mlp_gain.reshape(1, D), uw, dw,
        jnp.asarray(cosine), jnp.asarray(sine),
    )
    dma = pltpu.SemaphoreType.DMA
    rows = pl.pallas_call(
        layer_kernel,
        out_shape=pltpu.VMEM((ROWS, D // 8), BF),
        in_specs=[pl.BlockSpec(memory_space=pltpu.HBM)] * len(operands),
        out_specs=pl.BlockSpec(memory_space=pltpu.VMEM),
        scratch_shapes=[
            pltpu.VMEM((2, 4, 4, 160, 128), BF),
            pltpu.VMEM((2, 4, 4, 128, 512), BF),
            pltpu.VMEM((2, 4, 4, 512, 128), BF),
            pltpu.VMEM((8, ROWS, 256), BF),
            pltpu.VMEM((8, 2, 4, 4, 32, 128), BF),
            pltpu.VMEM((8, 192, 128), BF),
            pltpu.VMEM((ROWS, D), BF),
            pltpu.VMEM((8, ROWS, 256), BF),
            pltpu.VMEM((ROWS, 1024), BF),
            pltpu.VMEM((16, 2, 192, 128), BF),
            pltpu.VMEM((16, 2, 192, 128), BF),
            pltpu.VMEM((16, 2, 192, 128), BF),
            pltpu.VMEM((4, 2, 2, 192, 128), BF),
            pltpu.VMEM((4, 64, 128), BF),
            pltpu.VMEM((2, 1, D), F32),
            pltpu.VMEM((2, 128, 128), F32),
            pltpu.VMEM((ROWS, 256), F32),
            pltpu.VMEM((ROWS, 128), F32),
            pltpu.VMEM((ROWS, 512), BF),
            pltpu.VMEM((16, ROWS, 128), F32),
            pltpu.VMEM((ROWS, 1024), BF),
            pltpu.VMEM((2, 512, 128), BF),
            pltpu.VMEM((2, 192, 128), BF),
            dma((7,)), dma((6,)), dma((6,)), dma((12,)), dma((3,)), dma((12,)), dma((2,)), dma((6,)), dma((3,)), dma((3,)), dma((1,)), dma((1,)),
        ],
        compiler_params=pltpu.CompilerParams(
            collective_id=0, has_side_effects=True, vmem_limit_bytes=56 * 1024 * 1024
        ),
        name="layer",
    )(*operands)
    return rows


def solution(mesh):
    in_specs = (
        P(("rep", "fs"), "tp"), P(), P("fs", "tp"), P("fs", "tp"), P("fs", "tp"), P("fs", "tp"), P("tp", "fs"), P(),
        P("fs", "tp"), P("tp", "fs"),
    )
    return jax.shard_map(local, mesh=mesh, in_specs=in_specs, out_specs=P(("rep", "fs"), "tp"), check_vma=False)
```
